32 devices in a mesh: rep: 2 (over x), fs: 8 (over z, y), tp: 2 (over core).
Axes of the slice: x: 2, y: 2, z: 4, core: 2. Of those that a mesh axis runs over, the one named last changes fastest.
Arguments:
- tokens_in: bfloat16 [4096, 2048], P(('rep', 'fs', 'tp')), may hold values from -6 to 6
- norm_gains: float32 [3, 2048], replicated, may hold values from 0.1 to 1.9
- gate_w: float32 [2048, 3072], P('fs', 'tp'), may hold values from -0.125 to 0.125
- gate_scale: float32 [3072], P('tp'), may hold values from 0.5 to 2
- up_w: float32 [2048, 3072], P('fs', 'tp'), may hold values from -0.125 to 0.125
- up_scale: float32 [3072], P('tp'), may hold values from 0.5 to 2
- down_w: float32 [3072, 2048], P('tp', 'fs'), may hold values from -0.109375 to 0.109375
- down_scale: float32 [2048], P('fs'), may hold values from 0.5 to 2
- query_w: float32 [2048, 2048], P('fs', 'tp'), may hold values from -0.125 to 0.125
- query_scale: float32 [2048], P('tp'), may hold values from 0.5 to 2
- key_w: float32 [2048, 2048], P('fs', 'tp'), may hold values from -0.125 to 0.125
- key_scale: float32 [2048], P('tp'), may hold values from 0.5 to 2
- value_w: float32 [2048, 2048], P('fs', 'tp'), may hold values from -0.125 to 0.125
- value_scale: float32 [2048], P('tp'), may hold values from 0.5 to 2
- out_w: float32 [2048, 2048], P('tp', 'fs'), may hold values from -0.125 to 0.125
- out_scale: float32 [2048], P('fs'), may hold values from 0.5 to 2
- head_gain: float32 [256], replicated, may hold values from 0.1 to 1.9
- decay_rate: float32 [8], P('tp'), may hold values from 0 to 1, as said below
Outputs:
- tokens_out: bfloat16 [4096, 2048], P(('rep', 'fs', 'tp'))
The draws below stay inside these ranges and needn't reach their ends.
Inputs may be any that keep to these rules, and one draw needn't show every extreme that they name: `decay_rate`: each head's decay per position, positive.
All inputs are finite; a program needn't handle non-finite values.
Results may differ from the reference program's by a relative error of at most 0.02.
Values may be sent and summed in bfloat16 or wider, within the bound.
A program may use at most 128 MiB of HBM per device.

```python
import math
import jax
import jax.numpy as jnp
from jax import lax

D = 2048
FF = 3072
HEADS = 8
DK = 256
DV = 256
BLOCK = 64
SEQ = 256
TOKENS = 4096
N_TP = 2


def draw_decay_rate(key, part):
    uniform_draw = jax.random.uniform(key, (HEADS,), jnp.float32)
    lowest, highest = (0.5, 16.0)
    spread = jnp.log(highest) - jnp.log(lowest)
    return jnp.exp(jnp.log(lowest) + uniform_draw * spread) / SEQ


def steps_of(rng, shape, shards, least, high):
    level, own = 1.0, jax.random.fold_in(rng, 6)
    for dim, shards_of in shards:
        heights = jnp.exp(jax.random.uniform(jax.random.fold_in(own, dim), (shards_of,), jnp.float32, least / len(shards), high / len(shards)))
        level = level * jnp.repeat(heights, shape[dim] // shards_of).reshape([-1 if axis == dim else 1 for axis in range(len(shape))])
    return level


def noise(own_key, shape, width, most, cuts=(), held_as=jnp.bfloat16):
    drawn = jax.random.normal(own_key, shape, jnp.float32) * width
    if len(cuts) > 0:
        drawn = steps_of(own_key, shape, cuts, -0.22, 0.18) * drawn
    return jnp.clip(drawn, min=-most, max=most).astype(held_as)


def setup_inputs(seed: int = 0) -> dict:
    streams_of = jax.random.split(jax.random.key(seed), 19)
    tokens_in = noise(streams_of[0], (TOKENS, D), 1.0, 6.0, ((0, 32),))
    norm_gains = jnp.clip(1.0 + 0.18 * jax.random.normal(streams_of[1], (3, D), jnp.float32), 0.1, 1.9)
    gate_w = noise(streams_of[2], (D, FF), D ** -0.5, 0.125, ((0, 8), (1, 2)), jnp.float32)
    gate_scale = jnp.clip(jnp.exp(math.log(2.0) - 1.3862944 * jax.random.uniform(streams_of[3], (FF,), jnp.float32) ** steps_of(streams_of[3], (FF,), ((0, 2),), -0.2, 0.2)), 0.5, 2.0)
    up_w = noise(streams_of[4], (D, FF), D ** -0.5, 0.125, ((0, 8), (1, 2)), jnp.float32)
    up_scale = jnp.clip(jnp.exp(math.log(2.0) - 1.3862944 * jax.random.uniform(streams_of[5], (FF,), jnp.float32) ** steps_of(streams_of[5], (FF,), ((0, 2),), -0.2, 0.2)), 0.5, 2.0)
    down_w = noise(streams_of[6], (FF, D), FF ** -0.5, 0.109375, ((0, 2), (1, 8)), jnp.float32)
    down_scale = jnp.clip(jnp.exp(math.log(2.0) - 1.3862944 * jax.random.uniform(streams_of[7], (D,), jnp.float32) ** steps_of(streams_of[7], (D,), ((0, 8),), -0.2, 0.2)), 0.5, 2.0)
    query_w = noise(streams_of[8], (D, HEADS * DK), D ** -0.5, 0.125, ((0, 8), (1, 2)), jnp.float32)
    query_scale = jnp.clip(jnp.exp(math.log(2.0) - 1.3862944 * jax.random.uniform(streams_of[9], (HEADS * DK,), jnp.float32) ** steps_of(streams_of[9], (HEADS * DK,), ((0, 2),), -0.2, 0.2)), 0.5, 2.0)
    key_w = noise(streams_of[10], (D, HEADS * DK), D ** -0.5, 0.125, ((0, 8), (1, 2)), jnp.float32)
    key_scale = jnp.clip(jnp.exp(math.log(2.0) - 1.3862944 * jax.random.uniform(streams_of[11], (HEADS * DK,), jnp.float32) ** steps_of(streams_of[11], (HEADS * DK,), ((0, 2),), -0.2, 0.2)), 0.5, 2.0)
    value_w = noise(streams_of[12], (D, HEADS * DV), D ** -0.5, 0.125, ((0, 8), (1, 2)), jnp.float32)
    value_scale = jnp.clip(jnp.exp(math.log(2.0) - 1.3862944 * jax.random.uniform(streams_of[13], (HEADS * DV,), jnp.float32) ** steps_of(streams_of[13], (HEADS * DV,), ((0, 2),), -0.2, 0.2)), 0.5, 2.0)
    out_w = noise(streams_of[14], (HEADS * DV, D), (HEADS * DV) ** -0.5, 0.125, ((0, 2), (1, 8)), jnp.float32)
    out_scale = jnp.clip(jnp.exp(math.log(2.0) - 1.3862944 * jax.random.uniform(streams_of[15], (D,), jnp.float32) ** steps_of(streams_of[15], (D,), ((0, 8),), -0.2, 0.2)), 0.5, 2.0)
    head_gain = jnp.clip(1.0 + 0.18 * jax.random.normal(streams_of[16], (DV,), jnp.float32), 0.1, 1.9)
    decay_rate = draw_decay_rate(jax.random.fold_in(streams_of[18], 71), 0)
    return dict(tokens_in=tokens_in, norm_gains=norm_gains, gate_w=gate_w, gate_scale=gate_scale, up_w=up_w, up_scale=up_scale, down_w=down_w, down_scale=down_scale, query_w=query_w, query_scale=query_scale, key_w=key_w, key_scale=key_scale, value_w=value_w, value_scale=value_scale, out_w=out_w, out_scale=out_scale, head_gain=head_gain, decay_rate=decay_rate)


EPSILON = 1e-05

def rms_scale(stream, gain):
    return stream * lax.rsqrt(lax.optimization_barrier(jnp.mean(stream * stream, axis=-1, keepdims=True)) + EPSILON) * gain

def group_sum(hidden, weight, scale):
    groups = hidden.reshape(hidden.shape[0], N_TP, -1).transpose(1, 0, 2)
    blocks_w = weight.reshape(N_TP, -1, weight.shape[1])

    def one_group(operands):
        rounded = (jnp.dot(operands[0], operands[1], preferred_element_type=jnp.float32) * scale).astype(jnp.bfloat16)
        return lax.optimization_barrier(rounded).astype(jnp.float32)
    return lax.optimization_barrier(jnp.sum(lax.map(one_group, (groups, blocks_w)), axis=0))

def feed_forward(stream, gain, weights, scales):
    gate_b, up_b, down_b = weights
    normed = rms_scale(stream, gain).astype(jnp.bfloat16)
    gate_value = jnp.dot(normed, gate_b, preferred_element_type=jnp.float32) * scales[0]
    up_value = jnp.dot(normed, up_b, preferred_element_type=jnp.float32) * scales[1]
    hidden = (jax.nn.silu(gate_value) * up_value).astype(jnp.bfloat16)
    return group_sum(hidden, down_b, scales[2])

def retention(query, key_rows, value, decay_rate, head_gain):
    seq_len = query.shape[0]
    blocks = seq_len // BLOCK
    q_heads = query.astype(jnp.float32).reshape(blocks, BLOCK, HEADS, DK).transpose(0, 2, 1, 3)
    k_heads = key_rows.astype(jnp.float32).reshape(blocks, BLOCK, HEADS, DK).transpose(0, 2, 1, 3)
    v_heads = value.astype(jnp.float32).reshape(blocks, BLOCK, HEADS, DV).transpose(0, 2, 1, 3)
    offsets = jnp.arange(BLOCK, dtype=jnp.float32)
    inner_decay = jnp.exp(-decay_rate[:, None, None] * jnp.abs(offsets[:, None] - offsets[None, :]))
    query_decay = jnp.exp(-decay_rate[:, None] * offsets[None, :])[..., None]
    key_decay = jnp.exp(-decay_rate[:, None] * (BLOCK - offsets)[None, :])[..., None]
    block_decay = jnp.exp(-decay_rate * BLOCK)[:, None, None]

    def advance(state, inputs):
        q_blk, k_blk, v_blk = inputs
        scores = (jnp.einsum('hid,hjd->hij', q_blk, k_blk) * inner_decay).astype(jnp.bfloat16)
        scores = lax.optimization_barrier(scores).astype(jnp.float32)
        within = jnp.einsum('hij,hje->hie', scores, v_blk)
        carried = jnp.einsum('hid,hde->hie', q_blk * query_decay, state, precision=lax.Precision.HIGHEST)
        state = state * block_decay + jnp.einsum('hjd,hje->hde', k_blk * key_decay, v_blk, precision=lax.Precision.HIGHEST)
        return (state, within + carried)
    initial = jnp.zeros((HEADS, DK, DV), jnp.float32)
    _, retained = lax.scan(advance, initial, (q_heads, k_heads, v_heads))
    retained = retained.transpose(0, 2, 1, 3).reshape(seq_len, HEADS, DV)
    centred = retained - lax.optimization_barrier(jnp.mean(retained, axis=-1, keepdims=True))
    normed = centred * lax.rsqrt(lax.optimization_barrier(jnp.mean(centred * centred, axis=-1, keepdims=True)) + EPSILON) * head_gain
    return normed.reshape(seq_len, HEADS * DV).astype(jnp.bfloat16)

def reference(tokens_in, norm_gains, gate_w, gate_scale, up_w, up_scale, down_w, down_scale, query_w, query_scale, key_w, key_scale, value_w, value_scale, out_w, out_scale, head_gain, decay_rate):
    ffn_weights = (gate_w.astype(jnp.bfloat16), up_w.astype(jnp.bfloat16), down_w.astype(jnp.bfloat16))
    ffn_scales = (gate_scale, up_scale, down_scale)
    query_b = query_w.astype(jnp.bfloat16)
    key_b = key_w.astype(jnp.bfloat16)
    value_b = value_w.astype(jnp.bfloat16)
    out_b = out_w.astype(jnp.bfloat16)

    def one_sequence(stream_in):
        stream = stream_in.astype(jnp.float32)
        first = stream + 0.5 * feed_forward(stream, norm_gains[0], ffn_weights, ffn_scales)
        normed = rms_scale(first, norm_gains[1]).astype(jnp.bfloat16)
        query = (jnp.dot(normed, query_b, preferred_element_type=jnp.float32) * query_scale).astype(jnp.bfloat16)
        key_rows = (jnp.dot(normed, key_b, preferred_element_type=jnp.float32) * key_scale / math.sqrt(DK)).astype(jnp.bfloat16)
        value = (jnp.dot(normed, value_b, preferred_element_type=jnp.float32) * value_scale).astype(jnp.bfloat16)
        mixed = retention(query, key_rows, value, decay_rate, head_gain)
        second = first + group_sum(mixed, out_b, out_scale)
        final = second + 0.5 * feed_forward(second, norm_gains[2], ffn_weights, ffn_scales)
        return final.astype(jnp.bfloat16)
    sequences = tokens_in.reshape(-1, SEQ, D)
    return lax.map(one_sequence, sequences).reshape(-1, D)
```

```python
import functools
import math

import jax
import jax.numpy as jnp
from jax import lax
from jax.experimental import pallas as pl
from jax.experimental.pallas import tpu as pltpu
from jax.sharding import PartitionSpec as P

DK = 256
DV = 256
BLOCK = 64

EPSILON = 1e-05


def rms_scale(stream, gain):
    return stream * lax.rsqrt(jnp.mean(stream * stream, axis=-1, keepdims=True) + EPSILON) * gain


def snake(n):
    return [i for i in range(0, n, 2)] + [i for i in range(n - 1, 0, -1) if i % 2 == 1]


def snake_place(index, n):
    return jnp.where(index % 2 == 0, index // 2, n - 1 - index // 2)


def snake_index(place, n):
    half = (n + 1) // 2
    return jnp.where(place < half, 2 * place, 2 * (n - 1 - place) + 1)


def shift(x, axis, n, by):
    return lax.ppermute(x, axis, [(i, (i + by) % n) for i in range(n)])


def ring_gather(shards, n, forward_steps):
    order = snake(n)
    ahead = [(order[i], order[(i + 1) % n]) for i in range(n)]
    behind = [(b, a) for a, b in ahead]
    found = []
    for x, steps in zip(shards, forward_steps):
        forward, back = [x], [x]
        found.append((forward, back))
    for step in range(n):
        for (forward, back), steps in zip(found, forward_steps):
            if step < steps:
                forward.append(lax.ppermute(forward[-1], "fs", ahead))
            if step < n - 1 - steps:
                back.append(lax.ppermute(back[-1], "fs", behind))
    return [forward + back[:0:-1] for forward, back in found]


def chained(shards, before, hops):
    if not before:
        return shards
    last = []
    n = len(before[0])
    for pieces in before:
        last.extend([pieces[hops], pieces[n - hops]])
    return lax.optimization_barrier((tuple(shards), tuple(last)))[0]


def with_scale(weight, scale):
    high = lax.reduce_precision(scale, 8, 7)
    middle = lax.reduce_precision(scale - high, 8, 7)
    rows = jnp.stack([high, middle, scale - high - middle]).astype(jnp.bfloat16)
    return jnp.concatenate([weight, jnp.pad(rows, ((0, 13), (0, 0)))], axis=0)


def without_scale(pieces):
    size = pieces[0].shape[0] - 16
    weight = jnp.concatenate([p[:size] for p in pieces], axis=1)
    rows = jnp.concatenate([p[size:] for p in pieces], axis=1)[:3].astype(jnp.float32)
    return weight, rows[0] + rows[1] + rows[2]


def retain(query, key_rows, value, decay, head_gain):
    seq_len = query.shape[0]
    row = lax.broadcasted_iota(jnp.int32, (seq_len, seq_len), 0)
    col = lax.broadcasted_iota(jnp.int32, (seq_len, seq_len), 1)
    distance = jnp.abs(row - col).astype(jnp.float32)
    weight = jnp.where(col // BLOCK <= row // BLOCK, jnp.exp(-decay * distance), 0.0)
    scores = lax.dot_general(
        query, key_rows, (((1,), (1,)), ((), ())), preferred_element_type=jnp.float32
    )
    scores = (scores * weight).astype(jnp.bfloat16)
    retained = jnp.dot(scores, value, preferred_element_type=jnp.float32)
    centred = retained - jnp.mean(retained, axis=-1, keepdims=True)
    normed = (
        centred
        * lax.rsqrt(jnp.mean(centred * centred, axis=-1, keepdims=True) + EPSILON)
        * head_gain
    )
    return normed.astype(jnp.bfloat16)


def on_device(
    n_rep,
    n_fs,
    n_tp,
    tokens_in,
    norm_gains,
    gate_w,
    gate_scale,
    up_w,
    up_scale,
    down_w,
    down_scale,
    query_w,
    query_scale,
    key_w,
    key_scale,
    value_w,
    value_scale,
    out_w,
    out_scale,
    head_gain,
    decay_rate,
):
    rows = tokens_in.shape[0]
    width = gate_w.shape[0]
    heads = decay_rate.shape[0]
    units = gate_w.shape[1]
    share = n_rep if heads % n_rep == 0 and units % (n_rep * 128) == 0 else 1
    heads //= share
    units //= share
    rep = lax.axis_index("rep") if share > 1 else 0
    tp = lax.axis_index("tp")
    place = snake_place(lax.axis_index("fs"), n_fs)

    def part(x, axis):
        size = x.shape[axis] // share
        return lax.dynamic_slice_in_dim(x, rep * size, size, axis)

    gate_b, up_b, query_b, key_b, value_b = (
        part(w, 1).astype(jnp.bfloat16) for w in (gate_w, up_w, query_w, key_w, value_w)
    )
    down_b, out_b = (part(w, 0).astype(jnp.bfloat16) for w in (down_w, out_w))

    few, many = (n_fs - 1) // 2, n_fs // 2
    first_pieces = ring_gather([gate_b, up_b], n_fs, [many, few])
    half = down_b.shape[0] // 2
    second_pieces = ring_gather(
        chained([with_scale(down_b[:half], down_scale), down_b[half:]], first_pieces, max(1, n_fs // 4)),
        n_fs,
        [many, few],
    )
    third_pieces = ring_gather(chained([query_b, key_b], second_pieces, few), n_fs, [many, few])
    value_pieces, out_pieces = ring_gather(
        chained([value_b, with_scale(out_b, out_scale)], third_pieces, few), n_fs, [many, few]
    )

    gate_full, up_full = (jnp.concatenate(p, axis=0) for p in first_pieces)
    down_top, down_cols = without_scale(second_pieces[0])
    down_rest = jnp.concatenate(second_pieces[1], axis=1)
    down_full = lax.optimization_barrier(jnp.concatenate([down_top, down_rest], axis=0))
    query_full, key_full = (jnp.concatenate(p, axis=0) for p in third_pieces)
    value_full = jnp.concatenate(value_pieces, axis=0)
    out_full, out_cols = without_scale(out_pieces)

    def to_ring(x):
        blocks = [
            lax.dynamic_slice_in_dim(
                x, snake_index((place - k) % n_fs, n_fs) * width, width, axis=1
            )
            for k in range(n_fs)
        ]
        return jnp.concatenate(blocks, axis=1)

    def from_ring(x):
        blocks = [
            lax.dynamic_slice_in_dim(x, (place - snake(n_fs).index(o)) % n_fs * width, width, axis=1)
            for o in range(n_fs)
        ]
        return jnp.concatenate(blocks, axis=1)

    def over_tp(x, ordered):
        found = [x] + [shift(x, "tp", n_tp, k) for k in range(1, n_tp)]
        if not ordered:
            return jnp.concatenate(found, axis=0)
        twice = jnp.concatenate(found[::-1] * 2, axis=0)
        return lax.dynamic_slice_in_dim(twice, (n_tp - 1 - tp) * rows, n_tp * rows, axis=0)

    def gather_rows(normed, ordered=False):
        found = [normed] + [shift(normed, "rep", n_rep, k) for k in range(1, share)]
        return [over_tp(x, ordered) for x in found]

    def return_rows(parts, ordered=False):
        total = None
        for k in range(share - 1, -1, -1):

            def block(j):
                at = (tp - j) % n_tp * rows if ordered else j * rows
                return lax.dynamic_slice_in_dim(parts[k], at, rows, axis=0)

            mine = block(0)
            for j in range(1, n_tp):
                other = shift(block(j).astype(jnp.bfloat16), "tp", n_tp, n_tp - j)
                mine = mine + other.astype(jnp.float32)
            if k > 0:
                mine = shift(mine.astype(jnp.bfloat16), "rep", n_rep, n_rep - k).astype(jnp.float32)
            total = mine if total is None else total + mine
        return total

    def dot(a, b):
        return jnp.dot(a, b, preferred_element_type=jnp.float32)

    gate_col, up_col = part(gate_scale, 0), part(up_scale, 0)

    def feed_forward(stream, gain):
        parts = []
        for gathered in gather_rows(rms_scale(stream, gain).astype(jnp.bfloat16)):
            gate_value = dot(gathered, gate_full) * gate_col
            up_value = dot(gathered, up_full) * up_col
            hidden = (jax.nn.silu(gate_value) * up_value).astype(jnp.bfloat16)
            hidden = lax.optimization_barrier(hidden)
            parts.append(dot(hidden, down_full) * down_cols)
        return return_rows(parts)

    query_col, key_col, value_col = (part(s, 0) for s in (query_scale, key_scale, value_scale))
    decay = part(decay_rate, 0)
    gains = to_ring(norm_gains)

    stream = to_ring(tokens_in).astype(jnp.float32)
    stream = stream + 0.5 * feed_forward(stream, gains[0])
    parts = []
    for gathered in gather_rows(
        rms_scale(stream, gains[1]).astype(jnp.bfloat16), ordered=True
    ):
        query = (dot(gathered, query_full) * query_col).astype(jnp.bfloat16)
        key_rows = (dot(gathered, key_full) * key_col / math.sqrt(DK)).astype(jnp.bfloat16)
        value = (dot(gathered, value_full) * value_col).astype(jnp.bfloat16)
        mixed = [
            retain(
                query[:, h * DK : (h + 1) * DK],
                key_rows[:, h * DK : (h + 1) * DK],
                value[:, h * DV : (h + 1) * DV],
                decay[h],
                head_gain,
            )
            for h in range(heads)
        ]
        parts.append(dot(jnp.concatenate(mixed, axis=1), out_full) * out_cols)
    stream = stream + return_rows(parts, ordered=True)
    stream = stream + 0.5 * feed_forward(stream, gains[2])
    return from_ring(stream.astype(jnp.bfloat16))


MESH = pl.DeviceIdType.MESH
VMEM_LIMIT = 62 * 1024 * 1024


def fits(n_rep, n_fs, n_tp, tokens_in, norm_gains, gate_w, *rest):
    rows, features = tokens_in.shape
    width, units = gate_w.shape
    heads = rest[-1].shape[0]
    return (
        n_rep == 2
        and n_tp == 2
        and n_fs >= 4
        and n_fs % 2 == 0
        and rows % 128 == 0
        and width % 256 == 0
        and features == n_fs * width
        and units % (n_rep * 256) == 0
        and heads % n_rep == 0
    )


def layer_kernel(
    n,
    tokens_in,
    norm_gains,
    gate_w,
    gate_scale,
    up_w,
    up_scale,
    down_w,
    down_scale,
    query_w,
    query_scale,
    key_w,
    key_scale,
    value_w,
    value_scale,
    out_w,
    out_scale,
    head_gain,
    decay_rate,
    result,
    staged_in,
    staged_gate,
    staged_up,
    staged_down,
    staged_query,
    staged_key,
    staged_value,
    staged_out,
    gate_full,
    up_full,
    down_full,
    head_full,
    out_full,
    cols_full,
    gathered,
    factors,
    stream,
    squares,
    hidden,
    mixed,
    own_part,
    far_part,
    tp_out,
    tp_in,
    rep_out,
    rep_in,
    local_sem,
    ring_send,
    ring_recv,
    part_send,
    part_recv,
    row_send,
    row_recv,
    block_send,
    block_recv,
):
    f32, bf16 = jnp.float32, jnp.bfloat16
    rows, features = tokens_in.shape
    width = gate_w.shape[0]
    units = hidden.shape[1]
    heads = head_full.shape[0]
    tile = 256

    rep, fs, tp = (lax.axis_index(axis) for axis in ("rep", "fs", "tp"))
    odd = lax.rem(fs, 2)
    place = lax.div(fs, 2) * (1 - odd) + (n - 1 - lax.div(fs, 2)) * odd

    def at_place(offset):
        spot = lax.rem(place + offset + n, n)
        late = lax.div(spot, n // 2)
        return 2 * spot * (1 - late) + (2 * (n - 1 - spot) + 1) * late

    owner = [at_place(o) for o in range(n)]
    ahead, behind = {"fs": owner[1]}, {"fs": owner[n - 1]}
    tp_peer, rep_peer = {"tp": 1 - tp}, {"rep": 1 - rep}

    barrier = pltpu.get_barrier_semaphore()
    for peer in (ahead, behind, tp_peer, rep_peer):
        pl.semaphore_signal(barrier, inc=1, device_id=peer, device_id_type=MESH)

    def columns_of(f):
        return pl.ds(pl.multiple_of(f * width, width), width)

    unit_cols = pl.ds(pl.multiple_of(rep * units, 128), units)
    feature_cols = pl.ds(pl.multiple_of(rep * heads * DK, 128), heads * DK)
    value_cols = pl.ds(pl.multiple_of(rep * heads * DV, 128), heads * DV)
    local = [
        pltpu.make_async_copy(a, b, local_sem.at[i])
        for i, (a, b) in enumerate(
            [
                (gate_w.at[:, unit_cols], staged_gate),
                (up_w.at[:, unit_cols], staged_up),
                (tokens_in, staged_in),
                (down_w.at[unit_cols, :], staged_down),
                (query_w.at[:, feature_cols], staged_query),
                (key_w.at[:, feature_cols], staged_key),
                (value_w.at[:, value_cols], staged_value),
                (out_w.at[value_cols, :], staged_out),
            ]
        )
    ]
    for copy in local:
        copy.start()

    started = []
    few, many = (n - 1) // 2, n // 2

    def rows_of(f, size=width, first=0):
        return pl.ds(pl.multiple_of(f * width + first, size), size)

    half_units, half_width, half_out = units // 2, width // 2, heads * DV // 2
    pieces = [
        (lambda f: gate_full.at[rows_of(f), :], many),
        (lambda f: up_full.at[rows_of(f), :], few),
        (lambda f: down_full.at[f, pl.ds(0, half_units), :], many),
        (lambda f: down_full.at[f, pl.ds(half_units, half_units), :], few),
    ]
    rounds = [[0, 1], [2, 3]]
    for h in range(heads):
        rounds.append([len(pieces), len(pieces) + 1])
        pieces.append((lambda f, h=h: head_full.at[h, rows_of(f, half_width), :], many))
        pieces.append(
            (lambda f, h=h: head_full.at[h, rows_of(f, half_width, half_width), :], few)
        )
    rounds.append([len(pieces), len(pieces) + 1])
    pieces.append((lambda f: out_full.at[f, pl.ds(0, half_out), :], many))
    pieces.append((lambda f: out_full.at[f, pl.ds(half_out, half_out), :], few))
    scales = len(pieces)
    pieces.append((lambda f: cols_full.at[f], many))

    def hop_copy(kind, forward, hop):
        piece, hops = pieces[kind]
        source = owner[(1 - hop) % n if forward else (hop - 1) % n]
        sem = kind * (n - 1) + hop - 1 + (0 if forward else hops)
        return pltpu.make_async_remote_copy(
            src_ref=piece(source),
            dst_ref=piece(source),
            send_sem=ring_send.at[sem],
            recv_sem=ring_recv.at[sem],
            device_id=ahead if forward else behind,
            device_id_type=MESH,
        )

    def arrival(kind, forward, hop):
        piece, hops = pieces[kind]
        source = owner[-hop % n if forward else hop % n]
        sem = kind * (n - 1) + hop - 1 + (0 if forward else hops)
        return pltpu.make_async_remote_copy(
            src_ref=piece(source),
            dst_ref=piece(source),
            send_sem=ring_send.at[sem],
            recv_sem=ring_recv.at[sem],
            device_id=ahead if forward else behind,
            device_id_type=MESH,
        )

    arrived = set()

    def need(kind, forward, hop):
        if hop > 0 and (kind, forward, hop) not in arrived:
            arrived.add((kind, forward, hop))
            arrival(kind, forward, hop).wait_recv()

    def hops_of(kind, forward):
        return pieces[kind][1] if forward else n - 1 - pieces[kind][1]

    def need_piece(kind, offset):
        if offset > 0:
            if offset <= hops_of(kind, False):
                need(kind, False, offset)
            else:
                need(kind, True, n - offset)

    queue = []
    for index, kinds in enumerate(rounds):
        for hop in range(1, many + 1):
            for i in range(2):
                batch = []
                for forward, kind in ((True, kinds[i]), (False, kinds[1 - i])):
                    if hop <= hops_of(kind, forward):
                        batch.append((kind, forward, hop))
                if index == 1 and i == 0:
                    for forward in (True, False):
                        if hop <= hops_of(scales, forward):
                            batch.append((scales, forward, hop))
                if batch:
                    queue.append(batch)

    def pump(count):
        for _ in range(count):
            for kind, forward, hop in queue.pop(0):
                need(kind, forward, hop - 1)
                copy = hop_copy(kind, forward, hop)
                copy.start()
                started.append(copy)

    def send(src, dst, send_sem, recv_sem, peer):
        copy = pltpu.make_async_remote_copy(
            src_ref=src,
            dst_ref=dst,
            send_sem=send_sem,
            recv_sem=recv_sem,
            device_id=peer,
            device_id_type=MESH,
        )
        copy.start()
        started.append(copy)
        return copy

    me = owner[0]
    own_rows = rows_of(me)
    local[0].wait()
    gate_full[own_rows, :] = staged_gate[...].astype(bf16)
    local[1].wait()
    up_full[own_rows, :] = staged_up[...].astype(bf16)
    pl.semaphore_wait(barrier, 4)
    pump(2)

    local[2].wait()

    def norm_rows(source, which, target):
        gain = norm_gains[which : which + 1, :]

        def step(i, carry):
            block = pl.ds(pl.multiple_of(i * 16, 16), 16)
            x = source[block, :].astype(f32)
            mean = jnp.mean(x * x, axis=-1, keepdims=True)
            target[block, :] = (x * lax.rsqrt(mean + EPSILON) * gain).astype(bf16)
            return carry

        lax.fori_loop(0, rows // 16, step, 0)

    def slot(j, cols=slice(None)):
        return (pl.ds(j * rows, rows), cols)

    def share_rows(stage):
        part = gathered.at[stage]
        base = 3 * stage
        send(part.at[slot(0)], part.at[slot(1)], row_send.at[base], row_recv.at[base], tp_peer)
        send(
            part.at[slot(0)],
            part.at[slot(2)],
            row_send.at[base + 1],
            row_recv.at[base + 1],
            rep_peer,
        )

    def wait_rows(stage, i, j):
        part = gathered.at[stage]
        pltpu.make_async_remote_copy(
            src_ref=part.at[slot(0)],
            dst_ref=part.at[slot(j)],
            send_sem=row_send.at[3 * stage + i],
            recv_sem=row_recv.at[3 * stage + i],
            device_id=tp_peer,
            device_id_type=MESH,
        ).wait_recv()

    def relay_rows(stage):
        wait_rows(stage, 1, 2)
        part = gathered.at[stage]
        send(
            part.at[slot(2)],
            part.at[slot(3)],
            row_send.at[3 * stage + 2],
            row_recv.at[3 * stage + 2],
            tp_peer,
        )

    norm_rows(staged_in, 0, gathered.at[0])
    stream[...] = staged_in[...].astype(f32)
    share_rows(0)

    local[3].wait()
    down_full[me] = staged_down[...].astype(bf16)
    cols_full[me, 0:1, :] = down_scale[...]
    cols_full[me, 1:2, :] = out_scale[...]
    for i in (4, 5, 6):
        local[i].wait()
    for h in range(heads):
        keys, vals = slice(h * DK, (h + 1) * DK), slice(h * DV, (h + 1) * DV)
        head_full[h, own_rows, 0:DK] = staged_query[:, keys].astype(bf16)
        head_full[h, own_rows, DK : 2 * DK] = staged_key[:, keys].astype(bf16)
        head_full[h, own_rows, 2 * DK :] = staged_value[:, vals].astype(bf16)
    local[7].wait()
    out_full[me] = staged_out[...].astype(bf16)

    pump(2)
    relay_rows(0)
    pump(5)
    wait_rows(0, 0, 1)
    wait_rows(0, 2, 3)

    def dot(a, b):
        return jnp.dot(a, b, preferred_element_type=f32)

    def expand(stage, factor, count, hooks):
        for c in range(units // tile):
            cols = slice(c * tile, (c + 1) * tile)
            span = pl.ds(pl.multiple_of(rep * units + c * tile, 128), tile)
            gate = dot(gathered[stage], gate_full[:, cols])
            up = dot(gathered[stage], up_full[:, cols])
            if factor is not None:
                gate, up = gate * factor, up * factor
            gate, up = gate * gate_scale[:, span], up * up_scale[:, span]
            hidden[:, cols] = (gate / (1.0 + jnp.exp(-gate)) * up).astype(bf16)
            if c in hooks:
                pump(hooks[c])

    offsets = [0]
    for hop in range(1, many + 1):
        for o in (n - hop, hop):
            if o not in offsets:
                offsets.append(o)

    def part_of(stage, k, through, i, j):
        store_out, store_in = (tp_out, tp_in) if through == "tp" else (rep_out, rep_in)
        sem = (stage * n + k) * 2 + (0 if through == "tp" else 1)
        return pltpu.make_async_remote_copy(
            src_ref=store_out.at[stage, k],
            dst_ref=store_in.at[stage, k],
            send_sem=part_send.at[sem],
            recv_sem=part_recv.at[sem],
            device_id=tp_peer if through == "tp" else rep_peer,
            device_id_type=MESH,
        )

    def contract(stage, lhs, weight, row, kinds, hooks, finish, relay=None):
        def multiply(k):
            o = offsets[k]
            for kind in kinds:
                need_piece(kind, o)
            need_piece(scales, o)
            f = owner[o]
            part = dot(lhs[...], weight[f]) * cols_full[f, row : row + 1, :]
            own_part[k] = part[:rows]
            far_part[k] = part[2 * rows : 3 * rows]
            tp_out[stage, k, 0] = part[rows : 2 * rows].astype(bf16)
            tp_out[stage, k, 1] = part[3 * rows :].astype(bf16)
            copy = part_of(stage, k, "tp", 0, 0)
            copy.start()
            started.append(copy)

        def pass_on(k):
            part_of(stage, k, "tp", 0, 0).wait_recv()
            rep_out[stage, k] = (far_part[k] + tp_in[stage, k, 1].astype(f32)).astype(bf16)
            copy = part_of(stage, k, "rep", 0, 0)
            copy.start()
            started.append(copy)

        def collect(k):
            part_of(stage, k, "rep", 0, 0).wait_recv()
            total = own_part[k] + tp_in[stage, k, 0].astype(f32) + rep_in[stage, k].astype(f32)
            finish(k, owner[offsets[k]], total)

        lags = [(multiply, 0), (pass_on, 1), (collect, 3)]
        if relay is not None:
            lags.append((relay, 5))
        for step in range(n + lags[-1][1]):
            if step in hooks:
                pump(hooks[step])
            for action, lag in lags:
                if 0 <= step - lag < n:
                    action(step - lag)

    for kind in rounds[0]:
        for o in range(1, n):
            need_piece(kind, o)
    expand(0, None, 1, {1: 1, 2: 1})

    def add_half(k, f, total):
        cols = columns_of(f)
        stream[:, cols] = stream[:, cols] + 0.5 * total

    contract(0, hidden, down_full, 0, rounds[1], {3: 2, 5: 3}, add_half)

    norm_rows(stream, 1, gathered.at[1])
    share_rows(1)
    pump(4)
    relay_rows(1)
    pump(1)

    seq_len = 2 * rows
    row = lax.rem(
        lax.broadcasted_iota(jnp.int32, (seq_len, seq_len), 0) + tp * rows, seq_len
    )
    col = lax.rem(
        lax.broadcasted_iota(jnp.int32, (seq_len, seq_len), 1) + tp * rows, seq_len
    )

    def retain(h, hooks):
        places = [
            (query_scale, 0, DK, 1.0),
            (key_scale, DK, DK, 1.0 / math.sqrt(DK)),
            (value_scale, 2 * DK, DV, 1.0),
        ]
        made = []
        for i, (scale, first, size, factor) in enumerate(places):
            span = pl.ds(pl.multiple_of((rep * heads + h) * size, 128), size)
            product = dot(gathered[1], head_full[h, :, first : first + size])
            made.append((product * (scale[:, span] * factor)).astype(bf16))
            if i in hooks:
                pump(hooks[i])
        query, keys, values = made
        decay = decay_rate[rep * heads + h]
        distance = jnp.abs(row - col).astype(f32)
        weight = jnp.where(
            lax.div(col, BLOCK) <= lax.div(row, BLOCK), jnp.exp(-decay * distance), 0.0
        )
        for s in range(2):
            span = slice(s * seq_len, (s + 1) * seq_len)
            scores = lax.dot_general(
                query[span], keys[span], (((1,), (1,)), ((), ())), preferred_element_type=f32
            )
            scores = (scores * weight).astype(bf16)
            retained = dot(scores, values[span])
            centred = retained - jnp.mean(retained, axis=-1, keepdims=True)
            spread = jnp.mean(centred * centred, axis=-1, keepdims=True)
            mixed[span, h * DV : (h + 1) * DV] = (
                centred * lax.rsqrt(spread + EPSILON) * head_gain[...]
            ).astype(bf16)

    for h in range(heads):
        pump(2)
        if h == 0:
            wait_rows(1, 0, 1)
            wait_rows(1, 2, 3)
        for kind in rounds[2 + h]:
            for o in range(1, n):
                need_piece(kind, o)
        retain(h, {1: 1})
        if h < heads - 1:
            pump(4)

    last = gathered.at[2]

    def block_copy(k, i, start):
        cols = columns_of(owner[offsets[k]])
        a, b, peer = ((0, 1, tp_peer), (0, 2, rep_peer), (2, 3, tp_peer))[i]
        return pltpu.make_async_remote_copy(
            src_ref=last.at[slot(a, cols)],
            dst_ref=last.at[slot(b, cols)],
            send_sem=block_send.at[3 * k + i],
            recv_sem=block_recv.at[3 * k + i],
            device_id=peer,
            device_id_type=MESH,
        )

    def factor_copy(i):
        a, b, peer = ((0, 1, tp_peer), (0, 2, rep_peer), (2, 3, tp_peer))[i]
        return pltpu.make_async_remote_copy(
            src_ref=factors.at[a],
            dst_ref=factors.at[b],
            send_sem=block_send.at[3 * n + i],
            recv_sem=block_recv.at[3 * n + i],
            device_id=peer,
            device_id_type=MESH,
        )

    squares[...] = jnp.zeros_like(squares)

    def add_mix(k, f, total):
        cols = columns_of(f)
        second = stream[:, cols] + total
        stream[:, cols] = second
        last[slot(0, cols)] = (second * norm_gains[2:3, cols]).astype(bf16)
        square = second * second
        added = squares[...]
        for i in range(width // 128):
            added = added + square[:, i * 128 : (i + 1) * 128]
        squares[...] = added
        for i in (0, 1):
            copy = block_copy(k, i, True)
            copy.start()
            started.append(copy)
        if k == n - 1:
            mean = jnp.sum(added, axis=-1, keepdims=True) / features
            wide = jnp.broadcast_to(lax.rsqrt(mean + EPSILON), (rows, rows))
            factors[0] = wide.T[:8, :]
            for i in (0, 1):
                copy = factor_copy(i)
                copy.start()
                started.append(copy)

    def relay_block(k):
        block_copy(k, 1, False).wait_recv()
        copy = block_copy(k, 2, True)
        copy.start()
        started.append(copy)
        if k == n - 1:
            factor_copy(1).wait_recv()
            copy = factor_copy(2)
            copy.start()
            started.append(copy)

    contract(1, mixed, out_full, 1, rounds[-1], {1: 1, 3: 2, 5: 1}, add_mix, relay_block)
    for k in range(n):
        block_copy(k, 0, False).wait_recv()
        block_copy(k, 2, False).wait_recv()
    factor_copy(0).wait_recv()
    factor_copy(2).wait_recv()
    factor = jnp.concatenate(
        [jnp.broadcast_to(factors[j, 0:1, :], (rows, rows)).T[:, 0:1] for j in range(4)], axis=0
    )
    expand(2, factor, 1, {})

    def write(k, f, total):
        cols = columns_of(f)
        result[:, cols] = (stream[:, cols] + 0.5 * total).astype(bf16)

    contract(2, hidden, down_full, 0, rounds[1], {}, write)
    assert not queue
    for copy in started:
        copy.wait_send()


def fused(
    n_rep,
    n_fs,
    n_tp,
    tokens_in,
    norm_gains,
    gate_w,
    gate_scale,
    up_w,
    up_scale,
    down_w,
    down_scale,
    query_w,
    query_scale,
    key_w,
    key_scale,
    value_w,
    value_scale,
    out_w,
    out_scale,
    head_gain,
    decay_rate,
):
    f32, bf16 = jnp.float32, jnp.bfloat16
    n = n_fs
    rows, features = tokens_in.shape
    width, units = gate_w.shape[0], gate_w.shape[1] // n_rep
    heads = decay_rate.shape[0] // n_rep
    kinds = 4 + 2 * heads + 2 + 1
    any_space = pl.BlockSpec(memory_space=pl.ANY)
    vmem = pl.BlockSpec(memory_space=pltpu.VMEM)
    smem = pl.BlockSpec(memory_space=pltpu.SMEM)
    dma = pltpu.SemaphoreType.DMA

    def wide(x):
        return x.reshape(1, -1)

    return pl.pallas_call(
        functools.partial(layer_kernel, n),
        out_shape=jax.ShapeDtypeStruct((rows, features), bf16),
        in_specs=[any_space, vmem]
        + [any_space, vmem] * 7
        + [vmem, smem],
        out_specs=vmem,
        scratch_shapes=[
            pltpu.VMEM((rows, features), bf16),
            pltpu.VMEM((width, units), f32),
            pltpu.VMEM((width, units), f32),
            pltpu.VMEM((units, width), f32),
            pltpu.VMEM((width, heads * DK), f32),
            pltpu.VMEM((width, heads * DK), f32),
            pltpu.VMEM((width, heads * DV), f32),
            pltpu.VMEM((heads * DV, width), f32),
            pltpu.VMEM((features, units), bf16),
            pltpu.VMEM((features, units), bf16),
            pltpu.VMEM((n, units, width), bf16),
            pltpu.VMEM((heads, features, 2 * DK + DV), bf16),
            pltpu.VMEM((n, heads * DV, width), bf16),
            pltpu.VMEM((n, 8, width), f32),
            pltpu.VMEM((3, 4 * rows, features), bf16),
            pltpu.VMEM((4, 8, rows), f32),
            pltpu.VMEM((rows, features), f32),
            pltpu.VMEM((rows, 128), f32),
            pltpu.VMEM((4 * rows, units), bf16),
            pltpu.VMEM((4 * rows, heads * DV), bf16),
            pltpu.VMEM((n, rows, width), f32),
            pltpu.VMEM((n, rows, width), f32),
            pltpu.VMEM((3, n, 2, rows, width), bf16),
            pltpu.VMEM((3, n, 2, rows, width), bf16),
            pltpu.VMEM((3, n, rows, width), bf16),
            pltpu.VMEM((3, n, rows, width), bf16),
            dma((8,)),
            dma((kinds * (n - 1),)),
            dma((kinds * (n - 1),)),
            dma((3 * n * 2,)),
            dma((3 * n * 2,)),
            dma((6,)),
            dma((6,)),
            dma((3 * n + 3,)),
            dma((3 * n + 3,)),
        ],
        compiler_params=pltpu.CompilerParams(
            collective_id=0, has_side_effects=True, vmem_limit_bytes=VMEM_LIMIT
        ),
        name="layer",
    )(
        tokens_in,
        norm_gains,
        gate_w,
        wide(gate_scale),
        up_w,
        wide(up_scale),
        down_w,
        wide(down_scale),
        query_w,
        wide(query_scale),
        key_w,
        wide(key_scale),
        value_w,
        wide(value_scale),
        out_w,
        wide(out_scale),
        wide(head_gain),
        decay_rate,
    )


def solution(mesh):
    sizes = [mesh.shape[axis] for axis in ("rep", "fs", "tp")]
    placed = (
        P(("rep", "fs", "tp"), None),
        P(),
        P("fs", "tp"),
        P("tp"),
        P("fs", "tp"),
        P("tp"),
        P("tp", "fs"),
        P("fs"),
        P("fs", "tp"),
        P("tp"),
        P("fs", "tp"),
        P("tp"),
        P("fs", "tp"),
        P("tp"),
        P("tp", "fs"),
        P("fs"),
        P(),
        P("tp"),
    )
    return jax.shard_map(
        lambda *args: (fused if fits(*sizes, *args) else on_device)(*sizes, *args),
        mesh=mesh,
        in_specs=placed,
        out_specs=P(("rep", "fs", "tp"), None),
        check_vma=False,
    )
```

```python
import functools
import math

import jax
import jax.numpy as jnp
from jax import lax
from jax.experimental import pallas as pl
from jax.experimental.pallas import tpu as pltpu
from jax.sharding import PartitionSpec as P

DK = 256
DV = 256
BLOCK = 64

EPSILON = 1e-05


def rms_scale(stream, gain):
    return stream * lax.rsqrt(jnp.mean(stream * stream, axis=-1, keepdims=True) + EPSILON) * gain


def snake(n):
    return [i for i in range(0, n, 2)] + [i for i in range(n - 1, 0, -1) if i % 2 == 1]


def snake_place(index, n):
    return jnp.where(index % 2 == 0, index // 2, n - 1 - index // 2)


def snake_index(place, n):
    half = (n + 1) // 2
    return jnp.where(place < half, 2 * place, 2 * (n - 1 - place) + 1)


def shift(x, axis, n, by):
    return lax.ppermute(x, axis, [(i, (i + by) % n) for i in range(n)])


def ring_gather(shards, n, forward_steps):
    order = snake(n)
    ahead = [(order[i], order[(i + 1) % n]) for i in range(n)]
    behind = [(b, a) for a, b in ahead]
    found = []
    for x, steps in zip(shards, forward_steps):
        forward, back = [x], [x]
        found.append((forward, back))
    for step in range(n):
        for (forward, back), steps in zip(found, forward_steps):
            if step < steps:
                forward.append(lax.ppermute(forward[-1], "fs", ahead))
            if step < n - 1 - steps:
                back.append(lax.ppermute(back[-1], "fs", behind))
    return [forward + back[:0:-1] for forward, back in found]


def chained(shards, before, hops):
    if not before:
        return shards
    last = []
    n = len(before[0])
    for pieces in before:
        last.extend([pieces[hops], pieces[n - hops]])
    return lax.optimization_barrier((tuple(shards), tuple(last)))[0]


def with_scale(weight, scale):
    high = lax.reduce_precision(scale, 8, 7)
    middle = lax.reduce_precision(scale - high, 8, 7)
    rows = jnp.stack([high, middle, scale - high - middle]).astype(jnp.bfloat16)
    return jnp.concatenate([weight, jnp.pad(rows, ((0, 13), (0, 0)))], axis=0)


def without_scale(pieces):
    size = pieces[0].shape[0] - 16
    weight = jnp.concatenate([p[:size] for p in pieces], axis=1)
    rows = jnp.concatenate([p[size:] for p in pieces], axis=1)[:3].astype(jnp.float32)
    return weight, rows[0] + rows[1] + rows[2]


def retain(query, key_rows, value, decay, head_gain):
    seq_len = query.shape[0]
    row = lax.broadcasted_iota(jnp.int32, (seq_len, seq_len), 0)
    col = lax.broadcasted_iota(jnp.int32, (seq_len, seq_len), 1)
    distance = jnp.abs(row - col).astype(jnp.float32)
    weight = jnp.where(col // BLOCK <= row // BLOCK, jnp.exp(-decay * distance), 0.0)
    scores = lax.dot_general(
        query, key_rows, (((1,), (1,)), ((), ())), preferred_element_type=jnp.float32
    )
    scores = (scores * weight).astype(jnp.bfloat16)
    retained = jnp.dot(scores, value, preferred_element_type=jnp.float32)
    centred = retained - jnp.mean(retained, axis=-1, keepdims=True)
    normed = (
        centred
        * lax.rsqrt(jnp.mean(centred * centred, axis=-1, keepdims=True) + EPSILON)
        * head_gain
    )
    return normed.astype(jnp.bfloat16)


def on_device(
    n_rep,
    n_fs,
    n_tp,
    tokens_in,
    norm_gains,
    gate_w,
    gate_scale,
    up_w,
    up_scale,
    down_w,
    down_scale,
    query_w,
    query_scale,
    key_w,
    key_scale,
    value_w,
    value_scale,
    out_w,
    out_scale,
    head_gain,
    decay_rate,
):
    rows = tokens_in.shape[0]
    width = gate_w.shape[0]
    heads = decay_rate.shape[0]
    units = gate_w.shape[1]
    share = n_rep if heads % n_rep == 0 and units % (n_rep * 128) == 0 else 1
    heads //= share
    units //= share
    rep = lax.axis_index("rep") if share > 1 else 0
    tp = lax.axis_index("tp")
    place = snake_place(lax.axis_index("fs"), n_fs)

    def part(x, axis):
        size = x.shape[axis] // share
        return lax.dynamic_slice_in_dim(x, rep * size, size, axis)

    gate_b, up_b, query_b, key_b, value_b = (
        part(w, 1).astype(jnp.bfloat16) for w in (gate_w, up_w, query_w, key_w, value_w)
    )
    down_b, out_b = (part(w, 0).astype(jnp.bfloat16) for w in (down_w, out_w))

    few, many = (n_fs - 1) // 2, n_fs // 2
    first_pieces = ring_gather([gate_b, up_b], n_fs, [many, few])
    half = down_b.shape[0] // 2
    second_pieces = ring_gather(
        chained([with_scale(down_b[:half], down_scale), down_b[half:]], first_pieces, max(1, n_fs // 4)),
        n_fs,
        [many, few],
    )
    third_pieces = ring_gather(chained([query_b, key_b], second_pieces, few), n_fs, [many, few])
    value_pieces, out_pieces = ring_gather(
        chained([value_b, with_scale(out_b, out_scale)], third_pieces, few), n_fs, [many, few]
    )

    gate_full, up_full = (jnp.concatenate(p, axis=0) for p in first_pieces)
    down_top, down_cols = without_scale(second_pieces[0])
    down_rest = jnp.concatenate(second_pieces[1], axis=1)
    down_full = lax.optimization_barrier(jnp.concatenate([down_top, down_rest], axis=0))
    query_full, key_full = (jnp.concatenate(p, axis=0) for p in third_pieces)
    value_full = jnp.concatenate(value_pieces, axis=0)
    out_full, out_cols = without_scale(out_pieces)

    def to_ring(x):
        blocks = [
            lax.dynamic_slice_in_dim(
                x, snake_index((place - k) % n_fs, n_fs) * width, width, axis=1
            )
            for k in range(n_fs)
        ]
        return jnp.concatenate(blocks, axis=1)

    def from_ring(x):
        blocks = [
            lax.dynamic_slice_in_dim(x, (place - snake(n_fs).index(o)) % n_fs * width, width, axis=1)
            for o in range(n_fs)
        ]
        return jnp.concatenate(blocks, axis=1)

    def over_tp(x, ordered):
        found = [x] + [shift(x, "tp", n_tp, k) for k in range(1, n_tp)]
        if not ordered:
            return jnp.concatenate(found, axis=0)
        twice = jnp.concatenate(found[::-1] * 2, axis=0)
        return lax.dynamic_slice_in_dim(twice, (n_tp - 1 - tp) * rows, n_tp * rows, axis=0)

    def gather_rows(normed, ordered=False):
        found = [normed] + [shift(normed, "rep", n_rep, k) for k in range(1, share)]
        return [over_tp(x, ordered) for x in found]

    def return_rows(parts, ordered=False):
        total = None
        for k in range(share - 1, -1, -1):

            def block(j):
                at = (tp - j) % n_tp * rows if ordered else j * rows
                return lax.dynamic_slice_in_dim(parts[k], at, rows, axis=0)

            mine = block(0)
            for j in range(1, n_tp):
                other = shift(block(j).astype(jnp.bfloat16), "tp", n_tp, n_tp - j)
                mine = mine + other.astype(jnp.float32)
            if k > 0:
                mine = shift(mine.astype(jnp.bfloat16), "rep", n_rep, n_rep - k).astype(jnp.float32)
            total = mine if total is None else total + mine
        return total

    def dot(a, b):
        return jnp.dot(a, b, preferred_element_type=jnp.float32)

    gate_col, up_col = part(gate_scale, 0), part(up_scale, 0)

    def feed_forward(stream, gain):
        parts = []
        for gathered in gather_rows(rms_scale(stream, gain).astype(jnp.bfloat16)):
            gate_value = dot(gathered, gate_full) * gate_col
            up_value = dot(gathered, up_full) * up_col
            hidden = (jax.nn.silu(gate_value) * up_value).astype(jnp.bfloat16)
            hidden = lax.optimization_barrier(hidden)
            parts.append(dot(hidden, down_full) * down_cols)
        return return_rows(parts)

    query_col, key_col, value_col = (part(s, 0) for s in (query_scale, key_scale, value_scale))
    decay = part(decay_rate, 0)
    gains = to_ring(norm_gains)

    stream = to_ring(tokens_in).astype(jnp.float32)
    stream = stream + 0.5 * feed_forward(stream, gains[0])
    parts = []
    for gathered in gather_rows(
        rms_scale(stream, gains[1]).astype(jnp.bfloat16), ordered=True
    ):
        query = (dot(gathered, query_full) * query_col).astype(jnp.bfloat16)
        key_rows = (dot(gathered, key_full) * key_col / math.sqrt(DK)).astype(jnp.bfloat16)
        value = (dot(gathered, value_full) * value_col).astype(jnp.bfloat16)
        mixed = [
            retain(
                query[:, h * DK : (h + 1) * DK],
                key_rows[:, h * DK : (h + 1) * DK],
                value[:, h * DV : (h + 1) * DV],
                decay[h],
                head_gain,
            )
            for h in range(heads)
        ]
        parts.append(dot(jnp.concatenate(mixed, axis=1), out_full) * out_cols)
    stream = stream + return_rows(parts, ordered=True)
    stream = stream + 0.5 * feed_forward(stream, gains[2])
    return from_ring(stream.astype(jnp.bfloat16))


MESH = pl.DeviceIdType.MESH
VMEM_LIMIT = 62 * 1024 * 1024


def fits(n_rep, n_fs, n_tp, tokens_in, norm_gains, gate_w, *rest):
    rows, features = tokens_in.shape
    width, units = gate_w.shape
    heads = rest[-1].shape[0]
    return (
        n_rep == 2
        and n_tp == 2
        and n_fs >= 6
        and n_fs % 2 == 0
        and n_fs <= 16
        and rows % 128 == 0
        and width % 256 == 0
        and features == n_fs * width
        and units % 512 == 0
        and heads % 2 == 0
    )


def layer_kernel(
    n,
    tokens_in,
    norm_gains_in,
    gate_w,
    gate_scale_in,
    up_w,
    up_scale_in,
    down_w,
    down_scale_in,
    query_w,
    query_scale_in,
    key_w,
    key_scale_in,
    value_w,
    value_scale_in,
    out_w,
    out_scale_in,
    head_gain_in,
    decay_rate,
    result,
    norm_gains,
    gate_scale,
    up_scale,
    down_scale,
    query_scale,
    key_scale,
    value_scale,
    out_scale,
    head_gain,
    staged_in,
    staged_gate,
    staged_up,
    staged_down,
    staged_query,
    staged_key,
    staged_value,
    staged_out,
    gate_away,
    up_away,
    down_away,
    head_away,
    out_away,
    cols_away,
    gate_full,
    up_full,
    down_full,
    head_full,
    out_full,
    cols_full,
    gathered,
    factors,
    stream,
    squares,
    hidden,
    mixed,
    own_part,
    far_part,
    tp_out,
    tp_in,
    rep_out,
    rep_in,
    local_sem,
    side_send,
    side_recv,
    line_send,
    line_recv,
    twin_recv,
    part_send,
    part_recv,
    row_send,
    row_recv,
    block_send,
    block_recv,
):
    f32, bf16 = jnp.float32, jnp.bfloat16
    rows, features = tokens_in.shape
    width = gate_w.shape[0]
    units = hidden.shape[1]
    heads = head_full.shape[0]
    tile = 256

    twin, fs, tp = (lax.axis_index(axis) for axis in ("rep", "fs", "tp"))
    line = n // 2
    side, spot = lax.rem(fs, 2), lax.div(fs, 2)
    above, below = {"fs": fs + 2}, {"fs": fs - 2}
    side_peer, twin_peer, tp_peer = {"fs": fs + 1 - 2 * side}, {"rep": 1 - twin}, {"tp": 1 - tp}
    has_above, has_below = spot + 1 < line, spot > 0

    barrier = pltpu.get_barrier_semaphore()

    def greet(peer):
        pl.semaphore_signal(barrier, inc=1, device_id=peer, device_id_type=MESH)

    def meet():
        for peer in (side_peer, twin_peer, tp_peer):
            greet(peer)
        pl.when(has_above)(lambda: greet(above))
        pl.when(has_below)(lambda: greet(below))

    meet()

    def columns_of(f):
        return pl.ds(pl.multiple_of(f * width, width), width)

    def halves(size):
        return [pl.ds(pl.multiple_of(i * size, 128), size) for i in (side, 1 - side)]

    local, copies_of = [], {}

    def fetch(name, src, dst):
        copy = pltpu.make_async_copy(src, dst, local_sem.at[len(local)])
        copy.start()
        copies_of.setdefault(name, []).append(copy)
        local.append(copy)

    def fetched(name):
        for copy in copies_of[name]:
            copy.wait()

    for i, cols in enumerate(halves(units)):
        fetch(("gate", i), gate_w.at[:, cols], staged_gate.at[i])
    for i, cols in enumerate(halves(units)):
        fetch(("up", i), up_w.at[:, cols], staged_up.at[i])
    fetch("rows", tokens_in, staged_in)
    for src, dst in (
        (gate_scale_in, gate_scale),
        (up_scale_in, up_scale),
        (down_scale_in, down_scale),
        (query_scale_in, query_scale),
        (key_scale_in, key_scale),
        (value_scale_in, value_scale),
        (out_scale_in, out_scale),
        (head_gain_in, head_gain),
    ):
        fetch("small", src, dst.at[0])
    fetch("small", norm_gains_in, norm_gains)
    for i, cols in enumerate(halves(units)):
        fetch("down", down_w.at[cols, :], staged_down.at[i])
    for i, cols in enumerate(halves(heads * DK)):
        fetch("heads", query_w.at[:, cols], staged_query.at[i])
        fetch("heads", key_w.at[:, cols], staged_key.at[i])
    for i, cols in enumerate(halves(heads * DV)):
        fetch("heads", value_w.at[:, cols], staged_value.at[i])
        fetch("out", out_w.at[cols, :], staged_out.at[i])

    started = []
    half_units, half_width, half_out = units // 2, width // 2, heads * DV // 2

    def rows_of(f):
        return pl.ds(pl.multiple_of(f * width, width), width)

    def cut(ref, s, size):
        return ref.at[pl.ds(pl.multiple_of(s * size, size), size), :]

    kinds = [
        (lambda f: gate_full.at[rows_of(f), :], gate_away, half_width),
        (lambda f: up_full.at[rows_of(f), :], up_away, half_width),
        (lambda f: down_full.at[f], down_away, half_units),
    ]
    for h in range(heads):
        kinds.append(
            (lambda f, h=h: head_full.at[h, rows_of(f), :], head_away.at[h], half_width)
        )
    kinds.append((lambda f: out_full.at[f], out_away, half_out))
    scales = len(kinds)
    kinds.append((lambda f: cols_full.at[f], cols_away, 8))
    up_kind, down_kind, out_kind = 1, 2, scales - 1

    def piece(kind, f, s):
        return cut(kinds[kind][0](f), s, kinds[kind][2])

    def remote(src, dst, send_sem, recv_sem, peer):
        return pltpu.make_async_remote_copy(
            src_ref=src,
            dst_ref=dst,
            send_sem=send_sem,
            recv_sem=recv_sem,
            device_id=peer,
            device_id_type=MESH,
        )

    def across(o):
        return spot * 2 + side + o * (1 - 2 * side)

    def side_slot(kind, i):
        return kind * 2 + i if kind <= up_kind else kind + 2

    def side_copy(kind, i, f):
        slot_of = side_slot(kind, i)
        sems = side_send.at[slot_of], side_recv.at[slot_of]
        if kind <= up_kind:
            s = twin if i == 0 else 1 - twin
            return remote(
                cut(kinds[kind][1], s, kinds[kind][2]), piece(kind, f, s), *sems, side_peer
            )
        return remote(kinds[kind][1], kinds[kind][0](f), *sems, side_peer)

    def side_send_all(kind):
        for i in range(2 if kind <= up_kind else 1):
            copy = side_copy(kind, i, fs)
            copy.start()
            started.append(copy)

    side_done = set()

    def side_need(kind, i):
        i = i if kind <= up_kind else 0
        if (kind, i) not in side_done:
            side_done.add((kind, i))
            side_copy(kind, i, across(1)).wait_recv()

    span_of = 2 * (line - 1)
    sending = {}

    def push(kind, group, index, f, where, recv, peer):
        bank = 2 if kind == scales else kind % 2
        slot_of = (bank * 3 + group) * span_of + index
        copy = remote(piece(kind, f, twin), piece(kind, f, twin), line_send.at[slot_of], recv, peer)
        if slot_of in sending:
            sending.pop(slot_of)()
        guard = functools.partial(pl.when, where) if where is not None else None

        def begin():
            copy.start()

        def finish():
            copy.wait_send()

        if guard is None:
            begin()
            sending[slot_of] = finish
        else:
            guard()(begin)
            sending[slot_of] = lambda: guard()(finish)

    def line_slot(kind, away, o):
        return line_recv.at[kind * span_of + (away % line - 1) * 2 + o]

    def twin_slot(kind, away, o):
        return twin_recv.at[kind * span_of + (away - 1) * 2 + o]

    def send_own(kind, o):
        if o == 1:
            side_need(kind, 0)
        f = across(o)
        push(kind, 0, o, f, has_above, line_slot(kind, -1, o), above)
        push(kind, 1, o, f, has_below, line_slot(kind, 1, o), below)

    def pass_along(kind, d, o):
        for group, away in ((0, -d), (1, d)):
            from_spot = spot + away
            exists = from_spot >= 0 if away < 0 else from_spot < line
            f = from_spot * 2 + side + o * (1 - 2 * side)

            def receive(kind=kind, away=away, f=f):
                remote(
                    piece(kind, f, twin),
                    piece(kind, f, twin),
                    line_send.at[0],
                    line_slot(kind, away, o),
                    above,
                ).wait_recv()

            pl.when(exists)(receive)
            if d <= line - 2:
                further = -d - 1 if away < 0 else d + 1
                both = jnp.logical_and(exists, has_above if away < 0 else has_below)
                push(
                    kind,
                    group,
                    2 * d + o,
                    f,
                    both,
                    line_slot(kind, further, o),
                    above if away < 0 else below,
                )
            hand_over(kind, away, o, f, exists)

    def hand_over(kind, away, o, f, exists):
        index = (away % line - 1) * 2 + o
        bank = 2 if kind == scales else kind % 2
        slot_of = (bank * 3 + 2) * span_of + index
        first = away > 0
        copy = remote(
            piece(kind, f, twin),
            piece(kind, f, twin),
            line_send.at[slot_of],
            twin_slot(kind, away % line, o),
            twin_peer,
        )
        key = (slot_of, first)
        if key in sending:
            sending.pop(key)()
        pl.when(exists)(lambda: copy.start())
        sending[key] = lambda: pl.when(exists)(lambda: copy.wait_send())

    def pick(table):
        total = 0
        for v in range(line):
            total = total + (spot == v).astype(jnp.int32) * table[v]
        return total

    near = []
    for v in range(line):
        near.append(sorted((u for u in range(line) if u != v), key=lambda u: (abs(u - v), -u)))
    sources = [across(0), across(1)]
    twin_index = [None, None]
    for r in range(line - 1):
        at = pick([near[v][r] for v in range(line)])
        away = pick([(near[v][r] - v) % line for v in range(line)])
        for o in range(2):
            sources.append(at * 2 + side + o * (1 - 2 * side))
            twin_index.append((away - 1) * 2 + o)

    def need_piece(kind, k):
        if k == 1:
            side_need(kind, 0)
            side_need(kind, 1)
        if k > 1:
            remote(
                piece(kind, sources[k], 1 - twin),
                piece(kind, sources[k], 1 - twin),
                line_send.at[0],
                twin_recv.at[kind * span_of + twin_index[k]],
                twin_peer,
            ).wait_recv()

    queue = []
    later = []
    for kind in range(scales):
        members = [kind] if kind != down_kind else [kind, scales]
        for o in range(2):
            queue.append([functools.partial(send_own, m, o) for m in members])
        queue.extend(later)
        later = []
        for d in range(1, line):
            for o in range(2):
                unit = [functools.partial(pass_along, m, d, o) for m in members]
                (queue if d < line - 1 else later).append(unit)
    queue.extend(later)
    middle = 2 * (line - 2)

    def pump(count):
        for _ in range(count):
            for action in queue.pop(0):
                action()

    def send(src, dst, send_sem, recv_sem, peer):
        copy = remote(src, dst, send_sem, recv_sem, peer)
        copy.start()
        started.append(copy)
        return copy

    own_rows = rows_of(fs)
    fetched(("gate", 0))
    gate_full[own_rows, :] = staged_gate[0].astype(bf16)
    fetched(("gate", 1))
    gate_away[...] = staged_gate[1].astype(bf16)
    neighbours = has_above.astype(jnp.int32) + has_below.astype(jnp.int32)
    pl.semaphore_wait(barrier, 3 + neighbours)
    side_send_all(0)
    pump(1)
    fetched(("up", 0))
    up_full[own_rows, :] = staged_up[0].astype(bf16)
    fetched(("up", 1))
    up_away[...] = staged_up[1].astype(bf16)
    side_send_all(1)
    pump(1)
    fetched("rows")
    fetched("small")

    def norm_rows(source, which, target):
        gain = norm_gains[which : which + 1, :]

        def step(i, carry):
            block = pl.ds(pl.multiple_of(i * 16, 16), 16)
            x = source[block, :].astype(f32)
            mean = jnp.mean(x * x, axis=-1, keepdims=True)
            target[block, :] = (x * lax.rsqrt(mean + EPSILON) * gain).astype(bf16)
            return carry

        lax.fori_loop(0, rows // 16, step, 0)

    def slot(j, cols=slice(None)):
        return (pl.ds(j * rows, rows), cols)

    def share_rows(stage):
        part = gathered.at[stage]
        base = 3 * stage
        send(part.at[slot(0)], part.at[slot(1)], row_send.at[base], row_recv.at[base], tp_peer)
        send(
            part.at[slot(0)],
            part.at[slot(2)],
            row_send.at[base + 1],
            row_recv.at[base + 1],
            side_peer,
        )

    def wait_rows(stage, i, j):
        part = gathered.at[stage]
        pltpu.make_async_remote_copy(
            src_ref=part.at[slot(0)],
            dst_ref=part.at[slot(j)],
            send_sem=row_send.at[3 * stage + i],
            recv_sem=row_recv.at[3 * stage + i],
            device_id=tp_peer,
            device_id_type=MESH,
        ).wait_recv()

    def relay_rows(stage):
        wait_rows(stage, 1, 2)
        part = gathered.at[stage]
        send(
            part.at[slot(2)],
            part.at[slot(3)],
            row_send.at[3 * stage + 2],
            row_recv.at[3 * stage + 2],
            tp_peer,
        )

    norm_rows(staged_in, 0, gathered.at[0])
    stream[...] = staged_in[...].astype(f32)
    share_rows(0)

    fetched("down")
    down_full[fs] = staged_down[0].astype(bf16)
    down_away[...] = staged_down[1].astype(bf16)
    cols_full[fs, 0:1, :] = down_scale[...]
    cols_full[fs, 8:9, :] = out_scale[...]
    cols_away[0:1, :] = down_scale[...]
    cols_away[8:9, :] = out_scale[...]
    side_send_all(down_kind)
    side_send_all(scales)
    fetched("heads")
    for h in range(heads):
        keys, vals = slice(h * DK, (h + 1) * DK), slice(h * DV, (h + 1) * DV)
        for i in range(2):
            made = jnp.concatenate(
                [staged_query[i, :, keys], staged_key[i, :, keys], staged_value[i, :, vals]], axis=1
            ).astype(bf16)
            if i == 0:
                head_full[h, own_rows, :] = made
            else:
                head_away[h] = made
        side_send_all(down_kind + 1 + h)
    fetched("out")
    out_full[fs] = staged_out[0].astype(bf16)
    out_away[...] = staged_out[1].astype(bf16)
    side_send_all(out_kind)

    pump(middle + 4)
    relay_rows(0)
    pump(middle + 4)
    wait_rows(0, 0, 1)
    wait_rows(0, 2, 3)

    def dot(a, b):
        return jnp.dot(a, b, preferred_element_type=f32)

    def expand(stage, factor, count, hooks):
        for c in range(units // tile):
            cols = slice(c * tile, (c + 1) * tile)
            span = pl.ds(pl.multiple_of(side * units + c * tile, 128), tile)
            gate = dot(gathered[stage], gate_full[:, cols])
            up = dot(gathered[stage], up_full[:, cols])
            if factor is not None:
                gate, up = gate * factor, up * factor
            gate, up = gate * gate_scale[:, span], up * up_scale[:, span]
            hidden[:, cols] = (gate / (1.0 + jnp.exp(-gate)) * up).astype(bf16)
            if c in hooks:
                pump(hooks[c])

    def part_copy(stage, k, over_side, landing):
        store_out, store_in = (rep_out, rep_in) if over_side else (tp_out, tp_in)
        sem = (stage * n + k) * 2 + over_side
        return remote(
            store_out.at[stage, k],
            store_in.at[stage, landing],
            part_send.at[sem],
            part_recv.at[(stage * n + landing) * 2 + over_side],
            side_peer if over_side else tp_peer,
        )

    def part_start(stage, k, over_side):
        copy = part_copy(stage, k, over_side, k ^ over_side)
        copy.start()
        started.append(copy)

    def part_wait(stage, k, over_side):
        part_copy(stage, k, over_side, k).wait_recv()

    def contract(stage, lhs, weight, row, fresh, hooks, finish, relay=None):
        def multiply(k):
            if fresh is not None:
                need_piece(fresh, k)
                if fresh == down_kind:
                    need_piece(scales, k)
            f = sources[k]
            part = dot(lhs[...], weight[f]) * cols_full[f, 8 * row : 8 * row + 1, :]
            own_part[k] = part[:rows]
            far_part[k] = part[2 * rows : 3 * rows]
            tp_out[stage, k, 0] = part[rows : 2 * rows].astype(bf16)
            tp_out[stage, k, 1] = part[3 * rows :].astype(bf16)
            part_start(stage, k, 0)

        def pass_on(k):
            part_wait(stage, k, 0)
            rep_out[stage, k] = (far_part[k] + tp_in[stage, k, 1].astype(f32)).astype(bf16)
            part_start(stage, k, 1)

        def collect(k):
            part_wait(stage, k, 1)
            total = own_part[k] + tp_in[stage, k, 0].astype(f32) + rep_in[stage, k].astype(f32)
            finish(k, sources[k], total)

        lags = [(multiply, 0), (pass_on, 1), (collect, 3)]
        if relay is not None:
            lags.append((relay, 5))
        for step in range(n + lags[-1][1]):
            if step in hooks:
                pump(hooks[step])
            for action, lag in lags:
                if 0 <= step - lag < n:
                    action(step - lag)

    def need_all(kind):
        for k in range(1, n):
            need_piece(kind, k)

    def steps(taken, tail):
        hooks = {2 * r: 2 for r in range(1, line - 1)}
        hooks[2] = hooks[2] - taken
        hooks[2 * (line - 1)] = tail
        return hooks

    need_all(0)
    need_all(up_kind)
    expand(0, None, 1, {1: 1, 2: 1})

    def add_half(k, f, total):
        cols = columns_of(f)
        stream[:, cols] = stream[:, cols] + 0.5 * total

    contract(0, hidden, down_full, 0, down_kind, steps(2, 4), add_half)

    norm_rows(stream, 1, gathered.at[1])
    share_rows(1)
    pump(middle)
    relay_rows(1)
    pump(4)

    seq_len = 2 * rows
    row = lax.rem(
        lax.broadcasted_iota(jnp.int32, (seq_len, seq_len), 0) + tp * rows, seq_len
    )
    col = lax.rem(
        lax.broadcasted_iota(jnp.int32, (seq_len, seq_len), 1) + tp * rows, seq_len
    )

    def retain(h, hooks):
        places = [
            (query_scale, 0, DK, 1.0),
            (key_scale, DK, DK, 1.0 / math.sqrt(DK)),
            (value_scale, 2 * DK, DV, 1.0),
        ]
        made = []
        for i, (scale, first, size, factor) in enumerate(places):
            span = pl.ds(pl.multiple_of((side * heads + h) * size, 128), size)
            product = dot(gathered[1], head_full[h, :, first : first + size])
            made.append((product * (scale[:, span] * factor)).astype(bf16))
            if i in hooks:
                pump(hooks[i])
        query, keys, values = made
        decay = decay_rate[side * heads + h]
        distance = jnp.abs(row - col).astype(f32)
        weight = jnp.where(
            lax.div(col, BLOCK) <= lax.div(row, BLOCK), jnp.exp(-decay * distance), 0.0
        )
        for s in range(2):
            span = slice(s * seq_len, (s + 1) * seq_len)
            scores = lax.dot_general(
                query[span], keys[span], (((1,), (1,)), ((), ())), preferred_element_type=f32
            )
            scores = (scores * weight).astype(bf16)
            retained = dot(scores, values[span])
            centred = retained - jnp.mean(retained, axis=-1, keepdims=True)
            spread = jnp.mean(centred * centred, axis=-1, keepdims=True)
            mixed[span, h * DV : (h + 1) * DV] = (
                centred * lax.rsqrt(spread + EPSILON) * head_gain[...]
            ).astype(bf16)

    for h in range(heads):
        if h == 0:
            wait_rows(1, 0, 1)
            wait_rows(1, 2, 3)
        need_all(down_kind + 1 + h)
        retain(h, {1: 1})
        if h < heads - 1:
            pump(middle + 3)

    last = gathered.at[2]

    def block_copy(k, i, start):
        cols = columns_of(sources[k])
        a, b, peer = ((0, 1, tp_peer), (0, 2, side_peer), (2, 3, tp_peer))[i]
        return pltpu.make_async_remote_copy(
            src_ref=last.at[slot(a, cols)],
            dst_ref=last.at[slot(b, cols)],
            send_sem=block_send.at[3 * k + i],
            recv_sem=block_recv.at[3 * (k ^ 1 if i == 1 and start else k) + i],
            device_id=peer,
            device_id_type=MESH,
        )

    def factor_copy(i):
        a, b, peer = ((0, 1, tp_peer), (0, 2, side_peer), (2, 3, tp_peer))[i]
        return pltpu.make_async_remote_copy(
            src_ref=factors.at[a],
            dst_ref=factors.at[b],
            send_sem=block_send.at[3 * n + i],
            recv_sem=block_recv.at[3 * n + i],
            device_id=peer,
            device_id_type=MESH,
        )

    squares[...] = jnp.zeros_like(squares)

    def add_mix(k, f, total):
        cols = columns_of(f)
        second = stream[:, cols] + total
        stream[:, cols] = second
        last[slot(0, cols)] = (second * norm_gains[2:3, cols]).astype(bf16)
        square = second * second
        added = squares[...]
        for i in range(width // 128):
            added = added + square[:, i * 128 : (i + 1) * 128]
        squares[...] = added
        for i in (0, 1):
            copy = block_copy(k, i, True)
            copy.start()
            started.append(copy)
        if k == n - 1:
            mean = jnp.sum(added, axis=-1, keepdims=True) / features
            wide = jnp.broadcast_to(lax.rsqrt(mean + EPSILON), (rows, rows))
            factors[0] = wide.T[:8, :]
            for i in (0, 1):
                copy = factor_copy(i)
                copy.start()
                started.append(copy)

    def relay_block(k):
        block_copy(k, 1, False).wait_recv()
        copy = block_copy(k, 2, True)
        copy.start()
        started.append(copy)
        if k == n - 1:
            factor_copy(1).wait_recv()
            copy = factor_copy(2)
            copy.start()
            started.append(copy)

    contract(1, mixed, out_full, 1, out_kind, steps(1, 2), add_mix, relay_block)
    for k in range(n):
        block_copy(k, 0, False).wait_recv()
        block_copy(k, 2, False).wait_recv()
    factor_copy(0).wait_recv()
    factor_copy(2).wait_recv()
    factor = jnp.concatenate(
        [jnp.broadcast_to(factors[j, 0:1, :], (rows, rows)).T[:, 0:1] for j in range(4)], axis=0
    )
    expand(2, factor, 1, {})

    def write(k, f, total):
        cols = columns_of(f)
        result[:, cols] = (stream[:, cols] + 0.5 * total).astype(bf16)

    contract(2, hidden, down_full, 0, None, {}, write)
    assert not queue
    for finish in sending.values():
        finish()
    for copy in started:
        copy.wait_send()


def fused(
    n_rep,
    n_fs,
    n_tp,
    tokens_in,
    norm_gains,
    gate_w,
    gate_scale,
    up_w,
    up_scale,
    down_w,
    down_scale,
    query_w,
    query_scale,
    key_w,
    key_scale,
    value_w,
    value_scale,
    out_w,
    out_scale,
    head_gain,
    decay_rate,
):
    f32, bf16 = jnp.float32, jnp.bfloat16
    n = n_fs
    rows, features = tokens_in.shape
    width, units = gate_w.shape[0], gate_w.shape[1] // 2
    heads = decay_rate.shape[0] // 2
    kinds = heads + 5
    span_of = n - 2
    any_space = pl.BlockSpec(memory_space=pl.ANY)
    vmem = pl.BlockSpec(memory_space=pltpu.VMEM)
    smem = pl.BlockSpec(memory_space=pltpu.SMEM)
    dma = pltpu.SemaphoreType.DMA

    return pl.pallas_call(
        functools.partial(layer_kernel, n),
        out_shape=pltpu.VMEM((rows, features), bf16),
        in_specs=[any_space] * 17 + [smem],
        out_specs=vmem,
        scratch_shapes=[
            pltpu.VMEM(norm_gains.shape, f32),
        ]
        + [
            pltpu.VMEM((1, x.shape[0]), f32)
            for x in (
                gate_scale,
                up_scale,
                down_scale,
                query_scale,
                key_scale,
                value_scale,
                out_scale,
                head_gain,
            )
        ]
        + [
            pltpu.VMEM((rows, features), bf16),
            pltpu.VMEM((2, width, units), f32),
            pltpu.VMEM((2, width, units), f32),
            pltpu.VMEM((2, units, width), f32),
            pltpu.VMEM((2, width, heads * DK), f32),
            pltpu.VMEM((2, width, heads * DK), f32),
            pltpu.VMEM((2, width, heads * DV), f32),
            pltpu.VMEM((2, heads * DV, width), f32),
            pltpu.VMEM((width, units), bf16),
            pltpu.VMEM((width, units), bf16),
            pltpu.VMEM((units, width), bf16),
            pltpu.VMEM((heads, width, 2 * DK + DV), bf16),
            pltpu.VMEM((heads * DV, width), bf16),
            pltpu.VMEM((16, width), f32),
            pltpu.VMEM((features, units), bf16),
            pltpu.VMEM((features, units), bf16),
            pltpu.VMEM((n, units, width), bf16),
            pltpu.VMEM((heads, features, 2 * DK + DV), bf16),
            pltpu.VMEM((n, heads * DV, width), bf16),
            pltpu.VMEM((n, 16, width), f32),
            pltpu.VMEM((3, 4 * rows, features), bf16),
            pltpu.VMEM((4, 8, rows), f32),
            pltpu.VMEM((rows, features), f32),
            pltpu.VMEM((rows, 128), f32),
            pltpu.VMEM((4 * rows, units), bf16),
            pltpu.VMEM((4 * rows, heads * DV), bf16),
            pltpu.VMEM((n, rows, width), f32),
            pltpu.VMEM((n, rows, width), f32),
            pltpu.VMEM((3, n, 2, rows, width), bf16),
            pltpu.VMEM((3, n, 2, rows, width), bf16),
            pltpu.VMEM((3, n, rows, width), bf16),
            pltpu.VMEM((3, n, rows, width), bf16),
            dma((24,)),
            dma((kinds + 2,)),
            dma((kinds + 2,)),
            dma((9 * span_of,)),
            dma((kinds * span_of,)),
            dma((kinds * span_of,)),
            dma((3 * n * 2,)),
            dma((3 * n * 2,)),
            dma((6,)),
            dma((6,)),
            dma((3 * n + 3,)),
            dma((3 * n + 3,)),
        ],
        compiler_params=pltpu.CompilerParams(
            collective_id=0, has_side_effects=True, vmem_limit_bytes=VMEM_LIMIT
        ),
        name="layer",
    )(
        tokens_in,
        norm_gains,
        gate_w,
        gate_scale,
        up_w,
        up_scale,
        down_w,
        down_scale,
        query_w,
        query_scale,
        key_w,
        key_scale,
        value_w,
        value_scale,
        out_w,
        out_scale,
        head_gain,
        decay_rate,
    )


def solution(mesh):
    sizes = [mesh.shape[axis] for axis in ("rep", "fs", "tp")]
    placed = (
        P(("rep", "fs", "tp"), None),
        P(),
        P("fs", "tp"),
        P("tp"),
        P("fs", "tp"),
        P("tp"),
        P("tp", "fs"),
        P("fs"),
        P("fs", "tp"),
        P("tp"),
        P("fs", "tp"),
        P("tp"),
        P("fs", "tp"),
        P("tp"),
        P("tp", "fs"),
        P("fs"),
        P(),
        P("tp"),
    )
    return jax.shard_map(
        lambda *args: (fused if fits(*sizes, *args) else on_device)(*sizes, *args),
        mesh=mesh,
        in_specs=placed,
        out_specs=P(("rep", "fs", "tp"), None),
        check_vma=False,
    )
```

```python
import functools
import math

import jax
import jax.numpy as jnp
from jax import lax
from jax.experimental import pallas as pl
from jax.experimental.pallas import tpu as pltpu
from jax.sharding import PartitionSpec as P

DK = 256
DV = 256
BLOCK = 64

EPSILON = 1e-05


def rms_scale(stream, gain):
    return stream * lax.rsqrt(jnp.mean(stream * stream, axis=-1, keepdims=True) + EPSILON) * gain


def snake(n):
    return [i for i in range(0, n, 2)] + [i for i in range(n - 1, 0, -1) if i % 2 == 1]


def snake_place(index, n):
    return jnp.where(index % 2 == 0, index // 2, n - 1 - index // 2)


def snake_index(place, n):
    half = (n + 1) // 2
    return jnp.where(place < half, 2 * place, 2 * (n - 1 - place) + 1)


def shift(x, axis, n, by):
    return lax.ppermute(x, axis, [(i, (i + by) % n) for i in range(n)])


def ring_gather(shards, n, forward_steps):
    order = snake(n)
    ahead = [(order[i], order[(i + 1) % n]) for i in range(n)]
    behind = [(b, a) for a, b in ahead]
    found = []
    for x, steps in zip(shards, forward_steps):
        forward, back = [x], [x]
        found.append((forward, back))
    for step in range(n):
        for (forward, back), steps in zip(found, forward_steps):
            if step < steps:
                forward.append(lax.ppermute(forward[-1], "fs", ahead))
            if step < n - 1 - steps:
                back.append(lax.ppermute(back[-1], "fs", behind))
    return [forward + back[:0:-1] for forward, back in found]


def chained(shards, before, hops):
    if not before:
        return shards
    last = []
    n = len(before[0])
    for pieces in before:
        last.extend([pieces[hops], pieces[n - hops]])
    return lax.optimization_barrier((tuple(shards), tuple(last)))[0]


def with_scale(weight, scale):
    high = lax.reduce_precision(scale, 8, 7)
    middle = lax.reduce_precision(scale - high, 8, 7)
    rows = jnp.stack([high, middle, scale - high - middle]).astype(jnp.bfloat16)
    return jnp.concatenate([weight, jnp.pad(rows, ((0, 13), (0, 0)))], axis=0)


def without_scale(pieces):
    size = pieces[0].shape[0] - 16
    weight = jnp.concatenate([p[:size] for p in pieces], axis=1)
    rows = jnp.concatenate([p[size:] for p in pieces], axis=1)[:3].astype(jnp.float32)
    return weight, rows[0] + rows[1] + rows[2]


def retain(query, key_rows, value, decay, head_gain):
    seq_len = query.shape[0]
    row = lax.broadcasted_iota(jnp.int32, (seq_len, seq_len), 0)
    col = lax.broadcasted_iota(jnp.int32, (seq_len, seq_len), 1)
    distance = jnp.abs(row - col).astype(jnp.float32)
    weight = jnp.where(col // BLOCK <= row // BLOCK, jnp.exp(-decay * distance), 0.0)
    scores = lax.dot_general(
        query, key_rows, (((1,), (1,)), ((), ())), preferred_element_type=jnp.float32
    )
    scores = (scores * weight).astype(jnp.bfloat16)
    retained = jnp.dot(scores, value, preferred_element_type=jnp.float32)
    centred = retained - jnp.mean(retained, axis=-1, keepdims=True)
    normed = (
        centred
        * lax.rsqrt(jnp.mean(centred * centred, axis=-1, keepdims=True) + EPSILON)
        * head_gain
    )
    return normed.astype(jnp.bfloat16)


def on_device(
    n_rep,
    n_fs,
    n_tp,
    tokens_in,
    norm_gains,
    gate_w,
    gate_scale,
    up_w,
    up_scale,
    down_w,
    down_scale,
    query_w,
    query_scale,
    key_w,
    key_scale,
    value_w,
    value_scale,
    out_w,
    out_scale,
    head_gain,
    decay_rate,
):
    rows = tokens_in.shape[0]
    width = gate_w.shape[0]
    heads = decay_rate.shape[0]
    units = gate_w.shape[1]
    share = n_rep if heads % n_rep == 0 and units % (n_rep * 128) == 0 else 1
    heads //= share
    units //= share
    rep = lax.axis_index("rep") if share > 1 else 0
    tp = lax.axis_index("tp")
    place = snake_place(lax.axis_index("fs"), n_fs)

    def part(x, axis):
        size = x.shape[axis] // share
        return lax.dynamic_slice_in_dim(x, rep * size, size, axis)

    gate_b, up_b, query_b, key_b, value_b = (
        part(w, 1).astype(jnp.bfloat16) for w in (gate_w, up_w, query_w, key_w, value_w)
    )
    down_b, out_b = (part(w, 0).astype(jnp.bfloat16) for w in (down_w, out_w))

    few, many = (n_fs - 1) // 2, n_fs // 2
    first_pieces = ring_gather([gate_b, up_b], n_fs, [many, few])
    half = down_b.shape[0] // 2
    second_pieces = ring_gather(
        chained([with_scale(down_b[:half], down_scale), down_b[half:]], first_pieces, max(1, n_fs // 4)),
        n_fs,
        [many, few],
    )
    third_pieces = ring_gather(chained([query_b, key_b], second_pieces, few), n_fs, [many, few])
    value_pieces, out_pieces = ring_gather(
        chained([value_b, with_scale(out_b, out_scale)], third_pieces, few), n_fs, [many, few]
    )

    gate_full, up_full = (jnp.concatenate(p, axis=0) for p in first_pieces)
    down_top, down_cols = without_scale(second_pieces[0])
    down_rest = jnp.concatenate(second_pieces[1], axis=1)
    down_full = lax.optimization_barrier(jnp.concatenate([down_top, down_rest], axis=0))
    query_full, key_full = (jnp.concatenate(p, axis=0) for p in third_pieces)
    value_full = jnp.concatenate(value_pieces, axis=0)
    out_full, out_cols = without_scale(out_pieces)

    def to_ring(x):
        blocks = [
            lax.dynamic_slice_in_dim(
                x, snake_index((place - k) % n_fs, n_fs) * width, width, axis=1
            )
            for k in range(n_fs)
        ]
        return jnp.concatenate(blocks, axis=1)

    def from_ring(x):
        blocks = [
            lax.dynamic_slice_in_dim(x, (place - snake(n_fs).index(o)) % n_fs * width, width, axis=1)
            for o in range(n_fs)
        ]
        return jnp.concatenate(blocks, axis=1)

    def over_tp(x, ordered):
        found = [x] + [shift(x, "tp", n_tp, k) for k in range(1, n_tp)]
        if not ordered:
            return jnp.concatenate(found, axis=0)
        twice = jnp.concatenate(found[::-1] * 2, axis=0)
        return lax.dynamic_slice_in_dim(twice, (n_tp - 1 - tp) * rows, n_tp * rows, axis=0)

    def gather_rows(normed, ordered=False):
        found = [normed] + [shift(normed, "rep", n_rep, k) for k in range(1, share)]
        return [over_tp(x, ordered) for x in found]

    def return_rows(parts, ordered=False):
        total = None
        for k in range(share - 1, -1, -1):

            def block(j):
                at = (tp - j) % n_tp * rows if ordered else j * rows
                return lax.dynamic_slice_in_dim(parts[k], at, rows, axis=0)

            mine = block(0)
            for j in range(1, n_tp):
                other = shift(block(j).astype(jnp.bfloat16), "tp", n_tp, n_tp - j)
                mine = mine + other.astype(jnp.float32)
            if k > 0:
                mine = shift(mine.astype(jnp.bfloat16), "rep", n_rep, n_rep - k).astype(jnp.float32)
            total = mine if total is None else total + mine
        return total

    def dot(a, b):
        return jnp.dot(a, b, preferred_element_type=jnp.float32)

    gate_col, up_col = part(gate_scale, 0), part(up_scale, 0)

    def feed_forward(stream, gain):
        parts = []
        for gathered in gather_rows(rms_scale(stream, gain).astype(jnp.bfloat16)):
            gate_value = dot(gathered, gate_full) * gate_col
            up_value = dot(gathered, up_full) * up_col
            hidden = (jax.nn.silu(gate_value) * up_value).astype(jnp.bfloat16)
            hidden = lax.optimization_barrier(hidden)
            parts.append(dot(hidden, down_full) * down_cols)
        return return_rows(parts)

    query_col, key_col, value_col = (part(s, 0) for s in (query_scale, key_scale, value_scale))
    decay = part(decay_rate, 0)
    gains = to_ring(norm_gains)

    stream = to_ring(tokens_in).astype(jnp.float32)
    stream = stream + 0.5 * feed_forward(stream, gains[0])
    parts = []
    for gathered in gather_rows(
        rms_scale(stream, gains[1]).astype(jnp.bfloat16), ordered=True
    ):
        query = (dot(gathered, query_full) * query_col).astype(jnp.bfloat16)
        key_rows = (dot(gathered, key_full) * key_col / math.sqrt(DK)).astype(jnp.bfloat16)
        value = (dot(gathered, value_full) * value_col).astype(jnp.bfloat16)
        mixed = [
            retain(
                query[:, h * DK : (h + 1) * DK],
                key_rows[:, h * DK : (h + 1) * DK],
                value[:, h * DV : (h + 1) * DV],
                decay[h],
                head_gain,
            )
            for h in range(heads)
        ]
        parts.append(dot(jnp.concatenate(mixed, axis=1), out_full) * out_cols)
    stream = stream + return_rows(parts, ordered=True)
    stream = stream + 0.5 * feed_forward(stream, gains[2])
    return from_ring(stream.astype(jnp.bfloat16))


MESH = pl.DeviceIdType.MESH
VMEM_LIMIT = 62 * 1024 * 1024


def fits(n_rep, n_fs, n_tp, tokens_in, norm_gains, gate_w, *rest):
    rows, features = tokens_in.shape
    width, units = gate_w.shape
    heads = rest[-1].shape[0]
    return (
        n_rep == 2
        and n_tp == 2
        and n_fs >= 6
        and n_fs % 2 == 0
        and n_fs <= 16
        and rows % 128 == 0
        and width % 256 == 0
        and features == n_fs * width
        and units % 512 == 0
        and heads % 2 == 0
    )


def layer_kernel(
    n,
    tokens_in,
    norm_gains_in,
    gate_w,
    gate_scale_in,
    up_w,
    up_scale_in,
    down_w,
    down_scale_in,
    query_w,
    query_scale_in,
    key_w,
    key_scale_in,
    value_w,
    value_scale_in,
    out_w,
    out_scale_in,
    head_gain_in,
    decay_rate,
    result,
    norm_gains,
    gate_scale,
    up_scale,
    down_scale,
    query_scale,
    key_scale,
    value_scale,
    out_scale,
    head_gain,
    staged_in,
    staged_gate,
    staged_up,
    staged_down,
    staged_query,
    staged_key,
    staged_value,
    staged_out,
    gate_away,
    up_away,
    down_away,
    head_away,
    out_away,
    cols_away,
    gate_full,
    up_full,
    down_full,
    head_full,
    out_full,
    cols_full,
    gathered,
    factors,
    stream,
    squares,
    hidden,
    mixed,
    own_part,
    far_part,
    tp_out,
    tp_in,
    rep_out,
    rep_in,
    local_sem,
    side_send,
    side_recv,
    line_send,
    line_recv,
    twin_recv,
    part_send,
    part_recv,
    row_send,
    row_recv,
    block_send,
    block_recv,
):
    f32, bf16 = jnp.float32, jnp.bfloat16
    rows, features = tokens_in.shape
    width = gate_w.shape[0]
    units = hidden.shape[1]
    heads = head_full.shape[0]
    tile = 256

    twin, fs, tp = (lax.axis_index(axis) for axis in ("rep", "fs", "tp"))
    line = n // 2
    side, spot = lax.rem(fs, 2), lax.div(fs, 2)
    above, below = {"fs": fs + 2}, {"fs": fs - 2}
    side_peer, twin_peer, tp_peer = {"fs": fs + 1 - 2 * side}, {"rep": 1 - twin}, {"tp": 1 - tp}
    has_above, has_below = spot + 1 < line, spot > 0

    barrier = pltpu.get_barrier_semaphore()

    def greet(peer):
        pl.semaphore_signal(barrier, inc=1, device_id=peer, device_id_type=MESH)

    def meet():
        for peer in (side_peer, twin_peer, tp_peer):
            greet(peer)
        pl.when(has_above)(lambda: greet(above))
        pl.when(has_below)(lambda: greet(below))

    meet()

    def columns_of(f):
        return pl.ds(pl.multiple_of(f * width, width), width)

    def halves(size):
        return [pl.ds(pl.multiple_of(i * size, 128), size) for i in (side, 1 - side)]

    local, copies_of = [], {}

    def fetch(name, src, dst):
        copy = pltpu.make_async_copy(src, dst, local_sem.at[len(local)])
        copy.start()
        copies_of.setdefault(name, []).append(copy)
        local.append(copy)

    def fetched(name):
        for copy in copies_of[name]:
            copy.wait()

    for i, cols in enumerate(halves(units)):
        fetch(("gate", i), gate_w.at[:, cols], staged_gate.at[i])
    for i, cols in enumerate(halves(units)):
        fetch(("up", i), up_w.at[:, cols], staged_up.at[i])
    fetch("rows", tokens_in, staged_in)
    for src, dst in (
        (gate_scale_in, gate_scale),
        (up_scale_in, up_scale),
        (down_scale_in, down_scale),
        (query_scale_in, query_scale),
        (key_scale_in, key_scale),
        (value_scale_in, value_scale),
        (out_scale_in, out_scale),
        (head_gain_in, head_gain),
    ):
        fetch("small", src, dst.at[0])
    fetch("small", norm_gains_in, norm_gains)
    for i, cols in enumerate(halves(units)):
        fetch("down", down_w.at[cols, :], staged_down.at[i])
    for i, cols in enumerate(halves(heads * DK)):
        fetch("heads", query_w.at[:, cols], staged_query.at[i])
        fetch("heads", key_w.at[:, cols], staged_key.at[i])
    for i, cols in enumerate(halves(heads * DV)):
        fetch("heads", value_w.at[:, cols], staged_value.at[i])
        fetch("out", out_w.at[cols, :], staged_out.at[i])

    started = []
    half_units, half_width, half_out = units // 2, width // 2, heads * DV // 2

    def rows_of(f):
        return pl.ds(pl.multiple_of(f * width, width), width)

    def cut(ref, s, size):
        return ref.at[pl.ds(pl.multiple_of(s * size, size), size), :]

    kinds = [
        (lambda f: gate_full.at[rows_of(f), :], gate_away, half_width),
        (lambda f: up_full.at[rows_of(f), :], up_away, half_width),
        (lambda f: down_full.at[f], down_away, half_units),
    ]
    for h in range(heads):
        kinds.append(
            (lambda f, h=h: head_full.at[h, rows_of(f), :], head_away.at[h], half_width)
        )
    kinds.append((lambda f: out_full.at[f], out_away, half_out))
    scales = len(kinds)
    kinds.append((lambda f: cols_full.at[f], cols_away, 8))
    up_kind, down_kind, out_kind = 1, 2, scales - 1

    def piece(kind, f, s):
        return cut(kinds[kind][0](f), s, kinds[kind][2])

    def remote(src, dst, send_sem, recv_sem, peer):
        return pltpu.make_async_remote_copy(
            src_ref=src,
            dst_ref=dst,
            send_sem=send_sem,
            recv_sem=recv_sem,
            device_id=peer,
            device_id_type=MESH,
        )

    def across(o):
        return spot * 2 + side + o * (1 - 2 * side)

    def side_slot(kind, i):
        return kind * 2 + i if kind <= up_kind else kind + 2

    def side_copy(kind, i, f):
        slot_of = side_slot(kind, i)
        sems = side_send.at[slot_of], side_recv.at[slot_of]
        if kind <= up_kind:
            s = twin if i == 0 else 1 - twin
            return remote(
                cut(kinds[kind][1], s, kinds[kind][2]), piece(kind, f, s), *sems, side_peer
            )
        return remote(kinds[kind][1], kinds[kind][0](f), *sems, side_peer)

    def side_start(kind, i=0):
        copy = side_copy(kind, i, fs)
        copy.start()
        started.append(copy)

    side_done = set()

    def side_need(kind, i):
        i = i if kind <= up_kind else 0
        if (kind, i) not in side_done:
            side_done.add((kind, i))
            side_copy(kind, i, across(1)).wait_recv()

    span_of = 2 * (line - 1)
    sending = {}

    def push(kind, group, index, f, where, recv, peer):
        bank = 2 if kind == scales else kind % 2
        slot_of = (bank * 3 + group) * span_of + index
        copy = remote(piece(kind, f, twin), piece(kind, f, twin), line_send.at[slot_of], recv, peer)
        if slot_of in sending:
            sending.pop(slot_of)()
        guard = functools.partial(pl.when, where) if where is not None else None

        def begin():
            copy.start()

        def finish():
            copy.wait_send()

        if guard is None:
            begin()
            sending[slot_of] = finish
        else:
            guard()(begin)
            sending[slot_of] = lambda: guard()(finish)

    def line_slot(kind, away, o):
        return line_recv.at[kind * span_of + (away % line - 1) * 2 + o]

    def twin_slot(kind, away, o):
        return twin_recv.at[kind * span_of + (away - 1) * 2 + o]

    def send_own(kind, o):
        if o == 1:
            side_need(kind, 0)
        f = across(o)
        push(kind, 0, o, f, has_above, line_slot(kind, -1, o), above)
        push(kind, 1, o, f, has_below, line_slot(kind, 1, o), below)

    def places(d, o):
        for group, away in ((0, -d), (1, d)):
            from_spot = spot + away
            exists = from_spot >= 0 if away < 0 else from_spot < line
            yield group, away, exists, from_spot * 2 + side + o * (1 - 2 * side)

    def take_in(kind, d, o):
        for group, away, exists, f in places(d, o):

            def receive(kind=kind, away=away, f=f):
                remote(
                    piece(kind, f, twin),
                    piece(kind, f, twin),
                    line_send.at[0],
                    line_slot(kind, away, o),
                    above,
                ).wait_recv()

            pl.when(exists)(receive)
            hand_over(kind, away, o, f, exists)

    def move_on(kind, d, o):
        if d > line - 2:
            return
        for group, away, exists, f in places(d, o):
            further = -d - 1 if away < 0 else d + 1
            push(
                kind,
                group,
                2 * d + o,
                f,
                jnp.logical_and(exists, has_above if away < 0 else has_below),
                line_slot(kind, further, o),
                above if away < 0 else below,
            )

    def pass_along(kind, d, o):
        take_in(kind, d, o)
        move_on(kind, d, o)

    def hand_over(kind, away, o, f, exists):
        index = (away % line - 1) * 2 + o
        bank = 2 if kind == scales else kind % 2
        slot_of = (bank * 3 + 2) * span_of + index
        first = away > 0
        copy = remote(
            piece(kind, f, twin),
            piece(kind, f, twin),
            line_send.at[slot_of],
            twin_slot(kind, away % line, o),
            twin_peer,
        )
        key = (slot_of, first)
        if key in sending:
            sending.pop(key)()
        pl.when(exists)(lambda: copy.start())
        sending[key] = lambda: pl.when(exists)(lambda: copy.wait_send())

    def pick(table):
        total = 0
        for v in range(line):
            total = total + (spot == v).astype(jnp.int32) * table[v]
        return total

    near = []
    for v in range(line):
        near.append(sorted((u for u in range(line) if u != v), key=lambda u: (abs(u - v), -u)))
    sources = [across(0), across(1)]
    twin_index = [None, None]
    for r in range(line - 1):
        at = pick([near[v][r] for v in range(line)])
        away = pick([(near[v][r] - v) % line for v in range(line)])
        for o in range(2):
            sources.append(at * 2 + side + o * (1 - 2 * side))
            twin_index.append((away - 1) * 2 + o)

    def need_piece(kind, k):
        if k == 1:
            side_need(kind, 0)
            side_need(kind, 1)
        if k > 1:
            remote(
                piece(kind, sources[k], 1 - twin),
                piece(kind, sources[k], 1 - twin),
                line_send.at[0],
                twin_recv.at[kind * span_of + twin_index[k]],
                twin_peer,
            ).wait_recv()

    queue = []
    later = []
    for members in [[0, up_kind], [down_kind, scales]] + [[k] for k in range(down_kind + 1, scales)]:
        for o in range(2):
            queue.append([functools.partial(send_own, m, o) for m in members])
        queue.extend(later)
        later = []
        for d in range(1, line):
            for o in range(2):
                unit = [functools.partial(pass_along, m, d, o) for m in members]
                (queue if d < line - 1 else later).append(unit)
    queue.extend(later)
    middle = 2 * (line - 2)

    def pump(count):
        for _ in range(count):
            for action in queue.pop(0):
                action()

    def send(src, dst, send_sem, recv_sem, peer):
        copy = remote(src, dst, send_sem, recv_sem, peer)
        copy.start()
        started.append(copy)
        return copy

    own_rows = rows_of(fs)
    fetched(("gate", 0))
    gate_full[own_rows, :] = staged_gate[0].astype(bf16)
    fetched(("gate", 1))
    gate_away[...] = staged_gate[1].astype(bf16)
    neighbours = has_above.astype(jnp.int32) + has_below.astype(jnp.int32)
    pl.semaphore_wait(barrier, 3 + neighbours)
    side_start(0)
    first, second, _ = (queue.pop(0) for _ in range(3))
    first[0]()
    fetched(("up", 0))
    up_full[own_rows, :] = staged_up[0].astype(bf16)
    fetched(("up", 1))
    up_away[...] = staged_up[1].astype(bf16)
    first[1]()
    fetched("rows")
    fetched("small")

    def norm_rows(source, which, target):
        gain = norm_gains[which : which + 1, :]

        def step(i, carry):
            block = pl.ds(pl.multiple_of(i * 16, 16), 16)
            x = source[block, :].astype(f32)
            mean = jnp.mean(x * x, axis=-1, keepdims=True)
            target[block, :] = (x * lax.rsqrt(mean + EPSILON) * gain).astype(bf16)
            return carry

        lax.fori_loop(0, rows // 16, step, 0)

    def slot(j, cols=slice(None)):
        return (pl.ds(j * rows, rows), cols)

    def share_rows(stage):
        part = gathered.at[stage]
        base = 3 * stage
        send(part.at[slot(0)], part.at[slot(1)], row_send.at[base], row_recv.at[base], tp_peer)
        send(
            part.at[slot(0)],
            part.at[slot(2)],
            row_send.at[base + 1],
            row_recv.at[base + 1],
            side_peer,
        )

    def wait_rows(stage, i, j):
        part = gathered.at[stage]
        pltpu.make_async_remote_copy(
            src_ref=part.at[slot(0)],
            dst_ref=part.at[slot(j)],
            send_sem=row_send.at[3 * stage + i],
            recv_sem=row_recv.at[3 * stage + i],
            device_id=tp_peer,
            device_id_type=MESH,
        ).wait_recv()

    def relay_rows(stage):
        wait_rows(stage, 1, 2)
        part = gathered.at[stage]
        send(
            part.at[slot(2)],
            part.at[slot(3)],
            row_send.at[3 * stage + 2],
            row_recv.at[3 * stage + 2],
            tp_peer,
        )

    norm_rows(staged_in, 0, gathered.at[0])
    stream[...] = staged_in[...].astype(f32)
    take_in(0, 1, 0)
    second[0]()
    side_start(up_kind)
    take_in(up_kind, 1, 0)
    second[1]()
    move_on(0, 1, 0)
    move_on(up_kind, 1, 0)
    side_start(0, 1)
    side_start(up_kind, 1)
    share_rows(0)

    fetched("down")
    down_full[fs] = staged_down[0].astype(bf16)
    down_away[...] = staged_down[1].astype(bf16)
    cols_full[fs, 0:1, :] = down_scale[...]
    cols_full[fs, 8:9, :] = out_scale[...]
    cols_away[0:1, :] = down_scale[...]
    cols_away[8:9, :] = out_scale[...]
    side_start(down_kind)
    side_start(scales)
    fetched("heads")
    for h in range(heads):
        keys, vals = slice(h * DK, (h + 1) * DK), slice(h * DV, (h + 1) * DV)
        for i in range(2):
            made = jnp.concatenate(
                [staged_query[i, :, keys], staged_key[i, :, keys], staged_value[i, :, vals]], axis=1
            ).astype(bf16)
            if i == 0:
                head_full[h, own_rows, :] = made
            else:
                head_away[h] = made
        side_start(down_kind + 1 + h)
    fetched("out")
    out_full[fs] = staged_out[0].astype(bf16)
    out_away[...] = staged_out[1].astype(bf16)
    side_start(out_kind)

    pump(middle - 1)
    relay_rows(0)
    pump(middle + 4)
    wait_rows(0, 0, 1)
    wait_rows(0, 2, 3)

    def dot(a, b):
        return jnp.dot(a, b, preferred_element_type=f32)

    def expand(stage, factor, count, hooks):
        for c in range(units // tile):
            cols = slice(c * tile, (c + 1) * tile)
            span = pl.ds(pl.multiple_of(side * units + c * tile, 128), tile)
            gate = dot(gathered[stage], gate_full[:, cols])
            up = dot(gathered[stage], up_full[:, cols])
            if factor is not None:
                gate, up = gate * factor, up * factor
            gate, up = gate * gate_scale[:, span], up * up_scale[:, span]
            hidden[:, cols] = (gate / (1.0 + jnp.exp(-gate)) * up).astype(bf16)
            if c in hooks:
                pump(hooks[c])

    def part_copy(stage, k, over_side, landing):
        store_out, store_in = (rep_out, rep_in) if over_side else (tp_out, tp_in)
        sem = (stage * n + k) * 2 + over_side
        return remote(
            store_out.at[stage, k],
            store_in.at[stage, landing],
            part_send.at[sem],
            part_recv.at[(stage * n + landing) * 2 + over_side],
            side_peer if over_side else tp_peer,
        )

    def part_start(stage, k, over_side):
        copy = part_copy(stage, k, over_side, k ^ over_side)
        copy.start()
        started.append(copy)

    def part_wait(stage, k, over_side):
        part_copy(stage, k, over_side, k).wait_recv()

    def contract(stage, lhs, weight, row, fresh, order, finish, relay=None):
        def multiply(k):
            if fresh is not None:
                need_piece(fresh, k)
                if fresh == down_kind:
                    need_piece(scales, k)
            f = sources[k]
            part = dot(lhs[...], weight[f]) * cols_full[f, 8 * row : 8 * row + 1, :]
            own_part[k] = part[:rows]
            far_part[k] = part[2 * rows : 3 * rows]
            tp_out[stage, k, 0] = part[rows : 2 * rows].astype(bf16)
            tp_out[stage, k, 1] = part[3 * rows :].astype(bf16)
            part_start(stage, k, 0)

        def pass_on(k):
            part_wait(stage, k, 0)
            rep_out[stage, k] = (far_part[k] + tp_in[stage, k, 1].astype(f32)).astype(bf16)
            part_start(stage, k, 1)

        def collect(k):
            part_wait(stage, k, 1)
            total = own_part[k] + tp_in[stage, k, 0].astype(f32) + rep_in[stage, k].astype(f32)
            finish(k, sources[k], total)

        actions = {"m": multiply, "p": pass_on, "c": collect, "r": relay, "u": pump}
        for action, k in order:
            actions[action](k)

    def lagged(hooks):
        order = []
        for step in range(n + 3):
            if step in hooks:
                order.append(("u", hooks[step]))
            for action, lag in (("m", 0), ("p", 1), ("c", 3)):
                if 0 <= step - lag < n:
                    order.append((action, step - lag))
        return order

    def first_order():
        order = [("m", 0), ("m", 1), ("p", 0), ("p", 1), ("u", 4)]
        for k in range(2, n):
            if k == 2 * (line - 1):
                order.append(("u", 2))
            order.append(("m", k))
            if k > 2:
                order.append(("p", k - 1))
        order.append(("p", n - 1))
        return order + [("c", k) for k in range(n)]

    def tail_order():
        order, waiting, relayed = [], [], []

        def advance(r):
            ks = (2 * r, 2 * r + 1)
            order.extend([("m", k) for k in ks] + [("p", k) for k in ks])
            waiting.append(ks)

        def take():
            if waiting:
                ks = waiting.pop(0)
                order.extend(("c", k) for k in ks)
                relayed.append(ks)

        advance(0)
        advance(1)
        for r in range(2, line):
            for _ in range(1 if r == 2 else 2):
                order.append(("u", 1))
                if len(waiting) > 0 and r * 2 - len(waiting) < n:
                    take()
            if r > 2:
                advance(r - 1)
        for ks in relayed[:1]:
            order.extend(("r", k) for k in relayed.pop(0))
        advance(line - 1)
        while waiting:
            take()
        for ks in relayed:
            order.extend(("r", k) for k in ks)
        return order

    def need_all(kind):
        for k in range(1, n):
            need_piece(kind, k)

    need_all(0)
    need_all(up_kind)
    expand(0, None, 1, {})

    def add_half(k, f, total):
        cols = columns_of(f)
        stream[:, cols] = stream[:, cols] + 0.5 * total

    contract(0, hidden, down_full, 0, down_kind, first_order(), add_half)

    norm_rows(stream, 1, gathered.at[1])
    share_rows(1)
    pump(middle + 2)
    relay_rows(1)
    pump(2)

    seq_len = 2 * rows
    row = lax.rem(
        lax.broadcasted_iota(jnp.int32, (seq_len, seq_len), 0) + tp * rows, seq_len
    )
    col = lax.rem(
        lax.broadcasted_iota(jnp.int32, (seq_len, seq_len), 1) + tp * rows, seq_len
    )

    def retain(h, hooks):
        places = [
            (query_scale, 0, DK, 1.0),
            (key_scale, DK, DK, 1.0 / math.sqrt(DK)),
            (value_scale, 2 * DK, DV, 1.0),
        ]
        made = []
        for i, (scale, first, size, factor) in enumerate(places):
            span = pl.ds(pl.multiple_of((side * heads + h) * size, 128), size)
            product = dot(gathered[1], head_full[h, :, first : first + size])
            made.append((product * (scale[:, span] * factor)).astype(bf16))
            if i in hooks:
                pump(hooks[i])
        query, keys, values = made
        decay = decay_rate[side * heads + h]
        distance = jnp.abs(row - col).astype(f32)
        weight = jnp.where(
            lax.div(col, BLOCK) <= lax.div(row, BLOCK), jnp.exp(-decay * distance), 0.0
        )
        for s in range(2):
            span = slice(s * seq_len, (s + 1) * seq_len)
            scores = lax.dot_general(
                query[span], keys[span], (((1,), (1,)), ((), ())), preferred_element_type=f32
            )
            scores = (scores * weight).astype(bf16)
            retained = dot(scores, values[span])
            centred = retained - jnp.mean(retained, axis=-1, keepdims=True)
            spread = jnp.mean(centred * centred, axis=-1, keepdims=True)
            mixed[span, h * DV : (h + 1) * DV] = (
                centred * lax.rsqrt(spread + EPSILON) * head_gain[...]
            ).astype(bf16)

    for h in range(heads):
        if h == 0:
            wait_rows(1, 0, 1)
            wait_rows(1, 2, 3)
        need_all(down_kind + 1 + h)
        retain(h, {1: 1})
        if h < heads - 1:
            pump(middle - 3 + 6)

    last = gathered.at[2]

    def block_copy(k, i, start):
        cols = columns_of(sources[k])
        a, b, peer = ((0, 1, tp_peer), (0, 2, side_peer), (2, 3, tp_peer))[i]
        return pltpu.make_async_remote_copy(
            src_ref=last.at[slot(a, cols)],
            dst_ref=last.at[slot(b, cols)],
            send_sem=block_send.at[3 * k + i],
            recv_sem=block_recv.at[3 * (k ^ 1 if i == 1 and start else k) + i],
            device_id=peer,
            device_id_type=MESH,
        )

    def factor_copy(i):
        a, b, peer = ((0, 1, tp_peer), (0, 2, side_peer), (2, 3, tp_peer))[i]
        return pltpu.make_async_remote_copy(
            src_ref=factors.at[a],
            dst_ref=factors.at[b],
            send_sem=block_send.at[3 * n + i],
            recv_sem=block_recv.at[3 * n + i],
            device_id=peer,
            device_id_type=MESH,
        )

    squares[...] = jnp.zeros_like(squares)

    def add_mix(k, f, total):
        cols = columns_of(f)
        second = stream[:, cols] + total
        stream[:, cols] = second
        last[slot(0, cols)] = (second * norm_gains[2:3, cols]).astype(bf16)
        square = second * second
        added = squares[...]
        for i in range(width // 128):
            added = added + square[:, i * 128 : (i + 1) * 128]
        squares[...] = added
        for i in (0, 1):
            copy = block_copy(k, i, True)
            copy.start()
            started.append(copy)
        if k == n - 1:
            mean = jnp.sum(added, axis=-1, keepdims=True) / features
            wide = jnp.broadcast_to(lax.rsqrt(mean + EPSILON), (rows, rows))
            factors[0] = wide.T[:8, :]
            for i in (0, 1):
                copy = factor_copy(i)
                copy.start()
                started.append(copy)

    def relay_block(k):
        block_copy(k, 1, False).wait_recv()
        copy = block_copy(k, 2, True)
        copy.start()
        started.append(copy)
        if k == n - 1:
            factor_copy(1).wait_recv()
            copy = factor_copy(2)
            copy.start()
            started.append(copy)

    contract(1, mixed, out_full, 1, out_kind, tail_order(), add_mix, relay_block)
    for k in range(n):
        block_copy(k, 0, False).wait_recv()
        block_copy(k, 2, False).wait_recv()
    factor_copy(0).wait_recv()
    factor_copy(2).wait_recv()
    factor = jnp.concatenate(
        [jnp.broadcast_to(factors[j, 0:1, :], (rows, rows)).T[:, 0:1] for j in range(4)], axis=0
    )
    expand(2, factor, 1, {})

    def write(k, f, total):
        cols = columns_of(f)
        result[:, cols] = (stream[:, cols] + 0.5 * total).astype(bf16)

    contract(2, hidden, down_full, 0, None, lagged({}), write)
    assert not queue
    for finish in sending.values():
        finish()
    for copy in started:
        copy.wait_send()


def fused(
    n_rep,
    n_fs,
    n_tp,
    tokens_in,
    norm_gains,
    gate_w,
    gate_scale,
    up_w,
    up_scale,
    down_w,
    down_scale,
    query_w,
    query_scale,
    key_w,
    key_scale,
    value_w,
    value_scale,
    out_w,
    out_scale,
    head_gain,
    decay_rate,
):
    f32, bf16 = jnp.float32, jnp.bfloat16
    n = n_fs
    rows, features = tokens_in.shape
    width, units = gate_w.shape[0], gate_w.shape[1] // 2
    heads = decay_rate.shape[0] // 2
    kinds = heads + 5
    span_of = n - 2
    any_space = pl.BlockSpec(memory_space=pl.ANY)
    vmem = pl.BlockSpec(memory_space=pltpu.VMEM)
    smem = pl.BlockSpec(memory_space=pltpu.SMEM)
    dma = pltpu.SemaphoreType.DMA

    return pl.pallas_call(
        functools.partial(layer_kernel, n),
        out_shape=pltpu.VMEM((rows, features), bf16),
        in_specs=[any_space] * 17 + [smem],
        out_specs=vmem,
        scratch_shapes=[
            pltpu.VMEM(norm_gains.shape, f32),
        ]
        + [
            pltpu.VMEM((1, x.shape[0]), f32)
            for x in (
                gate_scale,
                up_scale,
                down_scale,
                query_scale,
                key_scale,
                value_scale,
                out_scale,
                head_gain,
            )
        ]
        + [
            pltpu.VMEM((rows, features), bf16),
            pltpu.VMEM((2, width, units), f32),
            pltpu.VMEM((2, width, units), f32),
            pltpu.VMEM((2, units, width), f32),
            pltpu.VMEM((2, width, heads * DK), f32),
            pltpu.VMEM((2, width, heads * DK), f32),
            pltpu.VMEM((2, width, heads * DV), f32),
            pltpu.VMEM((2, heads * DV, width), f32),
            pltpu.VMEM((width, units), bf16),
            pltpu.VMEM((width, units), bf16),
            pltpu.VMEM((units, width), bf16),
            pltpu.VMEM((heads, width, 2 * DK + DV), bf16),
            pltpu.VMEM((heads * DV, width), bf16),
            pltpu.VMEM((16, width), f32),
            pltpu.VMEM((features, units), bf16),
            pltpu.VMEM((features, units), bf16),
            pltpu.VMEM((n, units, width), bf16),
            pltpu.VMEM((heads, features, 2 * DK + DV), bf16),
            pltpu.VMEM((n, heads * DV, width), bf16),
            pltpu.VMEM((n, 16, width), f32),
            pltpu.VMEM((3, 4 * rows, features), bf16),
            pltpu.VMEM((4, 8, rows), f32),
            pltpu.VMEM((rows, features), f32),
            pltpu.VMEM((rows, 128), f32),
            pltpu.VMEM((4 * rows, units), bf16),
            pltpu.VMEM((4 * rows, heads * DV), bf16),
            pltpu.VMEM((n, rows, width), f32),
            pltpu.VMEM((n, rows, width), f32),
            pltpu.VMEM((3, n, 2, rows, width), bf16),
            pltpu.VMEM((3, n, 2, rows, width), bf16),
            pltpu.VMEM((3, n, rows, width), bf16),
            pltpu.VMEM((3, n, rows, width), bf16),
            dma((24,)),
            dma((kinds + 2,)),
            dma((kinds + 2,)),
            dma((9 * span_of,)),
            dma((kinds * span_of,)),
            dma((kinds * span_of,)),
            dma((3 * n * 2,)),
            dma((3 * n * 2,)),
            dma((6,)),
            dma((6,)),
            dma((3 * n + 3,)),
            dma((3 * n + 3,)),
        ],
        compiler_params=pltpu.CompilerParams(
            collective_id=0, has_side_effects=True, vmem_limit_bytes=VMEM_LIMIT
        ),
        name="layer",
    )(
        tokens_in,
        norm_gains,
        gate_w,
        gate_scale,
        up_w,
        up_scale,
        down_w,
        down_scale,
        query_w,
        query_scale,
        key_w,
        key_scale,
        value_w,
        value_scale,
        out_w,
        out_scale,
        head_gain,
        decay_rate,
    )


def solution(mesh):
    sizes = [mesh.shape[axis] for axis in ("rep", "fs", "tp")]
    placed = (
        P(("rep", "fs", "tp"), None),
        P(),
        P("fs", "tp"),
        P("tp"),
        P("fs", "tp"),
        P("tp"),
        P("tp", "fs"),
        P("fs"),
        P("fs", "tp"),
        P("tp"),
        P("fs", "tp"),
        P("tp"),
        P("fs", "tp"),
        P("tp"),
        P("tp", "fs"),
        P("fs"),
        P(),
        P("tp"),
    )
    return jax.shard_map(
        lambda *args: (fused if fits(*sizes, *args) else on_device)(*sizes, *args),
        mesh=mesh,
        in_specs=placed,
        out_specs=P(("rep", "fs", "tp"), None),
        check_vma=False,
    )
```

```python
import functools
import math

import jax
import jax.numpy as jnp
from jax import lax
from jax.experimental import pallas as pl
from jax.experimental.pallas import tpu as pltpu
from jax.sharding import PartitionSpec as P

DK = 256
DV = 256
BLOCK = 64

EPSILON = 1e-05


def rms_scale(stream, gain):
    return stream * lax.rsqrt(jnp.mean(stream * stream, axis=-1, keepdims=True) + EPSILON) * gain


def snake(n):
    return [i for i in range(0, n, 2)] + [i for i in range(n - 1, 0, -1) if i % 2 == 1]


def snake_place(index, n):
    return jnp.where(index % 2 == 0, index // 2, n - 1 - index // 2)


def snake_index(place, n):
    half = (n + 1) // 2
    return jnp.where(place < half, 2 * place, 2 * (n - 1 - place) + 1)


def shift(x, axis, n, by):
    return lax.ppermute(x, axis, [(i, (i + by) % n) for i in range(n)])


def ring_gather(shards, n, forward_steps):
    order = snake(n)
    ahead = [(order[i], order[(i + 1) % n]) for i in range(n)]
    behind = [(b, a) for a, b in ahead]
    found = []
    for x, steps in zip(shards, forward_steps):
        forward, back = [x], [x]
        found.append((forward, back))
    for step in range(n):
        for (forward, back), steps in zip(found, forward_steps):
            if step < steps:
                forward.append(lax.ppermute(forward[-1], "fs", ahead))
            if step < n - 1 - steps:
                back.append(lax.ppermute(back[-1], "fs", behind))
    return [forward + back[:0:-1] for forward, back in found]


def chained(shards, before, hops):
    if not before:
        return shards
    last = []
    n = len(before[0])
    for pieces in before:
        last.extend([pieces[hops], pieces[n - hops]])
    return lax.optimization_barrier((tuple(shards), tuple(last)))[0]


def with_scale(weight, scale):
    high = lax.reduce_precision(scale, 8, 7)
    middle = lax.reduce_precision(scale - high, 8, 7)
    rows = jnp.stack([high, middle, scale - high - middle]).astype(jnp.bfloat16)
    return jnp.concatenate([weight, jnp.pad(rows, ((0, 13), (0, 0)))], axis=0)


def without_scale(pieces):
    size = pieces[0].shape[0] - 16
    weight = jnp.concatenate([p[:size] for p in pieces], axis=1)
    rows = jnp.concatenate([p[size:] for p in pieces], axis=1)[:3].astype(jnp.float32)
    return weight, rows[0] + rows[1] + rows[2]


def retain(query, key_rows, value, decay, head_gain):
    seq_len = query.shape[0]
    row = lax.broadcasted_iota(jnp.int32, (seq_len, seq_len), 0)
    col = lax.broadcasted_iota(jnp.int32, (seq_len, seq_len), 1)
    distance = jnp.abs(row - col).astype(jnp.float32)
    weight = jnp.where(col // BLOCK <= row // BLOCK, jnp.exp(-decay * distance), 0.0)
    scores = lax.dot_general(
        query, key_rows, (((1,), (1,)), ((), ())), preferred_element_type=jnp.float32
    )
    scores = (scores * weight).astype(jnp.bfloat16)
    retained = jnp.dot(scores, value, preferred_element_type=jnp.float32)
    centred = retained - jnp.mean(retained, axis=-1, keepdims=True)
    normed = (
        centred
        * lax.rsqrt(jnp.mean(centred * centred, axis=-1, keepdims=True) + EPSILON)
        * head_gain
    )
    return normed.astype(jnp.bfloat16)


def on_device(
    n_rep,
    n_fs,
    n_tp,
    tokens_in,
    norm_gains,
    gate_w,
    gate_scale,
    up_w,
    up_scale,
    down_w,
    down_scale,
    query_w,
    query_scale,
    key_w,
    key_scale,
    value_w,
    value_scale,
    out_w,
    out_scale,
    head_gain,
    decay_rate,
):
    rows = tokens_in.shape[0]
    width = gate_w.shape[0]
    heads = decay_rate.shape[0]
    units = gate_w.shape[1]
    share = n_rep if heads % n_rep == 0 and units % (n_rep * 128) == 0 else 1
    heads //= share
    units //= share
    rep = lax.axis_index("rep") if share > 1 else 0
    tp = lax.axis_index("tp")
    place = snake_place(lax.axis_index("fs"), n_fs)

    def part(x, axis):
        size = x.shape[axis] // share
        return lax.dynamic_slice_in_dim(x, rep * size, size, axis)

    gate_b, up_b, query_b, key_b, value_b = (
        part(w, 1).astype(jnp.bfloat16) for w in (gate_w, up_w, query_w, key_w, value_w)
    )
    down_b, out_b = (part(w, 0).astype(jnp.bfloat16) for w in (down_w, out_w))

    few, many = (n_fs - 1) // 2, n_fs // 2
    first_pieces = ring_gather([gate_b, up_b], n_fs, [many, few])
    half = down_b.shape[0] // 2
    second_pieces = ring_gather(
        chained([with_scale(down_b[:half], down_scale), down_b[half:]], first_pieces, max(1, n_fs // 4)),
        n_fs,
        [many, few],
    )
    third_pieces = ring_gather(chained([query_b, key_b], second_pieces, few), n_fs, [many, few])
    value_pieces, out_pieces = ring_gather(
        chained([value_b, with_scale(out_b, out_scale)], third_pieces, few), n_fs, [many, few]
    )

    gate_full, up_full = (jnp.concatenate(p, axis=0) for p in first_pieces)
    down_top, down_cols = without_scale(second_pieces[0])
    down_rest = jnp.concatenate(second_pieces[1], axis=1)
    down_full = lax.optimization_barrier(jnp.concatenate([down_top, down_rest], axis=0))
    query_full, key_full = (jnp.concatenate(p, axis=0) for p in third_pieces)
    value_full = jnp.concatenate(value_pieces, axis=0)
    out_full, out_cols = without_scale(out_pieces)

    def to_ring(x):
        blocks = [
            lax.dynamic_slice_in_dim(
                x, snake_index((place - k) % n_fs, n_fs) * width, width, axis=1
            )
            for k in range(n_fs)
        ]
        return jnp.concatenate(blocks, axis=1)

    def from_ring(x):
        blocks = [
            lax.dynamic_slice_in_dim(x, (place - snake(n_fs).index(o)) % n_fs * width, width, axis=1)
            for o in range(n_fs)
        ]
        return jnp.concatenate(blocks, axis=1)

    def over_tp(x, ordered):
        found = [x] + [shift(x, "tp", n_tp, k) for k in range(1, n_tp)]
        if not ordered:
            return jnp.concatenate(found, axis=0)
        twice = jnp.concatenate(found[::-1] * 2, axis=0)
        return lax.dynamic_slice_in_dim(twice, (n_tp - 1 - tp) * rows, n_tp * rows, axis=0)

    def gather_rows(normed, ordered=False):
        found = [normed] + [shift(normed, "rep", n_rep, k) for k in range(1, share)]
        return [over_tp(x, ordered) for x in found]

    def return_rows(parts, ordered=False):
        total = None
        for k in range(share - 1, -1, -1):

            def block(j):
                at = (tp - j) % n_tp * rows if ordered else j * rows
                return lax.dynamic_slice_in_dim(parts[k], at, rows, axis=0)

            mine = block(0)
            for j in range(1, n_tp):
                other = shift(block(j).astype(jnp.bfloat16), "tp", n_tp, n_tp - j)
                mine = mine + other.astype(jnp.float32)
            if k > 0:
                mine = shift(mine.astype(jnp.bfloat16), "rep", n_rep, n_rep - k).astype(jnp.float32)
            total = mine if total is None else total + mine
        return total

    def dot(a, b):
        return jnp.dot(a, b, preferred_element_type=jnp.float32)

    gate_col, up_col = part(gate_scale, 0), part(up_scale, 0)

    def feed_forward(stream, gain):
        parts = []
        for gathered in gather_rows(rms_scale(stream, gain).astype(jnp.bfloat16)):
            gate_value = dot(gathered, gate_full) * gate_col
            up_value = dot(gathered, up_full) * up_col
            hidden = (jax.nn.silu(gate_value) * up_value).astype(jnp.bfloat16)
            hidden = lax.optimization_barrier(hidden)
            parts.append(dot(hidden, down_full) * down_cols)
        return return_rows(parts)

    query_col, key_col, value_col = (part(s, 0) for s in (query_scale, key_scale, value_scale))
    decay = part(decay_rate, 0)
    gains = to_ring(norm_gains)

    stream = to_ring(tokens_in).astype(jnp.float32)
    stream = stream + 0.5 * feed_forward(stream, gains[0])
    parts = []
    for gathered in gather_rows(
        rms_scale(stream, gains[1]).astype(jnp.bfloat16), ordered=True
    ):
        query = (dot(gathered, query_full) * query_col).astype(jnp.bfloat16)
        key_rows = (dot(gathered, key_full) * key_col / math.sqrt(DK)).astype(jnp.bfloat16)
        value = (dot(gathered, value_full) * value_col).astype(jnp.bfloat16)
        mixed = [
            retain(
                query[:, h * DK : (h + 1) * DK],
                key_rows[:, h * DK : (h + 1) * DK],
                value[:, h * DV : (h + 1) * DV],
                decay[h],
                head_gain,
            )
            for h in range(heads)
        ]
        parts.append(dot(jnp.concatenate(mixed, axis=1), out_full) * out_cols)
    stream = stream + return_rows(parts, ordered=True)
    stream = stream + 0.5 * feed_forward(stream, gains[2])
    return from_ring(stream.astype(jnp.bfloat16))


MESH = pl.DeviceIdType.MESH
VMEM_LIMIT = 62 * 1024 * 1024


def fits(n_rep, n_fs, n_tp, tokens_in, norm_gains, gate_w, *rest):
    rows, features = tokens_in.shape
    width, units = gate_w.shape
    heads = rest[-1].shape[0]
    return (
        n_rep == 2
        and n_tp == 2
        and n_fs >= 6
        and n_fs % 2 == 0
        and n_fs <= 16
        and rows % 128 == 0
        and width % 256 == 0
        and features == n_fs * width
        and units % 512 == 0
        and heads % 2 == 0
    )


def layer_kernel(
    n,
    tokens_in,
    norm_gains_in,
    gate_w,
    gate_scale_in,
    up_w,
    up_scale_in,
    down_w,
    down_scale_in,
    query_w,
    query_scale_in,
    key_w,
    key_scale_in,
    value_w,
    value_scale_in,
    out_w,
    out_scale_in,
    head_gain_in,
    decay_rate,
    result,
    norm_gains,
    gate_scale,
    up_scale,
    down_scale,
    query_scale,
    key_scale,
    value_scale,
    out_scale,
    head_gain,
    staged_in,
    staged_gate,
    staged_up,
    staged_down,
    staged_query,
    staged_key,
    staged_value,
    staged_out,
    gate_away,
    up_away,
    down_away,
    head_away,
    out_away,
    cols_away,
    gate_full,
    up_full,
    down_full,
    head_full,
    out_full,
    cols_full,
    gathered,
    factors,
    stream,
    squares,
    summed,
    hidden,
    mixed,
    own_part,
    far_part,
    tp_out,
    tp_in,
    rep_out,
    rep_in,
    local_sem,
    side_send,
    side_recv,
    line_send,
    line_recv,
    twin_recv,
    part_send,
    part_recv,
    row_send,
    row_recv,
    block_send,
    block_recv,
):
    f32, bf16 = jnp.float32, jnp.bfloat16
    rows, features = tokens_in.shape
    width = gate_w.shape[0]
    units = hidden.shape[1]
    heads = head_full.shape[0]
    tile = 256

    twin, fs, tp = (lax.axis_index(axis) for axis in ("rep", "fs", "tp"))
    line = n // 2
    side, spot = lax.rem(fs, 2), lax.div(fs, 2)
    above, below = {"fs": fs + 2}, {"fs": fs - 2}
    side_peer, twin_peer, tp_peer = {"fs": fs + 1 - 2 * side}, {"rep": 1 - twin}, {"tp": 1 - tp}
    has_above, has_below = spot + 1 < line, spot > 0

    barrier = pltpu.get_barrier_semaphore()

    def greet(peer):
        pl.semaphore_signal(barrier, inc=1, device_id=peer, device_id_type=MESH)

    def meet():
        for peer in (side_peer, twin_peer, tp_peer):
            greet(peer)
        pl.when(has_above)(lambda: greet(above))
        pl.when(has_below)(lambda: greet(below))

    def columns_of(f):
        return pl.ds(pl.multiple_of(f * width, width), width)

    def halves(size):
        return [pl.ds(pl.multiple_of(i * size, 128), size) for i in (side, 1 - side)]

    local, copies_of = [], {}

    def fetch(name, src, dst):
        copy = pltpu.make_async_copy(src, dst, local_sem.at[len(local)])
        copy.start()
        copies_of.setdefault(name, []).append(copy)
        local.append(copy)

    def fetched(name):
        for copy in copies_of[name]:
            copy.wait()

    gate_halves = halves(units)
    fetch(("gate", 0), gate_w.at[:, gate_halves[0]], staged_gate.at[0])
    meet()
    fetch(("gate", 1), gate_w.at[:, gate_halves[1]], staged_gate.at[1])
    for i, cols in enumerate(halves(units)):
        fetch(("up", i), up_w.at[:, cols], staged_up.at[i])
    fetch("rows", tokens_in, staged_in)
    for src, dst in (
        (gate_scale_in, gate_scale),
        (up_scale_in, up_scale),
        (down_scale_in, down_scale),
        (query_scale_in, query_scale),
        (key_scale_in, key_scale),
        (value_scale_in, value_scale),
        (out_scale_in, out_scale),
        (head_gain_in, head_gain),
    ):
        fetch("small", src, dst.at[0])
    fetch("small", norm_gains_in, norm_gains)
    for i, cols in enumerate(halves(units)):
        fetch("down", down_w.at[cols, :], staged_down.at[i])
    for i, cols in enumerate(halves(heads * DK)):
        fetch("heads", query_w.at[:, cols], staged_query.at[i])
        fetch("heads", key_w.at[:, cols], staged_key.at[i])
    for i, cols in enumerate(halves(heads * DV)):
        fetch("heads", value_w.at[:, cols], staged_value.at[i])
        fetch("out", out_w.at[cols, :], staged_out.at[i])

    started = []
    half_units, half_width, half_out = units // 2, width // 2, heads * DV // 2

    def rows_of(f):
        return pl.ds(pl.multiple_of(f * width, width), width)

    def cut(ref, s, size):
        return ref.at[pl.ds(pl.multiple_of(s * size, size), size), :]

    kinds = [
        (lambda f: gate_full.at[rows_of(f), :], gate_away, half_width),
        (lambda f: up_full.at[rows_of(f), :], up_away, half_width),
        (lambda f: down_full.at[f], down_away, half_units),
    ]
    for h in range(heads):
        kinds.append(
            (lambda f, h=h: head_full.at[h, rows_of(f), :], head_away.at[h], half_width)
        )
    kinds.append((lambda f: out_full.at[f], out_away, half_out))
    scales = len(kinds)
    kinds.append((lambda f: cols_full.at[f], cols_away, 8))
    up_kind, down_kind, out_kind = 1, 2, scales - 1

    def piece(kind, f, s):
        return cut(kinds[kind][0](f), s, kinds[kind][2])

    def remote(src, dst, send_sem, recv_sem, peer):
        return pltpu.make_async_remote_copy(
            src_ref=src,
            dst_ref=dst,
            send_sem=send_sem,
            recv_sem=recv_sem,
            device_id=peer,
            device_id_type=MESH,
        )

    def across(o):
        return spot * 2 + side + o * (1 - 2 * side)

    def side_slot(kind, i):
        return kind * 2 + i if kind <= up_kind else kind + 2

    def side_copy(kind, i, f):
        slot_of = side_slot(kind, i)
        sems = side_send.at[slot_of], side_recv.at[slot_of]
        if kind <= up_kind:
            s = twin if i == 0 else 1 - twin
            return remote(
                cut(kinds[kind][1], s, kinds[kind][2]), piece(kind, f, s), *sems, side_peer
            )
        return remote(kinds[kind][1], kinds[kind][0](f), *sems, side_peer)

    def side_start(kind, i=0):
        copy = side_copy(kind, i, fs)
        copy.start()
        started.append(copy)

    side_done = set()

    def side_need(kind, i):
        i = i if kind <= up_kind else 0
        if (kind, i) not in side_done:
            side_done.add((kind, i))
            side_copy(kind, i, across(1)).wait_recv()

    span_of = 2 * (line - 1)
    sending = {}

    def push(kind, group, index, f, where, recv, peer):
        bank = 1 if kind == scales else kind % 2
        slot_of = (bank * 3 + group) * span_of + index
        copy = remote(piece(kind, f, twin), piece(kind, f, twin), line_send.at[slot_of], recv, peer)
        if slot_of in sending:
            sending.pop(slot_of)()
        guard = functools.partial(pl.when, where) if where is not None else None

        def begin():
            copy.start()

        def finish():
            copy.wait_send()

        if guard is None:
            begin()
            sending[slot_of] = finish
        else:
            guard()(begin)
            sending[slot_of] = lambda: guard()(finish)

    def line_slot(kind, away, o):
        return line_recv.at[kind * span_of + (away % line - 1) * 2 + o]

    def twin_slot(kind, away, o):
        return twin_recv.at[kind * span_of + (away - 1) * 2 + o]

    def send_own(kind, o):
        if o == 1:
            side_need(kind, 0)
        f = across(o)
        push(kind, 0, o, f, has_above, line_slot(kind, -1, o), above)
        push(kind, 1, o, f, has_below, line_slot(kind, 1, o), below)

    def places(d, o):
        for group, away in ((0, -d), (1, d)):
            from_spot = spot + away
            exists = from_spot >= 0 if away < 0 else from_spot < line
            yield group, away, exists, from_spot * 2 + side + o * (1 - 2 * side)

    def take_in(kind, d, o):
        for group, away, exists, f in places(d, o):

            def receive(kind=kind, away=away, f=f):
                remote(
                    piece(kind, f, twin),
                    piece(kind, f, twin),
                    line_send.at[0],
                    line_slot(kind, away, o),
                    above,
                ).wait_recv()

            pl.when(exists)(receive)
            hand_over(kind, away, o, f, exists)

    def move_on(kind, d, o):
        if d > line - 2:
            return
        for group, away, exists, f in places(d, o):
            further = -d - 1 if away < 0 else d + 1
            push(
                kind,
                group,
                2 * d + o,
                f,
                jnp.logical_and(exists, has_above if away < 0 else has_below),
                line_slot(kind, further, o),
                above if away < 0 else below,
            )

    def pass_along(kind, d, o):
        take_in(kind, d, o)
        move_on(kind, d, o)

    def hand_over(kind, away, o, f, exists):
        index = (away % line - 1) * 2 + o
        bank = 1 if kind == scales else kind % 2
        slot_of = (bank * 3 + 2) * span_of + index
        first = away > 0
        copy = remote(
            piece(kind, f, twin),
            piece(kind, f, twin),
            line_send.at[slot_of],
            twin_slot(kind, away % line, o),
            twin_peer,
        )
        key = (slot_of, first)
        if key in sending:
            sending.pop(key)()
        pl.when(exists)(lambda: copy.start())
        sending[key] = lambda: pl.when(exists)(lambda: copy.wait_send())

    def pick(table):
        total = 0
        for v in range(line):
            total = total + (spot == v).astype(jnp.int32) * table[v]
        return total

    near = []
    for v in range(line):
        near.append(sorted((u for u in range(line) if u != v), key=lambda u: (abs(u - v), -u)))
    sources = [across(0), across(1)]
    twin_index = [None, None]
    for r in range(line - 1):
        at = pick([near[v][r] for v in range(line)])
        away = pick([(near[v][r] - v) % line for v in range(line)])
        for o in range(2):
            sources.append(at * 2 + side + o * (1 - 2 * side))
            twin_index.append((away - 1) * 2 + o)

    def need_piece(kind, k):
        if k == 1:
            side_need(kind, 0)
            side_need(kind, 1)
        if k > 1:
            remote(
                piece(kind, sources[k], 1 - twin),
                piece(kind, sources[k], 1 - twin),
                line_send.at[0],
                twin_recv.at[kind * span_of + twin_index[k]],
                twin_peer,
            ).wait_recv()

    queue = []
    later = []
    for members in [[0, up_kind], [down_kind, scales]] + [[k] for k in range(down_kind + 1, scales)]:
        for o in range(2):
            queue.append([functools.partial(send_own, m, o) for m in members])
        queue.extend(later)
        later = []
        for d in range(1, line):
            for o in range(2):
                unit = [functools.partial(pass_along, m, d, o) for m in members]
                (queue if d < line - 1 else later).append(unit)
    queue.extend(later)
    middle = 2 * (line - 2)

    def pump(count):
        for _ in range(count):
            for action in queue.pop(0):
                action()

    def send(src, dst, send_sem, recv_sem, peer):
        copy = remote(src, dst, send_sem, recv_sem, peer)
        copy.start()
        started.append(copy)
        return copy

    own_rows = rows_of(fs)
    fetched(("gate", 0))
    gate_full[own_rows, :] = staged_gate[0].astype(bf16)
    neighbours = has_above.astype(jnp.int32) + has_below.astype(jnp.int32)
    pl.semaphore_wait(barrier, 3 + neighbours)
    first, second, _ = (queue.pop(0) for _ in range(3))
    first[0]()
    fetched(("gate", 1))
    gate_away[...] = staged_gate[1].astype(bf16)
    side_start(0)
    fetched(("up", 0))
    up_full[own_rows, :] = staged_up[0].astype(bf16)
    first[1]()
    fetched(("up", 1))
    up_away[...] = staged_up[1].astype(bf16)
    side_start(up_kind)
    fetched("rows")
    fetched("small")

    def norm_rows(source, which, target):
        gain = norm_gains[which : which + 1, :]

        def step(i, carry):
            block = pl.ds(pl.multiple_of(i * 16, 16), 16)
            x = source[block, :].astype(f32)
            mean = jnp.mean(x * x, axis=-1, keepdims=True)
            target[block, :] = (x * lax.rsqrt(mean + EPSILON) * gain).astype(bf16)
            return carry

        lax.fori_loop(0, rows // 16, step, 0)

    def slot(j, cols=slice(None)):
        return (pl.ds(j * rows, rows), cols)

    def share_rows(stage):
        part = gathered.at[stage]
        base = 3 * stage
        send(part.at[slot(0)], part.at[slot(1)], row_send.at[base], row_recv.at[base], tp_peer)
        send(
            part.at[slot(0)],
            part.at[slot(2)],
            row_send.at[base + 1],
            row_recv.at[base + 1],
            side_peer,
        )

    def wait_rows(stage, i, j):
        part = gathered.at[stage]
        pltpu.make_async_remote_copy(
            src_ref=part.at[slot(0)],
            dst_ref=part.at[slot(j)],
            send_sem=row_send.at[3 * stage + i],
            recv_sem=row_recv.at[3 * stage + i],
            device_id=tp_peer,
            device_id_type=MESH,
        ).wait_recv()

    def relay_rows(stage):
        wait_rows(stage, 1, 2)
        part = gathered.at[stage]
        send(
            part.at[slot(2)],
            part.at[slot(3)],
            row_send.at[3 * stage + 2],
            row_recv.at[3 * stage + 2],
            tp_peer,
        )

    norm_rows(staged_in, 0, gathered.at[0])
    stream[...] = staged_in[...].astype(f32)
    fetched("down")
    down_full[fs] = staged_down[0].astype(bf16)
    down_away[...] = staged_down[1].astype(bf16)
    cols_full[fs, 0:1, :] = down_scale[...]
    cols_full[fs, 8:9, :] = out_scale[...]
    cols_away[0:1, :] = down_scale[...]
    cols_away[8:9, :] = out_scale[...]
    side_start(0, 1)
    side_start(up_kind, 1)
    side_start(down_kind)
    side_start(scales)
    take_in(0, 1, 0)
    second[0]()
    take_in(up_kind, 1, 0)
    second[1]()
    move_on(0, 1, 0)
    move_on(up_kind, 1, 0)
    share_rows(0)
    fetched("heads")
    for h in range(heads):
        keys, vals = slice(h * DK, (h + 1) * DK), slice(h * DV, (h + 1) * DV)
        for i in range(2):
            made = jnp.concatenate(
                [staged_query[i, :, keys], staged_key[i, :, keys], staged_value[i, :, vals]], axis=1
            ).astype(bf16)
            if i == 0:
                head_full[h, own_rows, :] = made
            else:
                head_away[h] = made
        side_start(down_kind + 1 + h)
    fetched("out")
    out_full[fs] = staged_out[0].astype(bf16)
    out_away[...] = staged_out[1].astype(bf16)
    side_start(out_kind)

    pump(middle + 2)
    relay_rows(0)
    pump(middle + 1)
    wait_rows(0, 0, 1)
    wait_rows(0, 2, 3)

    def dot(a, b):
        return jnp.dot(a, b, preferred_element_type=f32)

    def expand(stage, factor, part):
        for c in range(units // tile):
            cols = slice(c * tile, (c + 1) * tile)
            span = pl.ds(pl.multiple_of(side * units + c * tile, 128), tile)
            rows_in, lhs = part
            gate = dot(lhs, gate_full[rows_in, cols])
            up = dot(lhs, up_full[rows_in, cols])
            if factor is not None:
                gate = (gate + summed[0, :, cols]) * factor
                up = (up + summed[1, :, cols]) * factor
            gate, up = gate * gate_scale[:, span], up * up_scale[:, span]
            hidden[:, cols] = (gate / (1.0 + jnp.exp(-gate)) * up).astype(bf16)

    def part_copy(stage, k, over_side, landing):
        store_out, store_in = (rep_out, rep_in) if over_side else (tp_out, tp_in)
        return remote(
            store_out.at[stage, k],
            store_in.at[stage, landing],
            part_send.at[stage * 2 + over_side],
            part_recv.at[landing * 2 + over_side],
            side_peer if over_side else tp_peer,
        )

    def part_start(stage, k, over_side):
        part_copy(stage, k, over_side, k ^ over_side).start()

    def part_wait(stage, k, over_side):
        part_copy(stage, k, over_side, k).wait_recv()

    def parts_sent(stage):
        for over_side, (src, dst) in enumerate(((tp_out, tp_in), (rep_out, rep_in))):
            remote(
                src.at[stage],
                dst.at[stage],
                part_send.at[stage * 2 + over_side],
                part_recv.at[0],
                side_peer,
            ).wait_send()

    def contract(stage, lhs, weight, row, fresh, order, finish, relay=None, extra=None):
        def multiply(k):
            if fresh is not None:
                need_piece(fresh, k)
                if fresh == down_kind:
                    need_piece(scales, k)
            f = sources[k]
            part = dot(lhs[...], weight[f]) * cols_full[f, 8 * row : 8 * row + 1, :]
            own_part[k] = part[:rows]
            far_part[k] = part[2 * rows : 3 * rows]
            tp_out[stage, k, 0] = part[rows : 2 * rows].astype(bf16)
            tp_out[stage, k, 1] = part[3 * rows :].astype(bf16)
            part_start(stage, k, 0)

        def pass_on(k):
            part_wait(stage, k, 0)
            rep_out[stage, k] = (far_part[k] + tp_in[stage, k, 1].astype(f32)).astype(bf16)
            part_start(stage, k, 1)

        def collect(k):
            part_wait(stage, k, 1)
            total = own_part[k] + tp_in[stage, k, 0].astype(f32) + rep_in[stage, k].astype(f32)
            finish(k, sources[k], total)

        actions = {"m": multiply, "p": pass_on, "c": collect, "r": relay, "u": pump, "x": extra}
        for action, k in order:
            actions[action](k)

    def last_order():
        order = []
        for k in range(n):
            order.append(("m", k))
            if k > 0:
                order.append(("p", k - 1))
        return order + [("p", n - 1)] + [("c", k) for k in range(n)]

    def first_order():
        order = [("m", 0), ("m", 1), ("p", 0), ("p", 1), ("u", 4)]
        for k in range(2, n):
            if k == 2 * (line - 1):
                order.append(("u", 2))
            order.append(("m", k))
            if k > 2:
                order.append(("p", k - 1))
        order.append(("p", n - 1))
        order += [("c", k) for k in range(n)]
        order.insert(-2, ("u", 1))
        return order

    def tail_order():
        order, waiting, relayed = [], [], []

        def advance(r):
            ks = (2 * r, 2 * r + 1)
            order.extend([("m", k) for k in ks] + [("p", k) for k in ks])
            waiting.append(ks)

        def take():
            if waiting:
                ks = waiting.pop(0)
                order.extend(("c", k) for k in ks)
                relayed.append(ks)

        advance(0)
        order.insert(2, ("u", 1))
        advance(1)
        for r in range(2, line):
            for i in range(2):
                if r > 2:
                    order.append(("u", 1))
                if i == 1 and r == 2:
                    continue
                if len(waiting) > 0 and r * 2 - len(waiting) < n:
                    take()
            if r > 2:
                advance(r - 1)
        for ks in relayed[:1]:
            order.extend(("r", k) for k in relayed.pop(0))
        advance(line - 1)
        while waiting:
            take()
            order.extend(("r", k) for k in relayed.pop(0))
        order.extend(("r", k) for ks in relayed for k in ks)
        for r in range(line - 2):
            order.insert(order.index(("r", 2 * r + 3)) + 1, ("x", r))
        return order

    def need_all(kind):
        for k in range(1, n):
            need_piece(kind, k)

    need_all(0)
    need_all(up_kind)
    expand(0, None, (slice(None), gathered[0]))

    def add_half(k, f, total):
        cols = columns_of(f)
        stream[:, cols] = stream[:, cols] + 0.5 * total

    contract(0, hidden, down_full, 0, down_kind, first_order(), add_half)

    norm_rows(stream, 1, gathered.at[1])
    share_rows(1)
    pump(middle + 1)
    relay_rows(1)
    pump(2)

    seq_len = 2 * rows
    row = lax.rem(
        lax.broadcasted_iota(jnp.int32, (seq_len, seq_len), 0) + tp * rows, seq_len
    )
    col = lax.rem(
        lax.broadcasted_iota(jnp.int32, (seq_len, seq_len), 1) + tp * rows, seq_len
    )

    def retain(h, hooks):
        places = [
            (query_scale, 0, DK, 1.0),
            (key_scale, DK, DK, 1.0 / math.sqrt(DK)),
            (value_scale, 2 * DK, DV, 1.0),
        ]
        made = []
        for i, (scale, first, size, factor) in enumerate(places):
            span = pl.ds(pl.multiple_of((side * heads + h) * size, 128), size)
            product = dot(gathered[1], head_full[h, :, first : first + size])
            made.append((product * (scale[:, span] * factor)).astype(bf16))
            if i in hooks:
                pump(hooks[i])
        query, keys, values = made
        decay = decay_rate[side * heads + h]
        distance = jnp.abs(row - col).astype(f32)
        weight = jnp.where(
            lax.div(col, BLOCK) <= lax.div(row, BLOCK), jnp.exp(-decay * distance), 0.0
        )
        for s in range(2):
            span = slice(s * seq_len, (s + 1) * seq_len)
            scores = lax.dot_general(
                query[span], keys[span], (((1,), (1,)), ((), ())), preferred_element_type=f32
            )
            scores = (scores * weight).astype(bf16)
            retained = dot(scores, values[span])
            centred = retained - jnp.mean(retained, axis=-1, keepdims=True)
            spread = jnp.mean(centred * centred, axis=-1, keepdims=True)
            mixed[span, h * DV : (h + 1) * DV] = (
                centred * lax.rsqrt(spread + EPSILON) * head_gain[...]
            ).astype(bf16)

    for h in range(heads):
        if h == 0:
            wait_rows(1, 0, 1)
            wait_rows(1, 2, 3)
        need_all(down_kind + 1 + h)
        retain(h, {1: 1})
        if h < heads - 1:
            pump(middle - 3 + 6)

    last = gathered.at[2]

    def block_copy(k, i, start):
        cols = columns_of(sources[k])
        a, b, peer = ((0, 1, tp_peer), (0, 2, side_peer), (2, 3, tp_peer))[i]
        return pltpu.make_async_remote_copy(
            src_ref=last.at[slot(a, cols)],
            dst_ref=last.at[slot(b, cols)],
            send_sem=block_send.at[i],
            recv_sem=block_recv.at[3 * (k ^ 1 if i == 1 and start else k) + i],
            device_id=peer,
            device_id_type=MESH,
        )

    def factor_copy(i):
        a, b, peer = ((0, 1, tp_peer), (0, 2, side_peer), (2, 3, tp_peer))[i]
        return pltpu.make_async_remote_copy(
            src_ref=factors.at[a],
            dst_ref=factors.at[b],
            send_sem=block_send.at[3 + i],
            recv_sem=block_recv.at[3 * n + i],
            device_id=peer,
            device_id_type=MESH,
        )

    squares[...] = jnp.zeros_like(squares)

    def add_mix(k, f, total):
        cols = columns_of(f)
        second = stream[:, cols] + total
        stream[:, cols] = second
        last[slot(0, cols)] = (second * norm_gains[2:3, cols]).astype(bf16)
        square = second * second
        added = squares[...]
        for i in range(width // 128):
            added = added + square[:, i * 128 : (i + 1) * 128]
        squares[...] = added
        for i in (0, 1):
            block_copy(k, i, True).start()
        if k == n - 1:
            mean = jnp.sum(added, axis=-1, keepdims=True) / features
            wide = jnp.broadcast_to(lax.rsqrt(mean + EPSILON), (rows, rows))
            factors[0] = wide.T[:8, :]
            for i in (0, 1):
                copy = factor_copy(i)
                copy.start()
                started.append(copy)

    def relay_block(k):
        block_copy(k, 1, False).wait_recv()
        block_copy(k, 2, True).start()
        if k == n - 1:
            factor_copy(1).wait_recv()
            copy = factor_copy(2)
            copy.start()
            started.append(copy)

    spots = [spot] + [lax.div(sources[2 * r], 2) for r in range(1, line)]

    def arrived_block(r):
        for k in (2 * r, 2 * r + 1):
            block_copy(k, 0, False).wait_recv()
            block_copy(k, 2, False).wait_recv()
        return pl.ds(pl.multiple_of(spots[r] * 2 * width, 2 * width), 2 * width)

    def take_sum(r):
        rows_in = arrived_block(r)
        lhs = last[:, rows_in]
        for c in range(units // tile):
            cols = slice(c * tile, (c + 1) * tile)
            for i, weight in enumerate((gate_full, up_full)):
                part = dot(lhs, weight[rows_in, cols])
                summed[i, :, cols] = part if r == 0 else summed[i, :, cols] + part

    contract(1, mixed, out_full, 1, out_kind, tail_order(), add_mix, relay_block, take_sum)
    take_sum(line - 2)
    rows_in = arrived_block(line - 1)
    factor_copy(0).wait_recv()
    factor_copy(2).wait_recv()
    factor = jnp.concatenate(
        [jnp.broadcast_to(factors[j, 0:1, :], (rows, rows)).T[:, 0:1] for j in range(4)], axis=0
    )
    expand(2, factor, (rows_in, last[:, rows_in]))

    def write(k, f, total):
        cols = columns_of(f)
        result[:, cols] = (stream[:, cols] + 0.5 * total).astype(bf16)

    contract(2, hidden, down_full, 0, None, last_order(), write)
    assert not queue
    for stage in range(3):
        parts_sent(stage)
    for i, a in enumerate((0, 0, 2)):
        remote(
            last.at[slot(a)], last.at[slot(a)], block_send.at[i], block_recv.at[0], tp_peer
        ).wait_send()
    for finish in sending.values():
        finish()
    for copy in started:
        copy.wait_send()


def fused(
    n_rep,
    n_fs,
    n_tp,
    tokens_in,
    norm_gains,
    gate_w,
    gate_scale,
    up_w,
    up_scale,
    down_w,
    down_scale,
    query_w,
    query_scale,
    key_w,
    key_scale,
    value_w,
    value_scale,
    out_w,
    out_scale,
    head_gain,
    decay_rate,
):
    f32, bf16 = jnp.float32, jnp.bfloat16
    n = n_fs
    rows, features = tokens_in.shape
    width, units = gate_w.shape[0], gate_w.shape[1] // 2
    heads = decay_rate.shape[0] // 2
    kinds = heads + 5
    span_of = n - 2
    any_space = pl.BlockSpec(memory_space=pl.ANY)
    vmem = pl.BlockSpec(memory_space=pltpu.VMEM)
    smem = pl.BlockSpec(memory_space=pltpu.SMEM)
    dma = pltpu.SemaphoreType.DMA

    return pl.pallas_call(
        functools.partial(layer_kernel, n),
        out_shape=pltpu.VMEM((rows, features), bf16),
        in_specs=[any_space] * 17 + [smem],
        out_specs=vmem,
        scratch_shapes=[
            pltpu.VMEM(norm_gains.shape, f32),
        ]
        + [
            pltpu.VMEM((1, x.shape[0]), f32)
            for x in (
                gate_scale,
                up_scale,
                down_scale,
                query_scale,
                key_scale,
                value_scale,
                out_scale,
                head_gain,
            )
        ]
        + [
            pltpu.VMEM((rows, features), bf16),
            pltpu.VMEM((2, width, units), f32),
            pltpu.VMEM((2, width, units), f32),
            pltpu.VMEM((2, units, width), f32),
            pltpu.VMEM((2, width, heads * DK), f32),
            pltpu.VMEM((2, width, heads * DK), f32),
            pltpu.VMEM((2, width, heads * DV), f32),
            pltpu.VMEM((2, heads * DV, width), f32),
            pltpu.VMEM((width, units), bf16),
            pltpu.VMEM((width, units), bf16),
            pltpu.VMEM((units, width), bf16),
            pltpu.VMEM((heads, width, 2 * DK + DV), bf16),
            pltpu.VMEM((heads * DV, width), bf16),
            pltpu.VMEM((16, width), f32),
            pltpu.VMEM((features, units), bf16),
            pltpu.VMEM((features, units), bf16),
            pltpu.VMEM((n, units, width), bf16),
            pltpu.VMEM((heads, features, 2 * DK + DV), bf16),
            pltpu.VMEM((n, heads * DV, width), bf16),
            pltpu.VMEM((n, 16, width), f32),
            pltpu.VMEM((3, 4 * rows, features), bf16),
            pltpu.VMEM((4, 8, rows), f32),
            pltpu.VMEM((rows, features), f32),
            pltpu.VMEM((rows, 128), f32),
            pltpu.VMEM((2, 4 * rows, units), f32),
            pltpu.VMEM((4 * rows, units), bf16),
            pltpu.VMEM((4 * rows, heads * DV), bf16),
            pltpu.VMEM((n, rows, width), f32),
            pltpu.VMEM((n, rows, width), f32),
            pltpu.VMEM((3, n, 2, rows, width), bf16),
            pltpu.VMEM((3, n, 2, rows, width), bf16),
            pltpu.VMEM((3, n, rows, width), bf16),
            pltpu.VMEM((3, n, rows, width), bf16),
            dma((24,)),
            dma((kinds + 2,)),
            dma((kinds + 2,)),
            dma((6 * span_of,)),
            dma((kinds * span_of,)),
            dma((kinds * span_of,)),
            dma((6,)),
            dma((2 * n,)),
            dma((6,)),
            dma((6,)),
            dma((6,)),
            dma((3 * n + 3,)),
        ],
        compiler_params=pltpu.CompilerParams(
            collective_id=0, has_side_effects=True, vmem_limit_bytes=VMEM_LIMIT
        ),
        name="layer",
    )(
        tokens_in,
        norm_gains,
        gate_w,
        gate_scale,
        up_w,
        up_scale,
        down_w,
        down_scale,
        query_w,
        query_scale,
        key_w,
        key_scale,
        value_w,
        value_scale,
        out_w,
        out_scale,
        head_gain,
        decay_rate,
    )


def solution(mesh):
    sizes = [mesh.shape[axis] for axis in ("rep", "fs", "tp")]
    placed = (
        P(("rep", "fs", "tp"), None),
        P(),
        P("fs", "tp"),
        P("tp"),
        P("fs", "tp"),
        P("tp"),
        P("tp", "fs"),
        P("fs"),
        P("fs", "tp"),
        P("tp"),
        P("fs", "tp"),
        P("tp"),
        P("fs", "tp"),
        P("tp"),
        P("tp", "fs"),
        P("fs"),
        P(),
        P("tp"),
    )
    return jax.shard_map(
        lambda *args: (fused if fits(*sizes, *args) else on_device)(*sizes, *args),
        mesh=mesh,
        in_specs=placed,
        out_specs=P(("rep", "fs", "tp"), None),
        check_vma=False,
    )
```

```python
import functools
import math

import jax
import jax.numpy as jnp
from jax import lax
from jax.experimental import pallas as pl
from jax.experimental.pallas import tpu as pltpu
from jax.sharding import PartitionSpec as P

DK = 256
DV = 256
BLOCK = 64

EPSILON = 1e-05


def rms_scale(stream, gain):
    return stream * lax.rsqrt(jnp.mean(stream * stream, axis=-1, keepdims=True) + EPSILON) * gain


def snake(n):
    return [i for i in range(0, n, 2)] + [i for i in range(n - 1, 0, -1) if i % 2 == 1]


def snake_place(index, n):
    return jnp.where(index % 2 == 0, index // 2, n - 1 - index // 2)


def snake_index(place, n):
    half = (n + 1) // 2
    return jnp.where(place < half, 2 * place, 2 * (n - 1 - place) + 1)


def shift(x, axis, n, by):
    return lax.ppermute(x, axis, [(i, (i + by) % n) for i in range(n)])


def ring_gather(shards, n, forward_steps):
    order = snake(n)
    ahead = [(order[i], order[(i + 1) % n]) for i in range(n)]
    behind = [(b, a) for a, b in ahead]
    found = []
    for x, steps in zip(shards, forward_steps):
        forward, back = [x], [x]
        found.append((forward, back))
    for step in range(n):
        for (forward, back), steps in zip(found, forward_steps):
            if step < steps:
                forward.append(lax.ppermute(forward[-1], "fs", ahead))
            if step < n - 1 - steps:
                back.append(lax.ppermute(back[-1], "fs", behind))
    return [forward + back[:0:-1] for forward, back in found]


def chained(shards, before, hops):
    if not before:
        return shards
    last = []
    n = len(before[0])
    for pieces in before:
        last.extend([pieces[hops], pieces[n - hops]])
    return lax.optimization_barrier((tuple(shards), tuple(last)))[0]


def with_scale(weight, scale):
    high = lax.reduce_precision(scale, 8, 7)
    middle = lax.reduce_precision(scale - high, 8, 7)
    rows = jnp.stack([high, middle, scale - high - middle]).astype(jnp.bfloat16)
    return jnp.concatenate([weight, jnp.pad(rows, ((0, 13), (0, 0)))], axis=0)


def without_scale(pieces):
    size = pieces[0].shape[0] - 16
    weight = jnp.concatenate([p[:size] for p in pieces], axis=1)
    rows = jnp.concatenate([p[size:] for p in pieces], axis=1)[:3].astype(jnp.float32)
    return weight, rows[0] + rows[1] + rows[2]


def retain(query, key_rows, value, decay, head_gain):
    seq_len = query.shape[0]
    row = lax.broadcasted_iota(jnp.int32, (seq_len, seq_len), 0)
    col = lax.broadcasted_iota(jnp.int32, (seq_len, seq_len), 1)
    distance = jnp.abs(row - col).astype(jnp.float32)
    weight = jnp.where(col // BLOCK <= row // BLOCK, jnp.exp(-decay * distance), 0.0)
    scores = lax.dot_general(
        query, key_rows, (((1,), (1,)), ((), ())), preferred_element_type=jnp.float32
    )
    scores = (scores * weight).astype(jnp.bfloat16)
    retained = jnp.dot(scores, value, preferred_element_type=jnp.float32)
    centred = retained - jnp.mean(retained, axis=-1, keepdims=True)
    normed = (
        centred
        * lax.rsqrt(jnp.mean(centred * centred, axis=-1, keepdims=True) + EPSILON)
        * head_gain
    )
    return normed.astype(jnp.bfloat16)


def on_device(
    n_rep,
    n_fs,
    n_tp,
    tokens_in,
    norm_gains,
    gate_w,
    gate_scale,
    up_w,
    up_scale,
    down_w,
    down_scale,
    query_w,
    query_scale,
    key_w,
    key_scale,
    value_w,
    value_scale,
    out_w,
    out_scale,
    head_gain,
    decay_rate,
):
    rows = tokens_in.shape[0]
    width = gate_w.shape[0]
    heads = decay_rate.shape[0]
    units = gate_w.shape[1]
    share = n_rep if heads % n_rep == 0 and units % (n_rep * 128) == 0 else 1
    heads //= share
    units //= share
    rep = lax.axis_index("rep") if share > 1 else 0
    tp = lax.axis_index("tp")
    place = snake_place(lax.axis_index("fs"), n_fs)

    def part(x, axis):
        size = x.shape[axis] // share
        return lax.dynamic_slice_in_dim(x, rep * size, size, axis)

    gate_b, up_b, query_b, key_b, value_b = (
        part(w, 1).astype(jnp.bfloat16) for w in (gate_w, up_w, query_w, key_w, value_w)
    )
    down_b, out_b = (part(w, 0).astype(jnp.bfloat16) for w in (down_w, out_w))

    few, many = (n_fs - 1) // 2, n_fs // 2
    first_pieces = ring_gather([gate_b, up_b], n_fs, [many, few])
    half = down_b.shape[0] // 2
    second_pieces = ring_gather(
        chained([with_scale(down_b[:half], down_scale), down_b[half:]], first_pieces, max(1, n_fs // 4)),
        n_fs,
        [many, few],
    )
    third_pieces = ring_gather(chained([query_b, key_b], second_pieces, few), n_fs, [many, few])
    value_pieces, out_pieces = ring_gather(
        chained([value_b, with_scale(out_b, out_scale)], third_pieces, few), n_fs, [many, few]
    )

    gate_full, up_full = (jnp.concatenate(p, axis=0) for p in first_pieces)
    down_top, down_cols = without_scale(second_pieces[0])
    down_rest = jnp.concatenate(second_pieces[1], axis=1)
    down_full = lax.optimization_barrier(jnp.concatenate([down_top, down_rest], axis=0))
    query_full, key_full = (jnp.concatenate(p, axis=0) for p in third_pieces)
    value_full = jnp.concatenate(value_pieces, axis=0)
    out_full, out_cols = without_scale(out_pieces)

    def to_ring(x):
        blocks = [
            lax.dynamic_slice_in_dim(
                x, snake_index((place - k) % n_fs, n_fs) * width, width, axis=1
            )
            for k in range(n_fs)
        ]
        return jnp.concatenate(blocks, axis=1)

    def from_ring(x):
        blocks = [
            lax.dynamic_slice_in_dim(x, (place - snake(n_fs).index(o)) % n_fs * width, width, axis=1)
            for o in range(n_fs)
        ]
        return jnp.concatenate(blocks, axis=1)

    def over_tp(x, ordered):
        found = [x] + [shift(x, "tp", n_tp, k) for k in range(1, n_tp)]
        if not ordered:
            return jnp.concatenate(found, axis=0)
        twice = jnp.concatenate(found[::-1] * 2, axis=0)
        return lax.dynamic_slice_in_dim(twice, (n_tp - 1 - tp) * rows, n_tp * rows, axis=0)

    def gather_rows(normed, ordered=False):
        found = [normed] + [shift(normed, "rep", n_rep, k) for k in range(1, share)]
        return [over_tp(x, ordered) for x in found]

    def return_rows(parts, ordered=False):
        total = None
        for k in range(share - 1, -1, -1):

            def block(j):
                at = (tp - j) % n_tp * rows if ordered else j * rows
                return lax.dynamic_slice_in_dim(parts[k], at, rows, axis=0)

            mine = block(0)
            for j in range(1, n_tp):
                other = shift(block(j).astype(jnp.bfloat16), "tp", n_tp, n_tp - j)
                mine = mine + other.astype(jnp.float32)
            if k > 0:
                mine = shift(mine.astype(jnp.bfloat16), "rep", n_rep, n_rep - k).astype(jnp.float32)
            total = mine if total is None else total + mine
        return total

    def dot(a, b):
        return jnp.dot(a, b, preferred_element_type=jnp.float32)

    gate_col, up_col = part(gate_scale, 0), part(up_scale, 0)

    def feed_forward(stream, gain):
        parts = []
        for gathered in gather_rows(rms_scale(stream, gain).astype(jnp.bfloat16)):
            gate_value = dot(gathered, gate_full) * gate_col
            up_value = dot(gathered, up_full) * up_col
            hidden = (jax.nn.silu(gate_value) * up_value).astype(jnp.bfloat16)
            hidden = lax.optimization_barrier(hidden)
            parts.append(dot(hidden, down_full) * down_cols)
        return return_rows(parts)

    query_col, key_col, value_col = (part(s, 0) for s in (query_scale, key_scale, value_scale))
    decay = part(decay_rate, 0)
    gains = to_ring(norm_gains)

    stream = to_ring(tokens_in).astype(jnp.float32)
    stream = stream + 0.5 * feed_forward(stream, gains[0])
    parts = []
    for gathered in gather_rows(
        rms_scale(stream, gains[1]).astype(jnp.bfloat16), ordered=True
    ):
        query = (dot(gathered, query_full) * query_col).astype(jnp.bfloat16)
        key_rows = (dot(gathered, key_full) * key_col / math.sqrt(DK)).astype(jnp.bfloat16)
        value = (dot(gathered, value_full) * value_col).astype(jnp.bfloat16)
        mixed = [
            retain(
                query[:, h * DK : (h + 1) * DK],
                key_rows[:, h * DK : (h + 1) * DK],
                value[:, h * DV : (h + 1) * DV],
                decay[h],
                head_gain,
            )
            for h in range(heads)
        ]
        parts.append(dot(jnp.concatenate(mixed, axis=1), out_full) * out_cols)
    stream = stream + return_rows(parts, ordered=True)
    stream = stream + 0.5 * feed_forward(stream, gains[2])
    return from_ring(stream.astype(jnp.bfloat16))


MESH = pl.DeviceIdType.MESH
VMEM_LIMIT = 62 * 1024 * 1024


def fits(n_rep, n_fs, n_tp, tokens_in, norm_gains, gate_w, *rest):
    rows, features = tokens_in.shape
    width, units = gate_w.shape
    heads = rest[-1].shape[0]
    return (
        n_rep == 2
        and n_tp == 2
        and n_fs >= 6
        and n_fs % 2 == 0
        and n_fs <= 16
        and rows % 128 == 0
        and width % 256 == 0
        and features == n_fs * width
        and units % 512 == 0
        and heads % 2 == 0
    )


def layer_kernel(
    n,
    tokens_in,
    norm_gains_in,
    gate_w,
    gate_scale_in,
    up_w,
    up_scale_in,
    down_w,
    down_scale_in,
    query_w,
    query_scale_in,
    key_w,
    key_scale_in,
    value_w,
    value_scale_in,
    out_w,
    out_scale_in,
    head_gain_in,
    decay_rate,
    result,
    norm_gains,
    gate_scale,
    up_scale,
    down_scale,
    query_scale,
    key_scale,
    value_scale,
    out_scale,
    head_gain,
    staged_in,
    staged_gate,
    staged_up,
    staged_down,
    staged_query,
    staged_key,
    staged_value,
    staged_out,
    gate_away,
    up_away,
    down_away,
    head_away,
    out_away,
    cols_away,
    gate_full,
    up_full,
    down_full,
    head_full,
    out_full,
    cols_full,
    gathered,
    factors,
    stream,
    squares,
    summed,
    hidden,
    mixed,
    own_part,
    far_part,
    tp_out,
    tp_in,
    rep_out,
    rep_in,
    local_sem,
    side_send,
    side_recv,
    line_send,
    line_recv,
    twin_recv,
    part_send,
    part_recv,
    row_send,
    row_recv,
    block_send,
    block_recv,
):
    f32, bf16 = jnp.float32, jnp.bfloat16
    rows, features = tokens_in.shape
    width = gate_w.shape[0]
    units = hidden.shape[1]
    heads = head_full.shape[0]
    tile = 256

    twin, fs, tp = (lax.axis_index(axis) for axis in ("rep", "fs", "tp"))
    line = n // 2
    side, spot = lax.rem(fs, 2), lax.div(fs, 2)
    above, below = {"fs": fs + 2}, {"fs": fs - 2}
    side_peer, twin_peer, tp_peer = {"fs": fs + 1 - 2 * side}, {"rep": 1 - twin}, {"tp": 1 - tp}
    has_above, has_below = spot + 1 < line, spot > 0

    barrier = pltpu.get_barrier_semaphore()

    def greet(peer):
        pl.semaphore_signal(barrier, inc=1, device_id=peer, device_id_type=MESH)

    def meet():
        for peer in (side_peer, twin_peer, tp_peer):
            greet(peer)
        pl.when(has_above)(lambda: greet(above))
        pl.when(has_below)(lambda: greet(below))

    def columns_of(f):
        return pl.ds(pl.multiple_of(f * width, width), width)

    def halves(size):
        return [pl.ds(pl.multiple_of(i * size, 128), size) for i in (side, 1 - side)]

    local, copies_of = [], {}

    def fetch(name, src, dst):
        copy = pltpu.make_async_copy(src, dst, local_sem.at[len(local)])
        copy.start()
        copies_of.setdefault(name, []).append(copy)
        local.append(copy)

    def fetched(name):
        for copy in copies_of[name]:
            copy.wait()

    gate_halves = halves(units)
    fetch(("gate", 0), gate_w.at[:, gate_halves[0]], staged_gate.at[0])
    meet()
    fetch(("gate", 1), gate_w.at[:, gate_halves[1]], staged_gate.at[1])
    for i, cols in enumerate(halves(units)):
        fetch(("up", i), up_w.at[:, cols], staged_up.at[i])
    fetch("rows", tokens_in, staged_in)
    for src, dst in (
        (gate_scale_in, gate_scale),
        (up_scale_in, up_scale),
        (down_scale_in, down_scale),
        (query_scale_in, query_scale),
        (key_scale_in, key_scale),
        (value_scale_in, value_scale),
        (out_scale_in, out_scale),
        (head_gain_in, head_gain),
    ):
        fetch("small", src, dst.at[0])
    fetch("small", norm_gains_in, norm_gains)
    for i, cols in enumerate(halves(units)):
        fetch("down", down_w.at[cols, :], staged_down.at[i])
    for i, cols in enumerate(halves(heads * DK)):
        fetch("heads", query_w.at[:, cols], staged_query.at[i])
        fetch("heads", key_w.at[:, cols], staged_key.at[i])
    for i, cols in enumerate(halves(heads * DV)):
        fetch("heads", value_w.at[:, cols], staged_value.at[i])
        fetch("out", out_w.at[cols, :], staged_out.at[i])

    started = []
    half_units, half_width, half_out = units // 2, width // 2, heads * DV // 2

    def rows_of(f):
        return pl.ds(pl.multiple_of(f * width, width), width)

    def cut(ref, s, size):
        return ref.at[pl.ds(pl.multiple_of(s * size, size), size), :]

    def half_rows(f, i):
        return pl.ds(pl.multiple_of(f * width + i * half_width, half_width), half_width)

    kinds, head_kinds = [], []
    for i in range(2):
        kinds.append(
            (
                lambda f, i=i: gate_full.at[half_rows(f, i), :],
                gate_away.at[pl.ds(i * half_width, half_width), :],
                half_width // 2,
            )
        )
    kinds.append((lambda f: up_full.at[rows_of(f), :], up_away, half_width))
    kinds.append((lambda f: down_full.at[f], down_away, half_units))
    up_kind, down_kind = 2, 3
    for h in range(heads):
        head_kinds.append([len(kinds)])
        kinds.append(
            (lambda f, h=h: head_full.at[h, rows_of(f), :], head_away.at[h], half_width)
        )
    out_kind = len(kinds)
    kinds.append((lambda f: out_full.at[f], out_away, half_out))
    scales = len(kinds)
    kinds.append((lambda f: cols_full.at[f], cols_away, 8))
    rounds = [[0, 1, up_kind], [down_kind, scales], *head_kinds, [out_kind]]
    bank_of, last_bank = {}, 0
    for members in rounds:
        for kind in members:
            bank_of[kind] = last_bank
            last_bank = (last_bank + 1) % 3

    def piece(kind, f, s):
        if kind == scales:
            return kinds[kind][0](f).at[pl.ds(pl.multiple_of(s * 8, 8), 1), :]
        return cut(kinds[kind][0](f), s, kinds[kind][2])

    def remote(src, dst, send_sem, recv_sem, peer):
        return pltpu.make_async_remote_copy(
            src_ref=src,
            dst_ref=dst,
            send_sem=send_sem,
            recv_sem=recv_sem,
            device_id=peer,
            device_id_type=MESH,
        )

    def across(o):
        return spot * 2 + side + o * (1 - 2 * side)

    def side_slot(kind, i):
        return kind * 2 + i if kind <= up_kind else kind + 3

    def side_copy(kind, i, f):
        slot_of = side_slot(kind, i)
        sems = side_send.at[slot_of], side_recv.at[slot_of]
        if kind <= up_kind:
            s = twin if i == 0 else 1 - twin
            return remote(
                cut(kinds[kind][1], s, kinds[kind][2]), piece(kind, f, s), *sems, side_peer
            )
        return remote(kinds[kind][1], kinds[kind][0](f), *sems, side_peer)

    def side_start(kind, i=0):
        copy = side_copy(kind, i, fs)
        copy.start()
        started.append(copy)

    side_done = set()

    def side_need(kind, i):
        i = i if kind <= up_kind else 0
        if (kind, i) not in side_done:
            side_done.add((kind, i))
            side_copy(kind, i, across(1)).wait_recv()

    span_of = 2 * (line - 1)
    sending = {}

    def push(kind, group, index, f, where, recv, peer):
        bank = bank_of[kind]
        slot_of = (bank * 3 + group) * span_of + index
        copy = remote(piece(kind, f, twin), piece(kind, f, twin), line_send.at[slot_of], recv, peer)
        if slot_of in sending:
            sending.pop(slot_of)()
        guard = functools.partial(pl.when, where) if where is not None else None

        def begin():
            copy.start()

        def finish():
            copy.wait_send()

        if guard is None:
            begin()
            sending[slot_of] = finish
        else:
            guard()(begin)
            sending[slot_of] = lambda: guard()(finish)

    def line_slot(kind, away, o):
        return line_recv.at[kind * span_of + (away % line - 1) * 2 + o]

    def twin_slot(kind, away, o):
        return twin_recv.at[kind * span_of + (away - 1) * 2 + o]

    def send_own(kind, o):
        if o == 1:
            side_need(kind, 0)
        f = across(o)
        push(kind, 0, o, f, has_above, line_slot(kind, -1, o), above)
        push(kind, 1, o, f, has_below, line_slot(kind, 1, o), below)

    def places(d, o):
        for group, away in ((1, d), (0, -d)):
            from_spot = spot + away
            exists = from_spot >= 0 if away < 0 else from_spot < line
            yield group, away, exists, from_spot * 2 + side + o * (1 - 2 * side)

    def take_in(kind, d, o):
        for group, away, exists, f in places(d, o):

            def receive(kind=kind, away=away, f=f):
                remote(
                    piece(kind, f, twin),
                    piece(kind, f, twin),
                    line_send.at[0],
                    line_slot(kind, away, o),
                    above,
                ).wait_recv()

            pl.when(exists)(receive)
            hand_over(kind, away, o, f, exists)

    def move_on(kind, d, o):
        if d > line - 2:
            return
        for group, away, exists, f in places(d, o):
            further = -d - 1 if away < 0 else d + 1
            push(
                kind,
                group,
                2 * d + o,
                f,
                jnp.logical_and(exists, has_above if away < 0 else has_below),
                line_slot(kind, further, o),
                above if away < 0 else below,
            )

    def pass_along(kind, d, o):
        take_in(kind, d, o)
        move_on(kind, d, o)

    def hand_over(kind, away, o, f, exists):
        index = (away % line - 1) * 2 + o
        bank = bank_of[kind]
        slot_of = (bank * 3 + 2) * span_of + index
        first = away > 0
        copy = remote(
            piece(kind, f, twin),
            piece(kind, f, twin),
            line_send.at[slot_of],
            twin_slot(kind, away % line, o),
            twin_peer,
        )
        key = (slot_of, first)
        if key in sending:
            sending.pop(key)()
        pl.when(exists)(lambda: copy.start())
        sending[key] = lambda: pl.when(exists)(lambda: copy.wait_send())

    def pick(table):
        total = 0
        for v in range(line):
            total = total + (spot == v).astype(jnp.int32) * table[v]
        return total

    near = []
    for v in range(line):
        near.append(sorted((u for u in range(line) if u != v), key=lambda u: (abs(u - v), -u)))
    sources = [across(0), across(1)]
    twin_index = [None, None]
    for r in range(line - 1):
        at = pick([near[v][r] for v in range(line)])
        away = pick([(near[v][r] - v) % line for v in range(line)])
        for o in range(2):
            sources.append(at * 2 + side + o * (1 - 2 * side))
            twin_index.append((away - 1) * 2 + o)

    def need_piece(kind, k):
        if k == 1:
            side_need(kind, 0)
            side_need(kind, 1)
        if k > 1:
            remote(
                piece(kind, sources[k], 1 - twin),
                piece(kind, sources[k], 1 - twin),
                line_send.at[0],
                twin_recv.at[kind * span_of + twin_index[k]],
                twin_peer,
            ).wait_recv()

    queue = []
    later = []
    for members in rounds:
        for o in range(2):
            queue.append([functools.partial(send_own, m, o) for m in members])
        queue.extend(later)
        later = []
        for d in range(1, line):
            for o in range(2):
                unit = [functools.partial(pass_along, m, d, o) for m in members]
                (queue if d < line - 1 else later).append(unit)
    queue.extend(later)
    middle = 2 * (line - 2)

    def pump(count):
        for _ in range(count):
            for action in queue.pop(0):
                action()

    def send(src, dst, send_sem, recv_sem, peer):
        copy = remote(src, dst, send_sem, recv_sem, peer)
        copy.start()
        started.append(copy)
        return copy

    own_rows = rows_of(fs)
    fetched(("gate", 0))
    gate_full[own_rows, :] = staged_gate[0].astype(bf16)
    neighbours = has_above.astype(jnp.int32) + has_below.astype(jnp.int32)
    pl.semaphore_wait(barrier, 3 + neighbours)
    first, second, _ = (queue.pop(0) for _ in range(3))
    first[0]()
    first[1]()
    fetched(("gate", 1))
    gate_away[...] = staged_gate[1].astype(bf16)
    side_start(0)
    side_start(1)
    fetched(("up", 0))
    up_full[own_rows, :] = staged_up[0].astype(bf16)
    first[2]()
    fetched(("up", 1))
    up_away[...] = staged_up[1].astype(bf16)
    side_start(up_kind)
    fetched("rows")
    fetched("small")

    def norm_rows(source, which, target):
        gain = norm_gains[which : which + 1, :]

        def step(i, carry):
            block = pl.ds(pl.multiple_of(i * 16, 16), 16)
            x = source[block, :].astype(f32)
            mean = jnp.mean(x * x, axis=-1, keepdims=True)
            target[block, :] = (x * lax.rsqrt(mean + EPSILON) * gain).astype(bf16)
            return carry

        lax.fori_loop(0, rows // 16, step, 0)

    def slot(j, cols=slice(None)):
        return (pl.ds(j * rows, rows), cols)

    def share_rows(stage):
        part = gathered.at[stage]
        base = 3 * stage
        send(part.at[slot(0)], part.at[slot(1)], row_send.at[base], row_recv.at[base], tp_peer)
        send(
            part.at[slot(0)],
            part.at[slot(2)],
            row_send.at[base + 1],
            row_recv.at[base + 1],
            side_peer,
        )

    def wait_rows(stage, i, j):
        part = gathered.at[stage]
        pltpu.make_async_remote_copy(
            src_ref=part.at[slot(0)],
            dst_ref=part.at[slot(j)],
            send_sem=row_send.at[3 * stage + i],
            recv_sem=row_recv.at[3 * stage + i],
            device_id=tp_peer,
            device_id_type=MESH,
        ).wait_recv()

    def relay_rows(stage):
        wait_rows(stage, 1, 2)
        part = gathered.at[stage]
        send(
            part.at[slot(2)],
            part.at[slot(3)],
            row_send.at[3 * stage + 2],
            row_recv.at[3 * stage + 2],
            tp_peer,
        )

    norm_rows(staged_in, 0, gathered.at[0])
    stream[...] = staged_in[...].astype(f32)
    fetched("down")
    down_full[fs] = staged_down[0].astype(bf16)
    down_away[...] = staged_down[1].astype(bf16)
    cols_full[fs, 0:1, :] = down_scale[...]
    cols_full[fs, 8:9, :] = out_scale[...]
    cols_away[0:1, :] = down_scale[...]
    cols_away[8:9, :] = out_scale[...]
    side_start(0, 1)
    side_start(1, 1)
    side_start(up_kind, 1)
    side_start(down_kind)
    side_start(scales)
    take_in(0, 1, 0)
    take_in(1, 1, 0)
    second[0]()
    second[1]()
    take_in(up_kind, 1, 0)
    second[2]()
    move_on(0, 1, 0)
    move_on(1, 1, 0)
    move_on(up_kind, 1, 0)
    share_rows(0)
    fetched("heads")
    for h in range(heads):
        keys, vals = slice(h * DK, (h + 1) * DK), slice(h * DV, (h + 1) * DV)
        for i in range(2):
            made = jnp.concatenate(
                [staged_query[i, :, keys], staged_key[i, :, keys], staged_value[i, :, vals]], axis=1
            ).astype(bf16)
            if i == 0:
                head_full[h, own_rows, :] = made
            else:
                head_away[h] = made
        for kind in head_kinds[h]:
            side_start(kind)
    fetched("out")
    out_full[fs] = staged_out[0].astype(bf16)
    out_away[...] = staged_out[1].astype(bf16)
    side_start(out_kind)

    pump(middle + 2)
    relay_rows(0)
    pump(middle + 1)
    wait_rows(0, 0, 1)
    wait_rows(0, 2, 3)

    def dot(a, b):
        return jnp.dot(a, b, preferred_element_type=f32)

    def expand(factor, part, first=0, count=4 * rows):
        for c in range(units // tile):
            cols = slice(c * tile, (c + 1) * tile)
            span = pl.ds(pl.multiple_of(side * units + c * tile, 128), tile)
            rows_in, lhs = part
            block = slice(first, first + count)
            gate = dot(lhs[block], gate_full[rows_in, cols])
            up = dot(lhs[block], up_full[rows_in, cols])
            if factor is not None:
                gate = (gate + summed[0, block, cols]) * factor[block]
                up = (up + summed[1, block, cols]) * factor[block]
            gate, up = gate * gate_scale[:, span], up * up_scale[:, span]
            hidden[block, cols] = (gate / (1.0 + jnp.exp(-gate)) * up).astype(bf16)

    def part_copy(stage, k, way, landing):
        store_out, store_in = (rep_out, rep_in) if way == 2 else (tp_out, tp_in)
        return remote(
            store_out.at[stage, k] if way == 2 else store_out.at[stage, k, way],
            store_in.at[stage, landing] if way == 2 else store_in.at[stage, landing, way],
            part_send.at[stage * 2 + way // 2],
            part_recv.at[landing * 3 + way],
            side_peer if way == 2 else tp_peer,
        )

    def part_start(stage, k, way):
        part_copy(stage, k, way, k ^ 1 if way == 2 else k).start()

    def part_wait(stage, k, way):
        part_copy(stage, k, way, k).wait_recv()

    def parts_sent(stage):
        for over_side, (src, dst) in enumerate(((tp_out, tp_in), (rep_out, rep_in))):
            remote(
                src.at[stage],
                dst.at[stage],
                part_send.at[stage * 2 + over_side],
                part_recv.at[0],
                side_peer,
            ).wait_send()

    def contract(stage, lhs, weight, row, fresh, order, finish, relay=None, extra=None, near=None):
        def ready(k):
            if fresh is not None:
                need_piece(fresh, k)
                if fresh == down_kind:
                    need_piece(scales, k)

        def product(k, block):
            f = sources[k]
            return dot(lhs[block, :], weight[f]) * cols_full[f, 8 * row : 8 * row + 1, :]

        def keep(k, way, part):
            (far_part if way else own_part)[k] = part[:rows]
            tp_out[stage, k, way] = part[rows:].astype(bf16)
            part_start(stage, k, way)

        def multiply(k):
            ready(k)
            part = product(k, slice(None))
            keep(k, 1, part[2 * rows :])
            keep(k, 0, part[: 2 * rows])

        def multiply_far(k):
            ready(k)
            keep(k, 1, product(k, slice(2 * rows, 4 * rows)))

        def multiply_near(k):
            keep(k, 0, product(k, slice(0, 2 * rows)))

        def pass_on(k):
            part_wait(stage, k, 1)
            rep_out[stage, k] = (far_part[k] + tp_in[stage, k, 1].astype(f32)).astype(bf16)
            part_start(stage, k, 2)

        def collect(k):
            part_wait(stage, k, 0)
            part_wait(stage, k, 2)
            total = own_part[k] + tp_in[stage, k, 0].astype(f32) + rep_in[stage, k].astype(f32)
            finish(k, sources[k], total)

        actions = {"m": multiply, "p": pass_on, "c": collect, "r": relay, "u": pump, "x": extra}
        actions.update({"f": multiply_far, "n": multiply_near, "near": lambda _: near()})
        for action, k in order:
            actions[action](k)

    def last_order():
        order = []
        for k in range(n):
            order.append(("f", k))
            if k > 0:
                order.append(("p", k - 1))
        order += [("p", n - 1), ("near", 0)]
        return order + [("n", k) for k in range(n)] + [("c", k) for k in range(n)]

    def first_order():
        order = [("m", 0), ("m", 1), ("p", 0), ("p", 1), ("u", 4)]
        for k in range(2, n):
            if k == 2 * (line - 1):
                order.append(("u", 2))
            order.append(("m", k))
            if k > 2:
                order.append(("p", k - 1))
        order.append(("p", n - 1))
        order += [("c", k) for k in range(n)]
        order.insert(-2, ("u", 1))
        return order

    def tail_order():
        order, waiting, relayed = [], [], []

        def advance(r):
            ks = (2 * r, 2 * r + 1)
            order.extend([("m", k) for k in ks] + [("p", k) for k in ks])
            waiting.append(ks)

        def take():
            if waiting:
                ks = waiting.pop(0)
                order.extend(("c", k) for k in ks)
                relayed.append(ks)

        order.extend([("m", 0), ("m", 1), ("u", 1), ("p", 0), ("p", 1)])
        order.extend([("m", 2), ("m", 3), ("p", 2), ("p", 3), ("c", 0), ("c", 1)])
        waiting.append((2, 3))
        relayed.append((0, 1))
        for r in range(3, line):
            order.append(("u", 1))
            take()
            order.append(("u", 1))
            advance(r - 1)
        for ks in relayed[:1]:
            order.extend(("r", k) for k in relayed.pop(0))
        advance(line - 1)
        while waiting:
            take()
            order.extend(("r", k) for k in relayed.pop(0))
        order.extend(("r", k) for ks in relayed for k in ks)
        for r in range(line - 2):
            order.insert(order.index(("r", 2 * r + 3)) + 1, ("x", r))
        return order

    def need_all(kind):
        for k in range(1, n):
            need_piece(kind, k)

    need_all(0)
    need_all(1)
    need_all(up_kind)
    expand(None, (slice(None), gathered[0]))

    def add_half(k, f, total):
        cols = columns_of(f)
        stream[:, cols] = stream[:, cols] + 0.5 * total

    contract(0, hidden, down_full, 0, down_kind, first_order(), add_half)

    norm_rows(stream, 1, gathered.at[1])
    share_rows(1)
    pump(middle + 1)
    relay_rows(1)
    pump(2)

    seq_len = 2 * rows
    row = lax.rem(
        lax.broadcasted_iota(jnp.int32, (seq_len, seq_len), 0) + tp * rows, seq_len
    )
    col = lax.rem(
        lax.broadcasted_iota(jnp.int32, (seq_len, seq_len), 1) + tp * rows, seq_len
    )

    def retain(h, hooks, parts=(0, 1)):
        start, stop = parts[0] * seq_len, (parts[-1] + 1) * seq_len
        places = [
            (query_scale, 0, DK, 1.0),
            (key_scale, DK, DK, 1.0 / math.sqrt(DK)),
            (value_scale, 2 * DK, DV, 1.0),
        ]
        made = []
        for i, (scale, first, size, factor) in enumerate(places):
            span = pl.ds(pl.multiple_of((side * heads + h) * size, 128), size)
            product = dot(gathered[1, start:stop], head_full[h, :, first : first + size])
            made.append((product * (scale[:, span] * factor)).astype(bf16))
            if i in hooks:
                pump(hooks[i])
        query, keys, values = made
        decay = decay_rate[side * heads + h]
        distance = jnp.abs(row - col).astype(f32)
        weight = jnp.where(
            lax.div(col, BLOCK) <= lax.div(row, BLOCK), jnp.exp(-decay * distance), 0.0
        )
        for s in parts:
            span = slice(s * seq_len - start, (s + 1) * seq_len - start)
            scores = lax.dot_general(
                query[span], keys[span], (((1,), (1,)), ((), ())), preferred_element_type=f32
            )
            scores = (scores * weight).astype(bf16)
            retained = dot(scores, values[span])
            centred = retained - jnp.mean(retained, axis=-1, keepdims=True)
            spread = jnp.mean(centred * centred, axis=-1, keepdims=True)
            mixed[s * seq_len : (s + 1) * seq_len, h * DV : (h + 1) * DV] = (
                centred * lax.rsqrt(spread + EPSILON) * head_gain[...]
            ).astype(bf16)

    for h in range(heads):
        if h == 0:
            wait_rows(1, 0, 1)
            wait_rows(1, 2, 3)
        for kind in head_kinds[h]:
            need_all(kind)
        retain(h, {1: 1})
        if h < heads - 1:
            pump(middle - 3 + 6)

    last = gathered.at[2]

    def block_copy(k, i, start):
        cols = columns_of(sources[k])
        a, b, peer = ((0, 1, tp_peer), (0, 2, side_peer), (2, 3, tp_peer))[i]
        return pltpu.make_async_remote_copy(
            src_ref=last.at[slot(a, cols)],
            dst_ref=last.at[slot(b, cols)],
            send_sem=block_send.at[i],
            recv_sem=block_recv.at[3 * (k ^ 1 if i == 1 and start else k) + i],
            device_id=peer,
            device_id_type=MESH,
        )

    def factor_copy(i):
        a, b, peer = ((0, 1, tp_peer), (0, 2, side_peer), (2, 3, tp_peer))[i]
        return pltpu.make_async_remote_copy(
            src_ref=factors.at[a],
            dst_ref=factors.at[b],
            send_sem=block_send.at[3 + i],
            recv_sem=block_recv.at[3 * n + i],
            device_id=peer,
            device_id_type=MESH,
        )

    squares[...] = jnp.zeros_like(squares)

    def add_mix(k, f, total):
        cols = columns_of(f)
        second = stream[:, cols] + total
        stream[:, cols] = second
        last[slot(0, cols)] = (second * norm_gains[2:3, cols]).astype(bf16)
        square = second * second
        added = squares[...]
        for i in range(width // 128):
            added = added + square[:, i * 128 : (i + 1) * 128]
        squares[...] = added
        for i in (0, 1):
            block_copy(k, i, True).start()
        if k == n - 1:
            mean = jnp.sum(added, axis=-1, keepdims=True) / features
            wide = jnp.broadcast_to(lax.rsqrt(mean + EPSILON), (rows, rows))
            factors[0] = wide.T[:8, :]
            for i in (0, 1):
                copy = factor_copy(i)
                copy.start()
                started.append(copy)

    def relay_block(k):
        block_copy(k, 1, False).wait_recv()
        block_copy(k, 2, True).start()
        if k == n - 1:
            factor_copy(1).wait_recv()
            copy = factor_copy(2)
            copy.start()
            started.append(copy)

    spots = [spot] + [lax.div(sources[2 * r], 2) for r in range(1, line)]

    def arrived_block(r):
        for k in (2 * r, 2 * r + 1):
            block_copy(k, 0, False).wait_recv()
            block_copy(k, 2, False).wait_recv()
        return pl.ds(pl.multiple_of(spots[r] * 2 * width, 2 * width), 2 * width)

    def take_sum(r):
        rows_in = arrived_block(r)
        lhs = last[:, rows_in]
        for c in range(units // tile):
            cols = slice(c * tile, (c + 1) * tile)
            for i, weight in enumerate((gate_full, up_full)):
                part = dot(lhs, weight[rows_in, cols])
                summed[i, :, cols] = part if r == 0 else summed[i, :, cols] + part

    contract(1, mixed, out_full, 1, out_kind, tail_order(), add_mix, relay_block, take_sum)
    take_sum(line - 2)
    rows_in = arrived_block(line - 1)
    factor_copy(0).wait_recv()
    factor_copy(2).wait_recv()
    factor = jnp.concatenate(
        [jnp.broadcast_to(factors[j, 0:1, :], (rows, rows)).T[:, 0:1] for j in range(4)], axis=0
    )
    late = (rows_in, last[:, rows_in])
    expand(factor, late, 2 * rows, 2 * rows)

    def write(k, f, total):
        cols = columns_of(f)
        result[:, cols] = (stream[:, cols] + 0.5 * total).astype(bf16)

    contract(2, hidden, down_full, 0, None, last_order(), write, near=lambda: expand(factor, late, 0, 2 * rows))
    assert not queue
    for stage in range(3):
        parts_sent(stage)
    for i, a in enumerate((0, 0, 2)):
        remote(
            last.at[slot(a)], last.at[slot(a)], block_send.at[i], block_recv.at[0], tp_peer
        ).wait_send()
    for finish in sending.values():
        finish()
    for copy in started:
        copy.wait_send()


def fused(
    n_rep,
    n_fs,
    n_tp,
    tokens_in,
    norm_gains,
    gate_w,
    gate_scale,
    up_w,
    up_scale,
    down_w,
    down_scale,
    query_w,
    query_scale,
    key_w,
    key_scale,
    value_w,
    value_scale,
    out_w,
    out_scale,
    head_gain,
    decay_rate,
):
    f32, bf16 = jnp.float32, jnp.bfloat16
    n = n_fs
    rows, features = tokens_in.shape
    width, units = gate_w.shape[0], gate_w.shape[1] // 2
    heads = decay_rate.shape[0] // 2
    kinds = heads + 6
    span_of = n - 2
    any_space = pl.BlockSpec(memory_space=pl.ANY)
    vmem = pl.BlockSpec(memory_space=pltpu.VMEM)
    smem = pl.BlockSpec(memory_space=pltpu.SMEM)
    dma = pltpu.SemaphoreType.DMA

    return pl.pallas_call(
        functools.partial(layer_kernel, n),
        out_shape=pltpu.VMEM((rows, features), bf16),
        in_specs=[any_space] * 17 + [smem],
        out_specs=vmem,
        scratch_shapes=[
            pltpu.VMEM(norm_gains.shape, f32),
        ]
        + [
            pltpu.VMEM((1, x.shape[0]), f32)
            for x in (
                gate_scale,
                up_scale,
                down_scale,
                query_scale,
                key_scale,
                value_scale,
                out_scale,
                head_gain,
            )
        ]
        + [
            pltpu.VMEM((rows, features), bf16),
            pltpu.VMEM((2, width, units), f32),
            pltpu.VMEM((2, width, units), f32),
            pltpu.VMEM((2, units, width), f32),
            pltpu.VMEM((2, width, heads * DK), f32),
            pltpu.VMEM((2, width, heads * DK), f32),
            pltpu.VMEM((2, width, heads * DV), f32),
            pltpu.VMEM((2, heads * DV, width), f32),
            pltpu.VMEM((width, units), bf16),
            pltpu.VMEM((width, units), bf16),
            pltpu.VMEM((units, width), bf16),
            pltpu.VMEM((heads, width, 2 * DK + DV), bf16),
            pltpu.VMEM((heads * DV, width), bf16),
            pltpu.VMEM((16, width), f32),
            pltpu.VMEM((features, units), bf16),
            pltpu.VMEM((features, units), bf16),
            pltpu.VMEM((n, units, width), bf16),
            pltpu.VMEM((heads, features, 2 * DK + DV), bf16),
            pltpu.VMEM((n, heads * DV, width), bf16),
            pltpu.VMEM((n, 16, width), f32),
            pltpu.VMEM((3, 4 * rows, features), bf16),
            pltpu.VMEM((4, 8, rows), f32),
            pltpu.VMEM((rows, features), f32),
            pltpu.VMEM((rows, 128), f32),
            pltpu.VMEM((2, 4 * rows, units), f32),
            pltpu.VMEM((4 * rows, units), bf16),
            pltpu.VMEM((4 * rows, heads * DV), bf16),
            pltpu.VMEM((n, rows, width), f32),
            pltpu.VMEM((n, rows, width), f32),
            pltpu.VMEM((3, n, 2, rows, width), bf16),
            pltpu.VMEM((3, n, 2, rows, width), bf16),
            pltpu.VMEM((3, n, rows, width), bf16),
            pltpu.VMEM((3, n, rows, width), bf16),
            dma((24,)),
            dma((kinds + 3,)),
            dma((kinds + 3,)),
            dma((9 * span_of,)),
            dma((kinds * span_of,)),
            dma((kinds * span_of,)),
            dma((6,)),
            dma((3 * n,)),
            dma((6,)),
            dma((6,)),
            dma((6,)),
            dma((3 * n + 3,)),
        ],
        compiler_params=pltpu.CompilerParams(
            collective_id=0, has_side_effects=True, vmem_limit_bytes=VMEM_LIMIT
        ),
        name="layer",
    )(
        tokens_in,
        norm_gains,
        gate_w,
        gate_scale,
        up_w,
        up_scale,
        down_w,
        down_scale,
        query_w,
        query_scale,
        key_w,
        key_scale,
        value_w,
        value_scale,
        out_w,
        out_scale,
        head_gain,
        decay_rate,
    )


def solution(mesh):
    sizes = [mesh.shape[axis] for axis in ("rep", "fs", "tp")]
    placed = (
        P(("rep", "fs", "tp"), None),
        P(),
        P("fs", "tp"),
        P("tp"),
        P("fs", "tp"),
        P("tp"),
        P("tp", "fs"),
        P("fs"),
        P("fs", "tp"),
        P("tp"),
        P("fs", "tp"),
        P("tp"),
        P("fs", "tp"),
        P("tp"),
        P("tp", "fs"),
        P("fs"),
        P(),
        P("tp"),
    )
    return jax.shard_map(
        lambda *args: (fused if fits(*sizes, *args) else on_device)(*sizes, *args),
        mesh=mesh,
        in_specs=placed,
        out_specs=P(("rep", "fs", "tp"), None),
        check_vma=False,
    )
```

```python
import functools
import math

import jax
import jax.numpy as jnp
from jax import lax
from jax.experimental import pallas as pl
from jax.experimental.pallas import tpu as pltpu
from jax.sharding import PartitionSpec as P

DK = 256
DV = 256
BLOCK = 64

EPSILON = 1e-05


def rms_scale(stream, gain):
    return stream * lax.rsqrt(jnp.mean(stream * stream, axis=-1, keepdims=True) + EPSILON) * gain


def snake(n):
    return [i for i in range(0, n, 2)] + [i for i in range(n - 1, 0, -1) if i % 2 == 1]


def snake_place(index, n):
    return jnp.where(index % 2 == 0, index // 2, n - 1 - index // 2)


def snake_index(place, n):
    half = (n + 1) // 2
    return jnp.where(place < half, 2 * place, 2 * (n - 1 - place) + 1)


def shift(x, axis, n, by):
    return lax.ppermute(x, axis, [(i, (i + by) % n) for i in range(n)])


def ring_gather(shards, n, forward_steps):
    order = snake(n)
    ahead = [(order[i], order[(i + 1) % n]) for i in range(n)]
    behind = [(b, a) for a, b in ahead]
    found = []
    for x, steps in zip(shards, forward_steps):
        forward, back = [x], [x]
        found.append((forward, back))
    for step in range(n):
        for (forward, back), steps in zip(found, forward_steps):
            if step < steps:
                forward.append(lax.ppermute(forward[-1], "fs", ahead))
            if step < n - 1 - steps:
                back.append(lax.ppermute(back[-1], "fs", behind))
    return [forward + back[:0:-1] for forward, back in found]


def chained(shards, before, hops):
    if not before:
        return shards
    last = []
    n = len(before[0])
    for pieces in before:
        last.extend([pieces[hops], pieces[n - hops]])
    return lax.optimization_barrier((tuple(shards), tuple(last)))[0]


def with_scale(weight, scale):
    high = lax.reduce_precision(scale, 8, 7)
    middle = lax.reduce_precision(scale - high, 8, 7)
    rows = jnp.stack([high, middle, scale - high - middle]).astype(jnp.bfloat16)
    return jnp.concatenate([weight, jnp.pad(rows, ((0, 13), (0, 0)))], axis=0)


def without_scale(pieces):
    size = pieces[0].shape[0] - 16
    weight = jnp.concatenate([p[:size] for p in pieces], axis=1)
    rows = jnp.concatenate([p[size:] for p in pieces], axis=1)[:3].astype(jnp.float32)
    return weight, rows[0] + rows[1] + rows[2]


def retain(query, key_rows, value, decay, head_gain):
    seq_len = query.shape[0]
    row = lax.broadcasted_iota(jnp.int32, (seq_len, seq_len), 0)
    col = lax.broadcasted_iota(jnp.int32, (seq_len, seq_len), 1)
    distance = jnp.abs(row - col).astype(jnp.float32)
    weight = jnp.where(col // BLOCK <= row // BLOCK, jnp.exp(-decay * distance), 0.0)
    scores = lax.dot_general(
        query, key_rows, (((1,), (1,)), ((), ())), preferred_element_type=jnp.float32
    )
    scores = (scores * weight).astype(jnp.bfloat16)
    retained = jnp.dot(scores, value, preferred_element_type=jnp.float32)
    centred = retained - jnp.mean(retained, axis=-1, keepdims=True)
    normed = (
        centred
        * lax.rsqrt(jnp.mean(centred * centred, axis=-1, keepdims=True) + EPSILON)
        * head_gain
    )
    return normed.astype(jnp.bfloat16)


def on_device(
    n_rep,
    n_fs,
    n_tp,
    tokens_in,
    norm_gains,
    gate_w,
    gate_scale,
    up_w,
    up_scale,
    down_w,
    down_scale,
    query_w,
    query_scale,
    key_w,
    key_scale,
    value_w,
    value_scale,
    out_w,
    out_scale,
    head_gain,
    decay_rate,
):
    rows = tokens_in.shape[0]
    width = gate_w.shape[0]
    heads = decay_rate.shape[0]
    units = gate_w.shape[1]
    share = n_rep if heads % n_rep == 0 and units % (n_rep * 128) == 0 else 1
    heads //= share
    units //= share
    rep = lax.axis_index("rep") if share > 1 else 0
    tp = lax.axis_index("tp")
    place = snake_place(lax.axis_index("fs"), n_fs)

    def part(x, axis):
        size = x.shape[axis] // share
        return lax.dynamic_slice_in_dim(x, rep * size, size, axis)

    gate_b, up_b, query_b, key_b, value_b = (
        part(w, 1).astype(jnp.bfloat16) for w in (gate_w, up_w, query_w, key_w, value_w)
    )
    down_b, out_b = (part(w, 0).astype(jnp.bfloat16) for w in (down_w, out_w))

    few, many = (n_fs - 1) // 2, n_fs // 2
    first_pieces = ring_gather([gate_b, up_b], n_fs, [many, few])
    half = down_b.shape[0] // 2
    second_pieces = ring_gather(
        chained([with_scale(down_b[:half], down_scale), down_b[half:]], first_pieces, max(1, n_fs // 4)),
        n_fs,
        [many, few],
    )
    third_pieces = ring_gather(chained([query_b, key_b], second_pieces, few), n_fs, [many, few])
    value_pieces, out_pieces = ring_gather(
        chained([value_b, with_scale(out_b, out_scale)], third_pieces, few), n_fs, [many, few]
    )

    gate_full, up_full = (jnp.concatenate(p, axis=0) for p in first_pieces)
    down_top, down_cols = without_scale(second_pieces[0])
    down_rest = jnp.concatenate(second_pieces[1], axis=1)
    down_full = lax.optimization_barrier(jnp.concatenate([down_top, down_rest], axis=0))
    query_full, key_full = (jnp.concatenate(p, axis=0) for p in third_pieces)
    value_full = jnp.concatenate(value_pieces, axis=0)
    out_full, out_cols = without_scale(out_pieces)

    def to_ring(x):
        blocks = [
            lax.dynamic_slice_in_dim(
                x, snake_index((place - k) % n_fs, n_fs) * width, width, axis=1
            )
            for k in range(n_fs)
        ]
        return jnp.concatenate(blocks, axis=1)

    def from_ring(x):
        blocks = [
            lax.dynamic_slice_in_dim(x, (place - snake(n_fs).index(o)) % n_fs * width, width, axis=1)
            for o in range(n_fs)
        ]
        return jnp.concatenate(blocks, axis=1)

    def over_tp(x, ordered):
        found = [x] + [shift(x, "tp", n_tp, k) for k in range(1, n_tp)]
        if not ordered:
            return jnp.concatenate(found, axis=0)
        twice = jnp.concatenate(found[::-1] * 2, axis=0)
        return lax.dynamic_slice_in_dim(twice, (n_tp - 1 - tp) * rows, n_tp * rows, axis=0)

    def gather_rows(normed, ordered=False):
        found = [normed] + [shift(normed, "rep", n_rep, k) for k in range(1, share)]
        return [over_tp(x, ordered) for x in found]

    def return_rows(parts, ordered=False):
        total = None
        for k in range(share - 1, -1, -1):

            def block(j):
                at = (tp - j) % n_tp * rows if ordered else j * rows
                return lax.dynamic_slice_in_dim(parts[k], at, rows, axis=0)

            mine = block(0)
            for j in range(1, n_tp):
                other = shift(block(j).astype(jnp.bfloat16), "tp", n_tp, n_tp - j)
                mine = mine + other.astype(jnp.float32)
            if k > 0:
                mine = shift(mine.astype(jnp.bfloat16), "rep", n_rep, n_rep - k).astype(jnp.float32)
            total = mine if total is None else total + mine
        return total

    def dot(a, b):
        return jnp.dot(a, b, preferred_element_type=jnp.float32)

    gate_col, up_col = part(gate_scale, 0), part(up_scale, 0)

    def feed_forward(stream, gain):
        parts = []
        for gathered in gather_rows(rms_scale(stream, gain).astype(jnp.bfloat16)):
            gate_value = dot(gathered, gate_full) * gate_col
            up_value = dot(gathered, up_full) * up_col
            hidden = (jax.nn.silu(gate_value) * up_value).astype(jnp.bfloat16)
            hidden = lax.optimization_barrier(hidden)
            parts.append(dot(hidden, down_full) * down_cols)
        return return_rows(parts)

    query_col, key_col, value_col = (part(s, 0) for s in (query_scale, key_scale, value_scale))
    decay = part(decay_rate, 0)
    gains = to_ring(norm_gains)

    stream = to_ring(tokens_in).astype(jnp.float32)
    stream = stream + 0.5 * feed_forward(stream, gains[0])
    parts = []
    for gathered in gather_rows(
        rms_scale(stream, gains[1]).astype(jnp.bfloat16), ordered=True
    ):
        query = (dot(gathered, query_full) * query_col).astype(jnp.bfloat16)
        key_rows = (dot(gathered, key_full) * key_col / math.sqrt(DK)).astype(jnp.bfloat16)
        value = (dot(gathered, value_full) * value_col).astype(jnp.bfloat16)
        mixed = [
            retain(
                query[:, h * DK : (h + 1) * DK],
                key_rows[:, h * DK : (h + 1) * DK],
                value[:, h * DV : (h + 1) * DV],
                decay[h],
                head_gain,
            )
            for h in range(heads)
        ]
        parts.append(dot(jnp.concatenate(mixed, axis=1), out_full) * out_cols)
    stream = stream + return_rows(parts, ordered=True)
    stream = stream + 0.5 * feed_forward(stream, gains[2])
    return from_ring(stream.astype(jnp.bfloat16))


MESH = pl.DeviceIdType.MESH
VMEM_LIMIT = 62 * 1024 * 1024


def fits(n_rep, n_fs, n_tp, tokens_in, norm_gains, gate_w, *rest):
    rows, features = tokens_in.shape
    width, units = gate_w.shape
    heads = rest[-1].shape[0]
    return (
        n_rep == 2
        and n_tp == 2
        and n_fs >= 6
        and n_fs % 2 == 0
        and n_fs <= 16
        and rows % 128 == 0
        and width % 256 == 0
        and features == n_fs * width
        and units % 512 == 0
        and heads % 2 == 0
    )


def layer_kernel(
    n,
    tokens_in,
    norm_gains_in,
    gate_w,
    gate_scale_in,
    up_w,
    up_scale_in,
    down_w,
    down_scale_in,
    query_w,
    query_scale_in,
    key_w,
    key_scale_in,
    value_w,
    value_scale_in,
    out_w,
    out_scale_in,
    head_gain_in,
    decay_rate,
    result,
    norm_gains,
    gate_scale,
    up_scale,
    down_scale,
    query_scale,
    key_scale,
    value_scale,
    out_scale,
    head_gain,
    staged_in,
    staged_gate,
    staged_up,
    staged_down,
    staged_query,
    staged_key,
    staged_value,
    staged_out,
    gate_away,
    up_away,
    down_away,
    head_away,
    out_away,
    cols_away,
    gate_full,
    up_full,
    down_full,
    head_full,
    out_full,
    cols_full,
    gathered,
    factors,
    stream,
    squares,
    summed,
    projected,
    hidden,
    mixed,
    own_part,
    far_part,
    tp_out,
    tp_in,
    rep_out,
    rep_in,
    local_sem,
    side_send,
    side_recv,
    line_send,
    line_recv,
    twin_recv,
    part_send,
    part_recv,
    row_send,
    row_recv,
    block_send,
    block_recv,
):
    f32, bf16 = jnp.float32, jnp.bfloat16
    rows, features = tokens_in.shape
    width = gate_w.shape[0]
    units = hidden.shape[1]
    heads = head_full.shape[0]
    tile = 256

    twin, fs, tp = (lax.axis_index(axis) for axis in ("rep", "fs", "tp"))
    line = n // 2
    side, spot = lax.rem(fs, 2), lax.div(fs, 2)
    above, below = {"fs": fs + 2}, {"fs": fs - 2}
    side_peer, twin_peer, tp_peer = {"fs": fs + 1 - 2 * side}, {"rep": 1 - twin}, {"tp": 1 - tp}
    has_above, has_below = spot + 1 < line, spot > 0

    barrier = pltpu.get_barrier_semaphore()

    def greet(peer):
        pl.semaphore_signal(barrier, inc=1, device_id=peer, device_id_type=MESH)

    def meet():
        for peer in (side_peer, twin_peer, tp_peer):
            greet(peer)
        pl.when(has_above)(lambda: greet(above))
        pl.when(has_below)(lambda: greet(below))

    def columns_of(f):
        return pl.ds(pl.multiple_of(f * width, width), width)

    def halves(size):
        return [pl.ds(pl.multiple_of(i * size, 128), size) for i in (side, 1 - side)]

    local, copies_of = [], {}

    def fetch(name, src, dst):
        copy = pltpu.make_async_copy(src, dst, local_sem.at[len(local)])
        copy.start()
        copies_of.setdefault(name, []).append(copy)
        local.append(copy)

    def fetched(name):
        for copy in copies_of[name]:
            copy.wait()

    gate_halves = halves(units)
    fetch(("gate", 0), gate_w.at[:, gate_halves[0]], staged_gate.at[0])
    meet()
    fetch(("gate", 1), gate_w.at[:, gate_halves[1]], staged_gate.at[1])
    for i, cols in enumerate(halves(units)):
        fetch(("up", i), up_w.at[:, cols], staged_up.at[i])
    fetch("rows", tokens_in, staged_in)
    for src, dst in (
        (gate_scale_in, gate_scale),
        (up_scale_in, up_scale),
        (down_scale_in, down_scale),
        (query_scale_in, query_scale),
        (key_scale_in, key_scale),
        (value_scale_in, value_scale),
        (out_scale_in, out_scale),
        (head_gain_in, head_gain),
    ):
        fetch("small", src, dst.at[0])
    fetch("small", norm_gains_in, norm_gains)
    for i, cols in enumerate(halves(units)):
        fetch("down", down_w.at[cols, :], staged_down.at[i])
    for i, cols in enumerate(halves(heads * DK)):
        fetch("heads", query_w.at[:, cols], staged_query.at[i])
        fetch("heads", key_w.at[:, cols], staged_key.at[i])
    for i, cols in enumerate(halves(heads * DV)):
        fetch("heads", value_w.at[:, cols], staged_value.at[i])
        fetch("out", out_w.at[cols, :], staged_out.at[i])

    started = []
    half_units, half_width, half_out = units // 2, width // 2, heads * DV // 2

    def rows_of(f):
        return pl.ds(pl.multiple_of(f * width, width), width)

    def cut(ref, s, size):
        return ref.at[pl.ds(pl.multiple_of(s * size, size), size), :]

    def half_rows(f, i):
        return pl.ds(pl.multiple_of(f * width + i * half_width, half_width), half_width)

    kinds, head_kinds = [], []
    for i in range(2):
        kinds.append(
            (
                lambda f, i=i: gate_full.at[half_rows(f, i), :],
                gate_away.at[pl.ds(i * half_width, half_width), :],
                half_width // 2,
            )
        )
    kinds.append((lambda f: up_full.at[rows_of(f), :], up_away, half_width))
    kinds.append((lambda f: down_full.at[f], down_away, half_units))
    up_kind, down_kind = 2, 3
    for h in range(heads):
        head_kinds.append([len(kinds)])
        kinds.append(
            (lambda f, h=h: head_full.at[h, rows_of(f), :], head_away.at[h], half_width)
        )
    out_kind = len(kinds)
    kinds.append((lambda f: out_full.at[f], out_away, half_out))
    scales = len(kinds)
    kinds.append((lambda f: cols_full.at[f], cols_away, 8))
    rounds = [[0, 1, up_kind], [down_kind, scales], *head_kinds, [out_kind]]
    bank_of, last_bank = {}, 0
    for members in rounds:
        for kind in members:
            bank_of[kind] = last_bank
            last_bank = (last_bank + 1) % 3

    def piece(kind, f, s):
        if kind == scales:
            return kinds[kind][0](f).at[pl.ds(pl.multiple_of(s * 8, 8), 1), :]
        return cut(kinds[kind][0](f), s, kinds[kind][2])

    def remote(src, dst, send_sem, recv_sem, peer):
        return pltpu.make_async_remote_copy(
            src_ref=src,
            dst_ref=dst,
            send_sem=send_sem,
            recv_sem=recv_sem,
            device_id=peer,
            device_id_type=MESH,
        )

    def across(o):
        return spot * 2 + side + o * (1 - 2 * side)

    def side_slot(kind, i):
        return kind * 2 + i if kind <= up_kind else kind + 3

    def side_copy(kind, i, f):
        slot_of = side_slot(kind, i)
        sems = side_send.at[slot_of], side_recv.at[slot_of]
        if kind <= up_kind:
            s = twin if i == 0 else 1 - twin
            return remote(
                cut(kinds[kind][1], s, kinds[kind][2]), piece(kind, f, s), *sems, side_peer
            )
        return remote(kinds[kind][1], kinds[kind][0](f), *sems, side_peer)

    def side_start(kind, i=0):
        copy = side_copy(kind, i, fs)
        copy.start()
        started.append(copy)

    side_done = set()

    def side_need(kind, i):
        i = i if kind <= up_kind else 0
        if (kind, i) not in side_done:
            side_done.add((kind, i))
            side_copy(kind, i, across(1)).wait_recv()

    span_of = 2 * (line - 1)
    sending = {}

    def push(kind, group, index, f, where, recv, peer):
        bank = bank_of[kind]
        slot_of = (bank * 3 + group) * span_of + index
        copy = remote(piece(kind, f, twin), piece(kind, f, twin), line_send.at[slot_of], recv, peer)
        if slot_of in sending:
            sending.pop(slot_of)()
        guard = functools.partial(pl.when, where) if where is not None else None

        def begin():
            copy.start()

        def finish():
            copy.wait_send()

        if guard is None:
            begin()
            sending[slot_of] = finish
        else:
            guard()(begin)
            sending[slot_of] = lambda: guard()(finish)

    def line_slot(kind, away, o):
        return line_recv.at[kind * span_of + (away % line - 1) * 2 + o]

    def twin_slot(kind, away, o):
        return twin_recv.at[kind * span_of + (away - 1) * 2 + o]

    def send_own(kind, o):
        if o == 1:
            side_need(kind, 0)
        f = across(o)
        push(kind, 0, o, f, has_above, line_slot(kind, -1, o), above)
        push(kind, 1, o, f, has_below, line_slot(kind, 1, o), below)

    def places(d, o):
        for group, away in ((1, d), (0, -d)):
            from_spot = spot + away
            exists = from_spot >= 0 if away < 0 else from_spot < line
            yield group, away, exists, from_spot * 2 + side + o * (1 - 2 * side)

    def take_in(kind, d, o):
        for group, away, exists, f in places(d, o):

            def receive(kind=kind, away=away, f=f):
                remote(
                    piece(kind, f, twin),
                    piece(kind, f, twin),
                    line_send.at[0],
                    line_slot(kind, away, o),
                    above,
                ).wait_recv()

            pl.when(exists)(receive)
            hand_over(kind, away, o, f, exists)

    def move_on(kind, d, o):
        if d > line - 2:
            return
        for group, away, exists, f in places(d, o):
            further = -d - 1 if away < 0 else d + 1
            push(
                kind,
                group,
                2 * d + o,
                f,
                jnp.logical_and(exists, has_above if away < 0 else has_below),
                line_slot(kind, further, o),
                above if away < 0 else below,
            )

    def pass_along(kind, d, o):
        take_in(kind, d, o)
        move_on(kind, d, o)

    def hand_over(kind, away, o, f, exists):
        index = (away % line - 1) * 2 + o
        bank = bank_of[kind]
        slot_of = (bank * 3 + 2) * span_of + index
        first = away > 0
        copy = remote(
            piece(kind, f, twin),
            piece(kind, f, twin),
            line_send.at[slot_of],
            twin_slot(kind, away % line, o),
            twin_peer,
        )
        key = (slot_of, first)
        if key in sending:
            sending.pop(key)()
        pl.when(exists)(lambda: copy.start())
        sending[key] = lambda: pl.when(exists)(lambda: copy.wait_send())

    def pick(table):
        total = 0
        for v in range(line):
            total = total + (spot == v).astype(jnp.int32) * table[v]
        return total

    near = []
    for v in range(line):
        near.append(sorted((u for u in range(line) if u != v), key=lambda u: (abs(u - v), -u)))
    sources = [across(0), across(1)]
    twin_index = [None, None]
    for r in range(line - 1):
        at = pick([near[v][r] for v in range(line)])
        away = pick([(near[v][r] - v) % line for v in range(line)])
        for o in range(2):
            sources.append(at * 2 + side + o * (1 - 2 * side))
            twin_index.append((away - 1) * 2 + o)

    def need_piece(kind, k):
        if k == 1:
            side_need(kind, 0)
            side_need(kind, 1)
        if k > 1:
            remote(
                piece(kind, sources[k], 1 - twin),
                piece(kind, sources[k], 1 - twin),
                line_send.at[0],
                twin_recv.at[kind * span_of + twin_index[k]],
                twin_peer,
            ).wait_recv()

    spots = [spot] + [lax.div(sources[2 * r], 2) for r in range(1, line)]
    queue = []
    later = []
    for members in rounds:
        for o in range(2):
            queue.append([functools.partial(send_own, m, o) for m in members])
        queue.extend(later)
        later = []
        for d in range(1, line):
            for o in range(2):
                unit = [functools.partial(pass_along, m, d, o) for m in members]
                (queue if d < line - 1 else later).append(unit)
    queue.extend(later)
    middle = 2 * (line - 2)

    def pump(count):
        for _ in range(count):
            for action in queue.pop(0):
                action()

    def send(src, dst, send_sem, recv_sem, peer):
        copy = remote(src, dst, send_sem, recv_sem, peer)
        copy.start()
        started.append(copy)
        return copy

    own_rows = rows_of(fs)
    fetched(("gate", 0))
    gate_full[own_rows, :] = staged_gate[0].astype(bf16)
    neighbours = has_above.astype(jnp.int32) + has_below.astype(jnp.int32)
    pl.semaphore_wait(barrier, 3 + neighbours)
    first, second, _ = (queue.pop(0) for _ in range(3))
    first[0]()
    first[1]()
    fetched(("gate", 1))
    gate_away[...] = staged_gate[1].astype(bf16)
    side_start(0)
    side_start(1)
    fetched(("up", 0))
    up_full[own_rows, :] = staged_up[0].astype(bf16)
    first[2]()
    fetched(("up", 1))
    up_away[...] = staged_up[1].astype(bf16)
    side_start(up_kind)
    fetched("rows")
    fetched("small")

    def norm_rows(source, which, target):
        gain = norm_gains[which : which + 1, :]

        def step(i, carry):
            block = pl.ds(pl.multiple_of(i * 16, 16), 16)
            x = source[block, :].astype(f32)
            mean = jnp.mean(x * x, axis=-1, keepdims=True)
            target[block, :] = (x * lax.rsqrt(mean + EPSILON) * gain).astype(bf16)
            return carry

        lax.fori_loop(0, rows // 16, step, 0)

    def slot(j, cols=slice(None)):
        return (pl.ds(j * rows, rows), cols)

    def share_rows(stage):
        part = gathered.at[stage]
        base = 3 * stage
        send(part.at[slot(0)], part.at[slot(1)], row_send.at[base], row_recv.at[base], tp_peer)
        send(
            part.at[slot(0)],
            part.at[slot(2)],
            row_send.at[base + 1],
            row_recv.at[base + 1],
            side_peer,
        )

    def wait_rows(stage, i, j):
        part = gathered.at[stage]
        pltpu.make_async_remote_copy(
            src_ref=part.at[slot(0)],
            dst_ref=part.at[slot(j)],
            send_sem=row_send.at[3 * stage + i],
            recv_sem=row_recv.at[3 * stage + i],
            device_id=tp_peer,
            device_id_type=MESH,
        ).wait_recv()

    def relay_rows(stage):
        wait_rows(stage, 1, 2)
        part = gathered.at[stage]
        send(
            part.at[slot(2)],
            part.at[slot(3)],
            row_send.at[3 * stage + 2],
            row_recv.at[3 * stage + 2],
            tp_peer,
        )

    norm_rows(staged_in, 0, gathered.at[0])
    stream[...] = staged_in[...].astype(f32)
    fetched("down")
    down_full[fs] = staged_down[0].astype(bf16)
    down_away[...] = staged_down[1].astype(bf16)
    cols_full[fs, 0:1, :] = down_scale[...]
    cols_full[fs, 8:9, :] = out_scale[...]
    cols_away[0:1, :] = down_scale[...]
    cols_away[8:9, :] = out_scale[...]
    side_start(0, 1)
    side_start(1, 1)
    side_start(up_kind, 1)
    side_start(down_kind)
    side_start(scales)
    take_in(0, 1, 0)
    take_in(1, 1, 0)
    second[0]()
    second[1]()
    take_in(up_kind, 1, 0)
    second[2]()
    move_on(0, 1, 0)
    move_on(1, 1, 0)
    move_on(up_kind, 1, 0)
    share_rows(0)
    fetched("heads")
    for h in range(heads):
        keys, vals = slice(h * DK, (h + 1) * DK), slice(h * DV, (h + 1) * DV)
        for i in range(2):
            made = jnp.concatenate(
                [staged_query[i, :, keys], staged_key[i, :, keys], staged_value[i, :, vals]], axis=1
            ).astype(bf16)
            if i == 0:
                head_full[h, own_rows, :] = made
            else:
                head_away[h] = made
        for kind in head_kinds[h]:
            side_start(kind)
    fetched("out")
    out_full[fs] = staged_out[0].astype(bf16)
    out_away[...] = staged_out[1].astype(bf16)
    side_start(out_kind)

    pump(middle + 2)
    relay_rows(0)
    pump(middle + 1)
    wait_rows(0, 0, 1)
    wait_rows(0, 2, 3)

    def dot(a, b):
        return jnp.dot(a, b, preferred_element_type=f32)

    def expand(factor, part, first=0, count=4 * rows):
        for c in range(units // tile):
            cols = slice(c * tile, (c + 1) * tile)
            span = pl.ds(pl.multiple_of(side * units + c * tile, 128), tile)
            rows_in, lhs = part
            block = slice(first, first + count)
            gate = dot(lhs[block], gate_full[rows_in, cols])
            up = dot(lhs[block], up_full[rows_in, cols])
            if factor is not None:
                gate = (gate + summed[0, block, cols]) * factor[block]
                up = (up + summed[1, block, cols]) * factor[block]
            gate, up = gate * gate_scale[:, span], up * up_scale[:, span]
            hidden[block, cols] = (gate / (1.0 + jnp.exp(-gate)) * up).astype(bf16)

    def part_copy(stage, k, way, landing):
        store_out, store_in = (rep_out, rep_in) if way == 2 else (tp_out, tp_in)
        return remote(
            store_out.at[stage, k] if way == 2 else store_out.at[stage, k, way],
            store_in.at[stage, landing] if way == 2 else store_in.at[stage, landing, way],
            part_send.at[stage * 2 + way // 2],
            part_recv.at[landing * 3 + way],
            side_peer if way == 2 else tp_peer,
        )

    def part_start(stage, k, way):
        part_copy(stage, k, way, k ^ 1 if way == 2 else k).start()

    def part_wait(stage, k, way):
        part_copy(stage, k, way, k).wait_recv()

    def parts_sent(stage):
        for over_side, (src, dst) in enumerate(((tp_out, tp_in), (rep_out, rep_in))):
            remote(
                src.at[stage],
                dst.at[stage],
                part_send.at[stage * 2 + over_side],
                part_recv.at[0],
                side_peer,
            ).wait_send()

    def contract(stage, lhs, weight, row, fresh, order, finish, relay=None, extra=None, near=None):
        def ready(k):
            if fresh is not None:
                need_piece(fresh, k)
                if fresh == down_kind:
                    need_piece(scales, k)

        def product(k, block):
            f = sources[k]
            return dot(lhs[block, :], weight[f]) * cols_full[f, 8 * row : 8 * row + 1, :]

        def keep(k, way, part):
            (far_part if way else own_part)[k] = part[:rows]
            tp_out[stage, k, way] = part[rows:].astype(bf16)
            part_start(stage, k, way)

        def multiply(k):
            ready(k)
            part = product(k, slice(None))
            keep(k, 1, part[2 * rows :])
            keep(k, 0, part[: 2 * rows])

        def multiply_far(k):
            ready(k)
            keep(k, 1, product(k, slice(2 * rows, 4 * rows)))

        def multiply_near(k):
            keep(k, 0, product(k, slice(0, 2 * rows)))

        def pass_on(k):
            part_wait(stage, k, 1)
            rep_out[stage, k] = (far_part[k] + tp_in[stage, k, 1].astype(f32)).astype(bf16)
            part_start(stage, k, 2)

        def collect(k):
            part_wait(stage, k, 0)
            part_wait(stage, k, 2)
            total = own_part[k] + tp_in[stage, k, 0].astype(f32) + rep_in[stage, k].astype(f32)
            finish(k, sources[k], total)

        actions = {"m": multiply, "p": pass_on, "c": collect, "r": relay, "u": pump, "x": extra}
        actions.update({"f": multiply_far, "n": multiply_near, "near": lambda _: near()})
        for action, k in order:
            actions[action](k)

    def last_order():
        order = []
        for k in range(n):
            order.append(("f", k))
            if k > 0:
                order.append(("p", k - 1))
        order += [("p", n - 1), ("near", 0)]
        return order + [("n", k) for k in range(n)] + [("c", k) for k in range(n)]

    def first_order():
        order = [("m", 0), ("m", 1), ("p", 0), ("p", 1), ("u", 4)]
        for k in range(2, n):
            if k == 2 * (line - 1):
                order.append(("u", 2))
            order.append(("m", k))
            if k > 2:
                order.append(("p", k - 1))
        order.append(("p", n - 1))
        order += [("c", k) for k in range(n)]
        order.insert(-2, ("u", 1))
        return order

    def tail_order():
        order, waiting, relayed = [], [], []

        def advance(r):
            ks = (2 * r, 2 * r + 1)
            order.extend([("m", k) for k in ks] + [("p", k) for k in ks])
            waiting.append(ks)

        def take():
            if waiting:
                ks = waiting.pop(0)
                order.extend(("c", k) for k in ks)
                relayed.append(ks)

        order.extend([("m", 0), ("m", 1), ("u", 1), ("p", 0), ("p", 1)])
        order.extend([("m", 2), ("m", 3), ("p", 2), ("p", 3), ("c", 0), ("c", 1)])
        waiting.append((2, 3))
        relayed.append((0, 1))
        for r in range(3, line):
            order.append(("u", 1))
            take()
            order.append(("u", 1))
            advance(r - 1)
        for ks in relayed[:1]:
            order.extend(("r", k) for k in relayed.pop(0))
        advance(line - 1)
        while waiting:
            take()
            order.extend(("r", k) for k in relayed.pop(0))
        order.extend(("r", k) for ks in relayed for k in ks)
        for r in range(line - 2):
            order.insert(order.index(("r", 2 * r + 3)) + 1, ("x", r))
        return order

    def need_all(kind):
        for k in range(1, n):
            need_piece(kind, k)

    need_all(0)
    need_all(1)
    need_all(up_kind)
    expand(None, (slice(None), gathered[0]))

    def add_half(k, f, total):
        cols = columns_of(f)
        stream[:, cols] = stream[:, cols] + 0.5 * total

    contract(0, hidden, down_full, 0, down_kind, first_order(), add_half)

    norm_rows(stream, 1, gathered.at[1])
    share_rows(1)
    pump(middle + 1)
    relay_rows(1)
    pump(2)

    seq_len = 2 * rows
    row = lax.rem(
        lax.broadcasted_iota(jnp.int32, (seq_len, seq_len), 0) + tp * rows, seq_len
    )
    col = lax.rem(
        lax.broadcasted_iota(jnp.int32, (seq_len, seq_len), 1) + tp * rows, seq_len
    )

    def retain(h):
        places = [
            (query_scale, 0, DK, 1.0),
            (key_scale, DK, DK, 1.0 / math.sqrt(DK)),
            (value_scale, 2 * DK, DV, 1.0),
        ]
        for r in range(line):
            for k in (2 * r, 2 * r + 1):
                for kind in head_kinds[h]:
                    need_piece(kind, k)
            rows_in = pl.ds(pl.multiple_of(spots[r] * 2 * width, 2 * width), 2 * width)
            lhs, made = gathered[1, :, rows_in], []
            for scale, first, size, factor in places:
                cols = slice(first, first + size)
                product = dot(lhs, head_full[h, rows_in, cols])
                if r > 0:
                    product = product + projected[:, cols]
                if r < line - 1:
                    projected[:, cols] = product
                else:
                    span = pl.ds(pl.multiple_of((side * heads + h) * size, 128), size)
                    made.append((product * (scale[:, span] * factor)).astype(bf16))
        query, keys, values = made
        decay = decay_rate[side * heads + h]
        distance = jnp.abs(row - col).astype(f32)
        weight = jnp.where(
            lax.div(col, BLOCK) <= lax.div(row, BLOCK), jnp.exp(-decay * distance), 0.0
        )
        for s in range(2):
            span = slice(s * seq_len, (s + 1) * seq_len)
            scores = lax.dot_general(
                query[span], keys[span], (((1,), (1,)), ((), ())), preferred_element_type=f32
            )
            scores = (scores * weight).astype(bf16)
            retained = dot(scores, values[span])
            centred = retained - jnp.mean(retained, axis=-1, keepdims=True)
            spread = jnp.mean(centred * centred, axis=-1, keepdims=True)
            mixed[span, h * DV : (h + 1) * DV] = (
                centred * lax.rsqrt(spread + EPSILON) * head_gain[...]
            ).astype(bf16)

    for h in range(heads):
        if h == 0:
            wait_rows(1, 0, 1)
            wait_rows(1, 2, 3)
        retain(h)
        pump(1)
        if h < heads - 1:
            pump(middle - 3 + 6)

    last = gathered.at[2]

    def block_copy(k, i, start):
        cols = columns_of(sources[k])
        a, b, peer = ((0, 1, tp_peer), (0, 2, side_peer), (2, 3, tp_peer))[i]
        return pltpu.make_async_remote_copy(
            src_ref=last.at[slot(a, cols)],
            dst_ref=last.at[slot(b, cols)],
            send_sem=block_send.at[i],
            recv_sem=block_recv.at[3 * (k ^ 1 if i == 1 and start else k) + i],
            device_id=peer,
            device_id_type=MESH,
        )

    def factor_copy(i):
        a, b, peer = ((0, 1, tp_peer), (0, 2, side_peer), (2, 3, tp_peer))[i]
        return pltpu.make_async_remote_copy(
            src_ref=factors.at[a],
            dst_ref=factors.at[b],
            send_sem=block_send.at[3 + i],
            recv_sem=block_recv.at[3 * n + i],
            device_id=peer,
            device_id_type=MESH,
        )

    squares[...] = jnp.zeros_like(squares)

    def add_mix(k, f, total):
        cols = columns_of(f)
        second = stream[:, cols] + total
        stream[:, cols] = second
        last[slot(0, cols)] = (second * norm_gains[2:3, cols]).astype(bf16)
        square = second * second
        added = squares[...]
        for i in range(width // 128):
            added = added + square[:, i * 128 : (i + 1) * 128]
        squares[...] = added
        for i in (0, 1):
            block_copy(k, i, True).start()
        if k == n - 1:
            mean = jnp.sum(added, axis=-1, keepdims=True) / features
            wide = jnp.broadcast_to(lax.rsqrt(mean + EPSILON), (rows, rows))
            factors[0] = wide.T[:8, :]
            for i in (0, 1):
                copy = factor_copy(i)
                copy.start()
                started.append(copy)

    def relay_block(k):
        block_copy(k, 1, False).wait_recv()
        block_copy(k, 2, True).start()
        if k == n - 1:
            factor_copy(1).wait_recv()
            copy = factor_copy(2)
            copy.start()
            started.append(copy)


    def arrived_block(r):
        for k in (2 * r, 2 * r + 1):
            block_copy(k, 0, False).wait_recv()
            block_copy(k, 2, False).wait_recv()
        return pl.ds(pl.multiple_of(spots[r] * 2 * width, 2 * width), 2 * width)

    def take_sum(r):
        rows_in = arrived_block(r)
        lhs = last[:, rows_in]
        for c in range(units // tile):
            cols = slice(c * tile, (c + 1) * tile)
            for i, weight in enumerate((gate_full, up_full)):
                part = dot(lhs, weight[rows_in, cols])
                summed[i, :, cols] = part if r == 0 else summed[i, :, cols] + part

    contract(1, mixed, out_full, 1, out_kind, tail_order(), add_mix, relay_block, take_sum)
    take_sum(line - 2)
    rows_in = arrived_block(line - 1)
    factor_copy(0).wait_recv()
    factor_copy(2).wait_recv()
    factor = jnp.concatenate(
        [jnp.broadcast_to(factors[j, 0:1, :], (rows, rows)).T[:, 0:1] for j in range(4)], axis=0
    )
    late = (rows_in, last[:, rows_in])
    expand(factor, late, 2 * rows, 2 * rows)

    def write(k, f, total):
        cols = columns_of(f)
        result[:, cols] = (stream[:, cols] + 0.5 * total).astype(bf16)

    contract(2, hidden, down_full, 0, None, last_order(), write, near=lambda: expand(factor, late, 0, 2 * rows))
    assert not queue
    for stage in range(3):
        parts_sent(stage)
    for i, a in enumerate((0, 0, 2)):
        remote(
            last.at[slot(a)], last.at[slot(a)], block_send.at[i], block_recv.at[0], tp_peer
        ).wait_send()
    for finish in sending.values():
        finish()
    for copy in started:
        copy.wait_send()


def fused(
    n_rep,
    n_fs,
    n_tp,
    tokens_in,
    norm_gains,
    gate_w,
    gate_scale,
    up_w,
    up_scale,
    down_w,
    down_scale,
    query_w,
    query_scale,
    key_w,
    key_scale,
    value_w,
    value_scale,
    out_w,
    out_scale,
    head_gain,
    decay_rate,
):
    f32, bf16 = jnp.float32, jnp.bfloat16
    n = n_fs
    rows, features = tokens_in.shape
    width, units = gate_w.shape[0], gate_w.shape[1] // 2
    heads = decay_rate.shape[0] // 2
    kinds = heads + 6
    span_of = n - 2
    any_space = pl.BlockSpec(memory_space=pl.ANY)
    vmem = pl.BlockSpec(memory_space=pltpu.VMEM)
    smem = pl.BlockSpec(memory_space=pltpu.SMEM)
    dma = pltpu.SemaphoreType.DMA

    return pl.pallas_call(
        functools.partial(layer_kernel, n),
        out_shape=pltpu.VMEM((rows, features), bf16),
        in_specs=[any_space] * 17 + [smem],
        out_specs=vmem,
        scratch_shapes=[
            pltpu.VMEM(norm_gains.shape, f32),
        ]
        + [
            pltpu.VMEM((1, x.shape[0]), f32)
            for x in (
                gate_scale,
                up_scale,
                down_scale,
                query_scale,
                key_scale,
                value_scale,
                out_scale,
                head_gain,
            )
        ]
        + [
            pltpu.VMEM((rows, features), bf16),
            pltpu.VMEM((2, width, units), f32),
            pltpu.VMEM((2, width, units), f32),
            pltpu.VMEM((2, units, width), f32),
            pltpu.VMEM((2, width, heads * DK), f32),
            pltpu.VMEM((2, width, heads * DK), f32),
            pltpu.VMEM((2, width, heads * DV), f32),
            pltpu.VMEM((2, heads * DV, width), f32),
            pltpu.VMEM((width, units), bf16),
            pltpu.VMEM((width, units), bf16),
            pltpu.VMEM((units, width), bf16),
            pltpu.VMEM((heads, width, 2 * DK + DV), bf16),
            pltpu.VMEM((heads * DV, width), bf16),
            pltpu.VMEM((16, width), f32),
            pltpu.VMEM((features, units), bf16),
            pltpu.VMEM((features, units), bf16),
            pltpu.VMEM((n, units, width), bf16),
            pltpu.VMEM((heads, features, 2 * DK + DV), bf16),
            pltpu.VMEM((n, heads * DV, width), bf16),
            pltpu.VMEM((n, 16, width), f32),
            pltpu.VMEM((3, 4 * rows, features), bf16),
            pltpu.VMEM((4, 8, rows), f32),
            pltpu.VMEM((rows, features), f32),
            pltpu.VMEM((rows, 128), f32),
            pltpu.VMEM((2, 4 * rows, units), f32),
            pltpu.VMEM((4 * rows, 2 * DK + DV), f32),
            pltpu.VMEM((4 * rows, units), bf16),
            pltpu.VMEM((4 * rows, heads * DV), bf16),
            pltpu.VMEM((n, rows, width), f32),
            pltpu.VMEM((n, rows, width), f32),
            pltpu.VMEM((3, n, 2, rows, width), bf16),
            pltpu.VMEM((3, n, 2, rows, width), bf16),
            pltpu.VMEM((3, n, rows, width), bf16),
            pltpu.VMEM((3, n, rows, width), bf16),
            dma((24,)),
            dma((kinds + 3,)),
            dma((kinds + 3,)),
            dma((9 * span_of,)),
            dma((kinds * span_of,)),
            dma((kinds * span_of,)),
            dma((6,)),
            dma((3 * n,)),
            dma((6,)),
            dma((6,)),
            dma((6,)),
            dma((3 * n + 3,)),
        ],
        compiler_params=pltpu.CompilerParams(
            collective_id=0, has_side_effects=True, vmem_limit_bytes=VMEM_LIMIT
        ),
        name="layer",
    )(
        tokens_in,
        norm_gains,
        gate_w,
        gate_scale,
        up_w,
        up_scale,
        down_w,
        down_scale,
        query_w,
        query_scale,
        key_w,
        key_scale,
        value_w,
        value_scale,
        out_w,
        out_scale,
        head_gain,
        decay_rate,
    )


def solution(mesh):
    sizes = [mesh.shape[axis] for axis in ("rep", "fs", "tp")]
    placed = (
        P(("rep", "fs", "tp"), None),
        P(),
        P("fs", "tp"),
        P("tp"),
        P("fs", "tp"),
        P("tp"),
        P("tp", "fs"),
        P("fs"),
        P("fs", "tp"),
        P("tp"),
        P("fs", "tp"),
        P("tp"),
        P("fs", "tp"),
        P("tp"),
        P("tp", "fs"),
        P("fs"),
        P(),
        P("tp"),
    )
    return jax.shard_map(
        lambda *args: (fused if fits(*sizes, *args) else on_device)(*sizes, *args),
        mesh=mesh,
        in_specs=placed,
        out_specs=P(("rep", "fs", "tp"), None),
        check_vma=False,
    )
```

```python
import functools
import math

import jax
import jax.numpy as jnp
from jax import lax
from jax.experimental import pallas as pl
from jax.experimental.pallas import tpu as pltpu
from jax.sharding import PartitionSpec as P

DK = 256
DV = 256
BLOCK = 64

EPSILON = 1e-05


def rms_scale(stream, gain):
    return stream * lax.rsqrt(jnp.mean(stream * stream, axis=-1, keepdims=True) + EPSILON) * gain


def snake(n):
    return [i for i in range(0, n, 2)] + [i for i in range(n - 1, 0, -1) if i % 2 == 1]


def snake_place(index, n):
    return jnp.where(index % 2 == 0, index // 2, n - 1 - index // 2)


def snake_index(place, n):
    half = (n + 1) // 2
    return jnp.where(place < half, 2 * place, 2 * (n - 1 - place) + 1)


def shift(x, axis, n, by):
    return lax.ppermute(x, axis, [(i, (i + by) % n) for i in range(n)])


def ring_gather(shards, n, forward_steps):
    order = snake(n)
    ahead = [(order[i], order[(i + 1) % n]) for i in range(n)]
    behind = [(b, a) for a, b in ahead]
    found = []
    for x, steps in zip(shards, forward_steps):
        forward, back = [x], [x]
        found.append((forward, back))
    for step in range(n):
        for (forward, back), steps in zip(found, forward_steps):
            if step < steps:
                forward.append(lax.ppermute(forward[-1], "fs", ahead))
            if step < n - 1 - steps:
                back.append(lax.ppermute(back[-1], "fs", behind))
    return [forward + back[:0:-1] for forward, back in found]


def chained(shards, before, hops):
    if not before:
        return shards
    last = []
    n = len(before[0])
    for pieces in before:
        last.extend([pieces[hops], pieces[n - hops]])
    return lax.optimization_barrier((tuple(shards), tuple(last)))[0]


def with_scale(weight, scale):
    high = lax.reduce_precision(scale, 8, 7)
    middle = lax.reduce_precision(scale - high, 8, 7)
    rows = jnp.stack([high, middle, scale - high - middle]).astype(jnp.bfloat16)
    return jnp.concatenate([weight, jnp.pad(rows, ((0, 13), (0, 0)))], axis=0)


def without_scale(pieces):
    size = pieces[0].shape[0] - 16
    weight = jnp.concatenate([p[:size] for p in pieces], axis=1)
    rows = jnp.concatenate([p[size:] for p in pieces], axis=1)[:3].astype(jnp.float32)
    return weight, rows[0] + rows[1] + rows[2]


def retain(query, key_rows, value, decay, head_gain):
    seq_len = query.shape[0]
    row = lax.broadcasted_iota(jnp.int32, (seq_len, seq_len), 0)
    col = lax.broadcasted_iota(jnp.int32, (seq_len, seq_len), 1)
    distance = jnp.abs(row - col).astype(jnp.float32)
    weight = jnp.where(col // BLOCK <= row // BLOCK, jnp.exp(-decay * distance), 0.0)
    scores = lax.dot_general(
        query, key_rows, (((1,), (1,)), ((), ())), preferred_element_type=jnp.float32
    )
    scores = (scores * weight).astype(jnp.bfloat16)
    retained = jnp.dot(scores, value, preferred_element_type=jnp.float32)
    centred = retained - jnp.mean(retained, axis=-1, keepdims=True)
    normed = (
        centred
        * lax.rsqrt(jnp.mean(centred * centred, axis=-1, keepdims=True) + EPSILON)
        * head_gain
    )
    return normed.astype(jnp.bfloat16)


def on_device(
    n_rep,
    n_fs,
    n_tp,
    tokens_in,
    norm_gains,
    gate_w,
    gate_scale,
    up_w,
    up_scale,
    down_w,
    down_scale,
    query_w,
    query_scale,
    key_w,
    key_scale,
    value_w,
    value_scale,
    out_w,
    out_scale,
    head_gain,
    decay_rate,
):
    rows = tokens_in.shape[0]
    width = gate_w.shape[0]
    heads = decay_rate.shape[0]
    units = gate_w.shape[1]
    share = n_rep if heads % n_rep == 0 and units % (n_rep * 128) == 0 else 1
    heads //= share
    units //= share
    rep = lax.axis_index("rep") if share > 1 else 0
    tp = lax.axis_index("tp")
    place = snake_place(lax.axis_index("fs"), n_fs)

    def part(x, axis):
        size = x.shape[axis] // share
        return lax.dynamic_slice_in_dim(x, rep * size, size, axis)

    gate_b, up_b, query_b, key_b, value_b = (
        part(w, 1).astype(jnp.bfloat16) for w in (gate_w, up_w, query_w, key_w, value_w)
    )
    down_b, out_b = (part(w, 0).astype(jnp.bfloat16) for w in (down_w, out_w))

    few, many = (n_fs - 1) // 2, n_fs // 2
    first_pieces = ring_gather([gate_b, up_b], n_fs, [many, few])
    half = down_b.shape[0] // 2
    second_pieces = ring_gather(
        chained([with_scale(down_b[:half], down_scale), down_b[half:]], first_pieces, max(1, n_fs // 4)),
        n_fs,
        [many, few],
    )
    third_pieces = ring_gather(chained([query_b, key_b], second_pieces, few), n_fs, [many, few])
    value_pieces, out_pieces = ring_gather(
        chained([value_b, with_scale(out_b, out_scale)], third_pieces, few), n_fs, [many, few]
    )

    gate_full, up_full = (jnp.concatenate(p, axis=0) for p in first_pieces)
    down_top, down_cols = without_scale(second_pieces[0])
    down_rest = jnp.concatenate(second_pieces[1], axis=1)
    down_full = lax.optimization_barrier(jnp.concatenate([down_top, down_rest], axis=0))
    query_full, key_full = (jnp.concatenate(p, axis=0) for p in third_pieces)
    value_full = jnp.concatenate(value_pieces, axis=0)
    out_full, out_cols = without_scale(out_pieces)

    def to_ring(x):
        blocks = [
            lax.dynamic_slice_in_dim(
                x, snake_index((place - k) % n_fs, n_fs) * width, width, axis=1
            )
            for k in range(n_fs)
        ]
        return jnp.concatenate(blocks, axis=1)

    def from_ring(x):
        blocks = [
            lax.dynamic_slice_in_dim(x, (place - snake(n_fs).index(o)) % n_fs * width, width, axis=1)
            for o in range(n_fs)
        ]
        return jnp.concatenate(blocks, axis=1)

    def over_tp(x, ordered):
        found = [x] + [shift(x, "tp", n_tp, k) for k in range(1, n_tp)]
        if not ordered:
            return jnp.concatenate(found, axis=0)
        twice = jnp.concatenate(found[::-1] * 2, axis=0)
        return lax.dynamic_slice_in_dim(twice, (n_tp - 1 - tp) * rows, n_tp * rows, axis=0)

    def gather_rows(normed, ordered=False):
        found = [normed] + [shift(normed, "rep", n_rep, k) for k in range(1, share)]
        return [over_tp(x, ordered) for x in found]

    def return_rows(parts, ordered=False):
        total = None
        for k in range(share - 1, -1, -1):

            def block(j):
                at = (tp - j) % n_tp * rows if ordered else j * rows
                return lax.dynamic_slice_in_dim(parts[k], at, rows, axis=0)

            mine = block(0)
            for j in range(1, n_tp):
                other = shift(block(j).astype(jnp.bfloat16), "tp", n_tp, n_tp - j)
                mine = mine + other.astype(jnp.float32)
            if k > 0:
                mine = shift(mine.astype(jnp.bfloat16), "rep", n_rep, n_rep - k).astype(jnp.float32)
            total = mine if total is None else total + mine
        return total

    def dot(a, b):
        return jnp.dot(a, b, preferred_element_type=jnp.float32)

    gate_col, up_col = part(gate_scale, 0), part(up_scale, 0)

    def feed_forward(stream, gain):
        parts = []
        for gathered in gather_rows(rms_scale(stream, gain).astype(jnp.bfloat16)):
            gate_value = dot(gathered, gate_full) * gate_col
            up_value = dot(gathered, up_full) * up_col
            hidden = (jax.nn.silu(gate_value) * up_value).astype(jnp.bfloat16)
            hidden = lax.optimization_barrier(hidden)
            parts.append(dot(hidden, down_full) * down_cols)
        return return_rows(parts)

    query_col, key_col, value_col = (part(s, 0) for s in (query_scale, key_scale, value_scale))
    decay = part(decay_rate, 0)
    gains = to_ring(norm_gains)

    stream = to_ring(tokens_in).astype(jnp.float32)
    stream = stream + 0.5 * feed_forward(stream, gains[0])
    parts = []
    for gathered in gather_rows(
        rms_scale(stream, gains[1]).astype(jnp.bfloat16), ordered=True
    ):
        query = (dot(gathered, query_full) * query_col).astype(jnp.bfloat16)
        key_rows = (dot(gathered, key_full) * key_col / math.sqrt(DK)).astype(jnp.bfloat16)
        value = (dot(gathered, value_full) * value_col).astype(jnp.bfloat16)
        mixed = [
            retain(
                query[:, h * DK : (h + 1) * DK],
                key_rows[:, h * DK : (h + 1) * DK],
                value[:, h * DV : (h + 1) * DV],
                decay[h],
                head_gain,
            )
            for h in range(heads)
        ]
        parts.append(dot(jnp.concatenate(mixed, axis=1), out_full) * out_cols)
    stream = stream + return_rows(parts, ordered=True)
    stream = stream + 0.5 * feed_forward(stream, gains[2])
    return from_ring(stream.astype(jnp.bfloat16))


MESH = pl.DeviceIdType.MESH
VMEM_LIMIT = 62 * 1024 * 1024


def fits(n_rep, n_fs, n_tp, tokens_in, norm_gains, gate_w, *rest):
    rows, features = tokens_in.shape
    width, units = gate_w.shape
    heads = rest[-1].shape[0]
    return (
        n_rep == 2
        and n_tp == 2
        and n_fs >= 6
        and n_fs % 2 == 0
        and n_fs <= 16
        and rows % 128 == 0
        and width % 256 == 0
        and features == n_fs * width
        and units % 512 == 0
        and heads % 2 == 0
    )


def layer_kernel(
    n,
    tokens_in,
    norm_gains_in,
    gate_w,
    gate_scale_in,
    up_w,
    up_scale_in,
    down_w,
    down_scale_in,
    query_w,
    query_scale_in,
    key_w,
    key_scale_in,
    value_w,
    value_scale_in,
    out_w,
    out_scale_in,
    head_gain_in,
    decay_rate,
    result,
    norm_gains,
    gate_scale,
    up_scale,
    down_scale,
    query_scale,
    key_scale,
    value_scale,
    out_scale,
    head_gain,
    staged_in,
    staged_gate,
    staged_up,
    staged_down,
    staged_query,
    staged_key,
    staged_value,
    staged_out,
    gate_away,
    up_away,
    down_away,
    head_away,
    out_away,
    cols_away,
    gate_full,
    up_full,
    down_full,
    head_full,
    out_full,
    cols_full,
    gathered,
    factors,
    stream,
    squares,
    summed,
    projected,
    hidden,
    mixed,
    own_part,
    far_part,
    tp_out,
    tp_in,
    rep_out,
    rep_in,
    local_sem,
    side_send,
    side_recv,
    line_send,
    line_recv,
    twin_send,
    twin_recv,
    part_send,
    part_recv,
    row_send,
    row_recv,
    block_send,
    block_recv,
):
    f32, bf16 = jnp.float32, jnp.bfloat16
    rows, features = tokens_in.shape
    width = gate_w.shape[0]
    units = hidden.shape[1]
    heads = head_full.shape[0]
    tile = 256

    twin, fs, tp = (lax.axis_index(axis) for axis in ("rep", "fs", "tp"))
    line = n // 2
    side, spot = lax.rem(fs, 2), lax.div(fs, 2)
    above, below = {"fs": fs + 2}, {"fs": fs - 2}
    side_peer, twin_peer, tp_peer = {"fs": fs + 1 - 2 * side}, {"rep": 1 - twin}, {"tp": 1 - tp}
    has_above, has_below = spot + 1 < line, spot > 0

    barrier = pltpu.get_barrier_semaphore()

    def greet(peer):
        pl.semaphore_signal(barrier, inc=1, device_id=peer, device_id_type=MESH)

    def meet():
        for peer in (side_peer, twin_peer, tp_peer):
            greet(peer)
        pl.when(has_above)(lambda: greet(above))
        pl.when(has_below)(lambda: greet(below))

    def columns_of(f):
        return pl.ds(pl.multiple_of(f * width, width), width)

    def halves(size):
        return [pl.ds(pl.multiple_of(i * size, 128), size) for i in (side, 1 - side)]

    local, copies_of = [], {}

    def fetch(name, src, dst):
        copy = pltpu.make_async_copy(src, dst, local_sem.at[len(local)])
        copy.start()
        copies_of.setdefault(name, []).append(copy)
        local.append(copy)

    def fetched(name):
        for copy in copies_of[name]:
            copy.wait()

    gate_halves = halves(units)
    fetch(("gate", 0), gate_w.at[:, gate_halves[0]], staged_gate.at[0])
    meet()
    fetch(("gate", 1), gate_w.at[:, gate_halves[1]], staged_gate.at[1])
    for i, cols in enumerate(halves(units)):
        fetch(("up", i), up_w.at[:, cols], staged_up.at[i])
    fetch("rows", tokens_in, staged_in)
    for src, dst in (
        (gate_scale_in, gate_scale),
        (up_scale_in, up_scale),
        (down_scale_in, down_scale),
        (query_scale_in, query_scale),
        (key_scale_in, key_scale),
        (value_scale_in, value_scale),
        (out_scale_in, out_scale),
        (head_gain_in, head_gain),
    ):
        fetch("small", src, dst.at[0])
    fetch("small", norm_gains_in, norm_gains)
    for i, cols in enumerate(halves(units)):
        fetch("down", down_w.at[cols, :], staged_down.at[i])
    for i, cols in enumerate(halves(heads * DK)):
        fetch("heads", query_w.at[:, cols], staged_query.at[i])
        fetch("heads", key_w.at[:, cols], staged_key.at[i])
    for i, cols in enumerate(halves(heads * DV)):
        fetch("heads", value_w.at[:, cols], staged_value.at[i])
        fetch("out", out_w.at[cols, :], staged_out.at[i])

    started = []
    half_units, half_width, half_out = units // 2, width // 2, heads * DV // 2

    def rows_of(f):
        return pl.ds(pl.multiple_of(f * width, width), width)

    def cut(ref, s, size):
        return ref.at[pl.ds(pl.multiple_of(s * size, size), size), :]

    def half_rows(f, i):
        return pl.ds(pl.multiple_of(f * width + i * half_width, half_width), half_width)

    kinds, head_kinds = [], []
    for i in range(2):
        kinds.append(
            (
                lambda f, i=i: gate_full.at[half_rows(f, i), :],
                gate_away.at[pl.ds(i * half_width, half_width), :],
                half_width // 2,
            )
        )
    kinds.append((lambda f: up_full.at[rows_of(f), :], up_away, half_width))
    kinds.append((lambda f: down_full.at[f], down_away, half_units))
    up_kind, down_kind = 2, 3
    for h in range(heads):
        head_kinds.append([len(kinds)])
        kinds.append(
            (lambda f, h=h: head_full.at[h, rows_of(f), :], head_away.at[h], half_width)
        )
    out_kind = len(kinds)
    kinds.append((lambda f: out_full.at[f], out_away, half_out))
    scales = len(kinds)
    kinds.append((lambda f: cols_full.at[f], cols_away, 8))
    rounds = [[0, 1, up_kind], [down_kind, scales], *head_kinds, [out_kind]]
    bank_of, last_bank = {}, 0
    for members in rounds:
        for kind in members:
            bank_of[kind] = last_bank
            last_bank = (last_bank + 1) % 3

    def piece(kind, f, s):
        if kind == scales:
            return kinds[kind][0](f).at[pl.ds(pl.multiple_of(s * 8, 8), 1), :]
        return cut(kinds[kind][0](f), s, kinds[kind][2])

    def remote(src, dst, send_sem, recv_sem, peer):
        return pltpu.make_async_remote_copy(
            src_ref=src,
            dst_ref=dst,
            send_sem=send_sem,
            recv_sem=recv_sem,
            device_id=peer,
            device_id_type=MESH,
        )

    def across(o):
        return spot * 2 + side + o * (1 - 2 * side)

    def side_slot(kind, i):
        return kind * 2 + i if kind <= up_kind else kind + 3

    def side_copy(kind, i, f):
        slot_of = side_slot(kind, i)
        sems = side_send.at[slot_of], side_recv.at[slot_of]
        if kind <= up_kind:
            s = twin if i == 0 else 1 - twin
            return remote(
                cut(kinds[kind][1], s, kinds[kind][2]), piece(kind, f, s), *sems, side_peer
            )
        return remote(kinds[kind][1], kinds[kind][0](f), *sems, side_peer)

    def side_start(kind, i=0):
        copy = side_copy(kind, i, fs)
        copy.start()
        started.append(copy)

    side_done = set()

    def side_need(kind, i):
        i = i if kind <= up_kind else 0
        if (kind, i) not in side_done:
            side_done.add((kind, i))
            side_copy(kind, i, across(1)).wait_recv()

    span_of = 2 * (line - 1)
    sending = {}

    def push(kind, group, index, f, where, recv, peer):
        bank = bank_of[kind]
        slot_of = (bank * 2 + group) * span_of + index
        copy = remote(piece(kind, f, twin), piece(kind, f, twin), line_send.at[slot_of], recv, peer)
        if slot_of in sending:
            sending.pop(slot_of)()
        guard = functools.partial(pl.when, where) if where is not None else None

        def begin():
            copy.start()

        def finish():
            copy.wait_send()

        if guard is None:
            begin()
            sending[slot_of] = finish
        else:
            guard()(begin)
            sending[slot_of] = lambda: guard()(finish)

    def line_slot(kind, away, o):
        return line_recv.at[kind * span_of + (away % line - 1) * 2 + o]

    def twin_slot(kind, away, o):
        return twin_recv.at[kind * span_of + (away - 1) * 2 + o]

    def send_own(kind, o):
        if o == 1:
            side_need(kind, 0)
        f = across(o)
        push(kind, 0, o, f, has_above, line_slot(kind, -1, o), above)
        push(kind, 1, o, f, has_below, line_slot(kind, 1, o), below)

    def places(d, o):
        for group, away in ((1, d), (0, -d)):
            from_spot = spot + away
            exists = from_spot >= 0 if away < 0 else from_spot < line
            yield group, away, exists, from_spot * 2 + side + o * (1 - 2 * side)

    def take_in(kind, d, o):
        for group, away, exists, f in places(d, o):

            def receive(kind=kind, away=away, f=f):
                remote(
                    piece(kind, f, twin),
                    piece(kind, f, twin),
                    line_send.at[0],
                    line_slot(kind, away, o),
                    above,
                ).wait_recv()

            pl.when(exists)(receive)
            hand_over(kind, away, o, f, exists)

    def move_on(kind, d, o):
        if d > line - 2:
            return
        for group, away, exists, f in places(d, o):
            further = -d - 1 if away < 0 else d + 1
            push(
                kind,
                group,
                2 * d + o,
                f,
                jnp.logical_and(exists, has_above if away < 0 else has_below),
                line_slot(kind, further, o),
                above if away < 0 else below,
            )

    def pass_along(kind, d, o):
        take_in(kind, d, o)
        move_on(kind, d, o)

    def hand_over(kind, away, o, f, exists):
        copy = remote(
            piece(kind, f, twin),
            piece(kind, f, twin),
            twin_send.at[kind],
            twin_slot(kind, away % line, o),
            twin_peer,
        )
        pl.when(exists)(lambda: copy.start())

    def handed_over():
        shards = pl.ds(0, line - 1)
        sent = [gate_full.at[pl.ds(0, (line - 1) * half_width), :]] * 2
        sent += [up_full.at[pl.ds(0, (line - 1) * width), :], down_full.at[shards]]
        sent += [head_full.at[h, pl.ds(0, (line - 1) * width), :] for h in range(heads)]
        sent += [out_full.at[shards], cols_full.at[0, pl.ds(0, span_of), :]]
        for kind, ref in enumerate(sent):
            remote(ref, ref, twin_send.at[kind], twin_recv.at[0], twin_peer).wait_send()

    def pick(table):
        total = 0
        for v in range(line):
            total = total + (spot == v).astype(jnp.int32) * table[v]
        return total

    near = []
    for v in range(line):
        near.append(sorted((u for u in range(line) if u != v), key=lambda u: (abs(u - v), -u)))
    sources = [across(0), across(1)]
    twin_index = [None, None]
    for r in range(line - 1):
        at = pick([near[v][r] for v in range(line)])
        away = pick([(near[v][r] - v) % line for v in range(line)])
        for o in range(2):
            sources.append(at * 2 + side + o * (1 - 2 * side))
            twin_index.append((away - 1) * 2 + o)

    def need_piece(kind, k):
        if k == 1:
            side_need(kind, 0)
            side_need(kind, 1)
        if k > 1:
            remote(
                piece(kind, sources[k], 1 - twin),
                piece(kind, sources[k], 1 - twin),
                line_send.at[0],
                twin_recv.at[kind * span_of + twin_index[k]],
                twin_peer,
            ).wait_recv()

    spots = [spot] + [lax.div(sources[2 * r], 2) for r in range(1, line)]
    queue = []
    later = []
    for members in rounds:
        for o in range(2):
            queue.append([functools.partial(send_own, m, o) for m in members])
        queue.extend(later)
        later = []
        for d in range(1, line):
            for o in range(2):
                unit = [functools.partial(pass_along, m, d, o) for m in members]
                (queue if d < line - 1 else later).append(unit)
    queue.extend(later)
    middle = 2 * (line - 2)

    def pump(count):
        for _ in range(count):
            for action in queue.pop(0):
                action()

    def send(src, dst, send_sem, recv_sem, peer):
        copy = remote(src, dst, send_sem, recv_sem, peer)
        copy.start()
        started.append(copy)
        return copy

    own_rows = rows_of(fs)
    fetched(("gate", 0))
    gate_full[own_rows, :] = staged_gate[0].astype(bf16)
    neighbours = has_above.astype(jnp.int32) + has_below.astype(jnp.int32)
    pl.semaphore_wait(barrier, 3 + neighbours)
    first, second, _ = (queue.pop(0) for _ in range(3))
    first[0]()
    first[1]()
    fetched(("gate", 1))
    gate_away[...] = staged_gate[1].astype(bf16)
    side_start(0)
    side_start(1)
    fetched(("up", 0))
    up_full[own_rows, :] = staged_up[0].astype(bf16)
    first[2]()
    fetched(("up", 1))
    up_away[...] = staged_up[1].astype(bf16)
    side_start(up_kind)
    fetched("rows")
    fetched("small")

    def norm_rows(source, which, target):
        gain = norm_gains[which : which + 1, :]

        def step(i, carry):
            block = pl.ds(pl.multiple_of(i * 16, 16), 16)
            x = source[block, :].astype(f32)
            mean = jnp.mean(x * x, axis=-1, keepdims=True)
            target[block, :] = (x * lax.rsqrt(mean + EPSILON) * gain).astype(bf16)
            return carry

        lax.fori_loop(0, rows // 16, step, 0)

    def slot(j, cols=slice(None)):
        return (pl.ds(j * rows, rows), cols)

    def share_rows(stage):
        part = gathered.at[stage]
        base = 3 * stage
        send(part.at[slot(0)], part.at[slot(1)], row_send.at[base], row_recv.at[base], tp_peer)
        send(
            part.at[slot(0)],
            part.at[slot(2)],
            row_send.at[base + 1],
            row_recv.at[base + 1],
            side_peer,
        )

    def wait_rows(stage, i, j):
        part = gathered.at[stage]
        pltpu.make_async_remote_copy(
            src_ref=part.at[slot(0)],
            dst_ref=part.at[slot(j)],
            send_sem=row_send.at[3 * stage + i],
            recv_sem=row_recv.at[3 * stage + i],
            device_id=tp_peer,
            device_id_type=MESH,
        ).wait_recv()

    def relay_rows(stage):
        wait_rows(stage, 1, 2)
        part = gathered.at[stage]
        send(
            part.at[slot(2)],
            part.at[slot(3)],
            row_send.at[3 * stage + 2],
            row_recv.at[3 * stage + 2],
            tp_peer,
        )

    norm_rows(staged_in, 0, gathered.at[0])
    stream[...] = staged_in[...].astype(f32)
    fetched("down")
    down_full[fs] = staged_down[0].astype(bf16)
    down_away[...] = staged_down[1].astype(bf16)
    cols_full[fs, 0:1, :] = down_scale[...]
    cols_full[fs, 8:9, :] = out_scale[...]
    cols_away[0:1, :] = down_scale[...]
    cols_away[8:9, :] = out_scale[...]
    side_start(0, 1)
    side_start(1, 1)
    side_start(up_kind, 1)
    side_start(down_kind)
    side_start(scales)
    take_in(0, 1, 0)
    take_in(1, 1, 0)
    second[0]()
    second[1]()
    take_in(up_kind, 1, 0)
    second[2]()
    move_on(0, 1, 0)
    move_on(1, 1, 0)
    move_on(up_kind, 1, 0)
    share_rows(0)
    fetched("heads")
    for h in range(heads):
        keys, vals = slice(h * DK, (h + 1) * DK), slice(h * DV, (h + 1) * DV)
        for i in range(2):
            made = jnp.concatenate(
                [staged_query[i, :, keys], staged_key[i, :, keys], staged_value[i, :, vals]], axis=1
            ).astype(bf16)
            if i == 0:
                head_full[h, own_rows, :] = made
            else:
                head_away[h] = made
        for kind in head_kinds[h]:
            side_start(kind)
    fetched("out")
    out_full[fs] = staged_out[0].astype(bf16)
    out_away[...] = staged_out[1].astype(bf16)
    side_start(out_kind)

    pump(middle + 2)
    relay_rows(0)
    pump(middle + 1)
    wait_rows(0, 0, 1)
    wait_rows(0, 2, 3)

    def dot(a, b):
        return jnp.dot(a, b, preferred_element_type=f32)

    def expand(factor, part, first=0, count=4 * rows):
        for c in range(units // tile):
            cols = slice(c * tile, (c + 1) * tile)
            span = pl.ds(pl.multiple_of(side * units + c * tile, 128), tile)
            rows_in, lhs = part
            block = slice(first, first + count)
            gate = dot(lhs[block], gate_full[rows_in, cols])
            up = dot(lhs[block], up_full[rows_in, cols])
            if factor is not None:
                gate = (gate + summed[0, block, cols]) * factor[block]
                up = (up + summed[1, block, cols]) * factor[block]
            gate, up = gate * gate_scale[:, span], up * up_scale[:, span]
            hidden[block, cols] = (gate / (1.0 + jnp.exp(-gate)) * up).astype(bf16)

    def part_copy(stage, k, way, landing):
        store_out, store_in = (rep_out, rep_in) if way == 2 else (tp_out, tp_in)
        return remote(
            store_out.at[stage, k] if way == 2 else store_out.at[stage, k, way],
            store_in.at[stage, landing] if way == 2 else store_in.at[stage, landing, way],
            part_send.at[stage * 2 + way // 2],
            part_recv.at[landing * 3 + way],
            side_peer if way == 2 else tp_peer,
        )

    def part_start(stage, k, way):
        part_copy(stage, k, way, k ^ 1 if way == 2 else k).start()

    def part_wait(stage, k, way):
        part_copy(stage, k, way, k).wait_recv()

    def parts_sent(stage):
        for over_side, (src, dst) in enumerate(((tp_out, tp_in), (rep_out, rep_in))):
            remote(
                src.at[stage],
                dst.at[stage],
                part_send.at[stage * 2 + over_side],
                part_recv.at[0],
                side_peer,
            ).wait_send()

    def contract(stage, lhs, weight, row, fresh, order, finish, relay=None, extra=None, near=None):
        def ready(k):
            if fresh is not None:
                need_piece(fresh, k)
                if fresh == down_kind:
                    need_piece(scales, k)

        def product(k, block):
            f = sources[k]
            return dot(lhs[block, :], weight[f]) * cols_full[f, 8 * row : 8 * row + 1, :]

        def keep(k, way, part):
            (far_part if way else own_part)[k] = part[:rows]
            tp_out[stage, k, way] = part[rows:].astype(bf16)
            part_start(stage, k, way)

        def multiply(k):
            ready(k)
            part = product(k, slice(None))
            keep(k, 1, part[2 * rows :])
            keep(k, 0, part[: 2 * rows])

        def multiply_far(k):
            ready(k)
            keep(k, 1, product(k, slice(2 * rows, 4 * rows)))

        def multiply_near(k):
            keep(k, 0, product(k, slice(0, 2 * rows)))

        def pass_on(k):
            part_wait(stage, k, 1)
            rep_out[stage, k] = (far_part[k] + tp_in[stage, k, 1].astype(f32)).astype(bf16)
            part_start(stage, k, 2)

        def collect(k):
            part_wait(stage, k, 0)
            part_wait(stage, k, 2)
            total = own_part[k] + tp_in[stage, k, 0].astype(f32) + rep_in[stage, k].astype(f32)
            finish(k, sources[k], total)

        actions = {"m": multiply, "p": pass_on, "c": collect, "r": relay, "u": pump, "x": extra}
        actions.update({"f": multiply_far, "n": multiply_near, "near": lambda _: near()})
        for action, k in order:
            actions[action](k)

    def last_order():
        order = []
        for k in range(n):
            order.append(("f", k))
            if k > 0:
                order.append(("p", k - 1))
        order += [("p", n - 1), ("near", 0)]
        return order + [("n", k) for k in range(n)] + [("c", k) for k in range(n)]

    def first_order():
        order = [("m", 0), ("m", 1), ("p", 0), ("p", 1), ("u", 4)]
        for k in range(2, n):
            if k == 2 * (line - 1):
                order.append(("u", 2))
            order.append(("m", k))
            if k > 2:
                order.append(("p", k - 1))
        order.append(("p", n - 1))
        order += [("c", k) for k in range(n)]
        order.insert(-2, ("u", 1))
        return order

    def tail_order():
        order, waiting, relayed = [], [], []

        def advance(r):
            ks = (2 * r, 2 * r + 1)
            order.extend([("m", k) for k in ks] + [("p", k) for k in ks])
            waiting.append(ks)

        def take():
            if waiting:
                ks = waiting.pop(0)
                order.extend(("c", k) for k in ks)
                relayed.append(ks)

        order.extend([("f", 0), ("f", 1), ("p", 0), ("p", 1), ("u", 2)])
        order.extend([("f", 2), ("near", 0), ("n", 0), ("n", 1), ("n", 2)])
        order.extend([("p", 2), ("f", 3), ("n", 3), ("p", 3), ("c", 0), ("c", 1)])
        waiting.append((2, 3))
        relayed.append((0, 1))
        for r in range(3, line):
            order.append(("u", 2))
            advance(r - 1)
            take()
        advance(line - 1)
        for ks in relayed[:1]:
            order.extend(("r", k) for k in relayed.pop(0))
        while waiting:
            take()
            order.extend(("r", k) for k in relayed.pop(0))
        order.extend(("r", k) for ks in relayed for k in ks)
        for r in range(line - 2):
            order.insert(order.index(("r", 2 * r + 3)) + 1, ("x", r))
        return order

    def need_all(kind):
        for k in range(1, n):
            need_piece(kind, k)

    need_all(0)
    need_all(1)
    need_all(up_kind)
    expand(None, (slice(None), gathered[0]))

    def add_half(k, f, total):
        cols = columns_of(f)
        stream[:, cols] = stream[:, cols] + 0.5 * total

    contract(0, hidden, down_full, 0, down_kind, first_order(), add_half)

    norm_rows(stream, 1, gathered.at[1])
    share_rows(1)
    pump(middle + 1)
    relay_rows(1)
    pump(2)

    seq_len = 2 * rows
    row = lax.rem(
        lax.broadcasted_iota(jnp.int32, (seq_len, seq_len), 0) + tp * rows, seq_len
    )
    col = lax.rem(
        lax.broadcasted_iota(jnp.int32, (seq_len, seq_len), 1) + tp * rows, seq_len
    )

    def retain(h, parts=(0, 1), again=False):
        start, stop = parts[0] * seq_len, (parts[-1] + 1) * seq_len
        places = [
            (query_scale, 0, DK, 1.0),
            (key_scale, DK, DK, 1.0 / math.sqrt(DK)),
            (value_scale, 2 * DK, DV, 1.0),
        ]
        for r in range(line - 1 if again else 0, line):
            for k in (2 * r, 2 * r + 1):
                for kind in head_kinds[h] if not again else []:
                    need_piece(kind, k)
            rows_in = pl.ds(pl.multiple_of(spots[r] * 2 * width, 2 * width), 2 * width)
            block = slice(start, stop) if r == line - 1 else slice(0, 2 * seq_len)
            lhs, made = gathered[1, block, rows_in], []
            for scale, first, size, factor in places:
                cols = slice(first, first + size)
                product = dot(lhs, head_full[h, rows_in, cols])
                if r > 0:
                    product = product + projected[block, cols]
                if r < line - 1:
                    projected[block, cols] = product
                else:
                    span = pl.ds(pl.multiple_of((side * heads + h) * size, 128), size)
                    made.append((product * (scale[:, span] * factor)).astype(bf16))
        query, keys, values = made
        decay = decay_rate[side * heads + h]
        distance = jnp.abs(row - col).astype(f32)
        weight = jnp.where(
            lax.div(col, BLOCK) <= lax.div(row, BLOCK), jnp.exp(-decay * distance), 0.0
        )
        for s in parts:
            span = slice(s * seq_len - start, (s + 1) * seq_len - start)
            scores = lax.dot_general(
                query[span], keys[span], (((1,), (1,)), ((), ())), preferred_element_type=f32
            )
            scores = (scores * weight).astype(bf16)
            retained = dot(scores, values[span])
            centred = retained - jnp.mean(retained, axis=-1, keepdims=True)
            spread = jnp.mean(centred * centred, axis=-1, keepdims=True)
            mixed[s * seq_len : (s + 1) * seq_len, h * DV : (h + 1) * DV] = (
                centred * lax.rsqrt(spread + EPSILON) * head_gain[...]
            ).astype(bf16)

    for h in range(heads):
        if h == 0:
            wait_rows(1, 0, 1)
            wait_rows(1, 2, 3)
        if h < heads - 1:
            retain(h)
            pump(1)
        else:
            retain(h, (1,))
        if h < heads - 1:
            pump(middle - 3 + 6)

    last = gathered.at[2]

    def block_copy(k, i, start):
        cols = columns_of(sources[k])
        a, b, peer = ((0, 1, tp_peer), (0, 2, side_peer), (2, 3, tp_peer))[i]
        return pltpu.make_async_remote_copy(
            src_ref=last.at[slot(a, cols)],
            dst_ref=last.at[slot(b, cols)],
            send_sem=block_send.at[i],
            recv_sem=block_recv.at[3 * (k ^ 1 if i == 1 and start else k) + i],
            device_id=peer,
            device_id_type=MESH,
        )

    def factor_copy(i):
        a, b, peer = ((0, 1, tp_peer), (0, 2, side_peer), (2, 3, tp_peer))[i]
        return pltpu.make_async_remote_copy(
            src_ref=factors.at[a],
            dst_ref=factors.at[b],
            send_sem=block_send.at[3 + i],
            recv_sem=block_recv.at[3 * n + i],
            device_id=peer,
            device_id_type=MESH,
        )

    squares[...] = jnp.zeros_like(squares)

    def add_mix(k, f, total):
        cols = columns_of(f)
        second = stream[:, cols] + total
        stream[:, cols] = second
        last[slot(0, cols)] = (second * norm_gains[2:3, cols]).astype(bf16)
        square = second * second
        added = squares[...]
        for i in range(width // 128):
            added = added + square[:, i * 128 : (i + 1) * 128]
        squares[...] = added
        for i in (0, 1):
            block_copy(k, i, True).start()
        if k == n - 1:
            mean = jnp.sum(added, axis=-1, keepdims=True) / features
            wide = jnp.broadcast_to(lax.rsqrt(mean + EPSILON), (rows, rows))
            factors[0] = wide.T[:8, :]
            for i in (0, 1):
                copy = factor_copy(i)
                copy.start()
                started.append(copy)

    def relay_block(k):
        block_copy(k, 1, False).wait_recv()
        block_copy(k, 2, True).start()
        if k == n - 1:
            factor_copy(1).wait_recv()
            copy = factor_copy(2)
            copy.start()
            started.append(copy)


    def arrived_block(r):
        for k in (2 * r, 2 * r + 1):
            block_copy(k, 0, False).wait_recv()
            block_copy(k, 2, False).wait_recv()
        return pl.ds(pl.multiple_of(spots[r] * 2 * width, 2 * width), 2 * width)

    def take_sum(r):
        rows_in = arrived_block(r)
        lhs = last[:, rows_in]
        for c in range(units // tile):
            cols = slice(c * tile, (c + 1) * tile)
            for i, weight in enumerate((gate_full, up_full)):
                part = dot(lhs, weight[rows_in, cols])
                summed[i, :, cols] = part if r == 0 else summed[i, :, cols] + part

    contract(1, mixed, out_full, 1, out_kind, tail_order(), add_mix, relay_block, take_sum, lambda: retain(heads - 1, (0,), True))
    take_sum(line - 2)
    rows_in = arrived_block(line - 1)
    factor_copy(0).wait_recv()
    factor_copy(2).wait_recv()
    factor = jnp.concatenate(
        [jnp.broadcast_to(factors[j, 0:1, :], (rows, rows)).T[:, 0:1] for j in range(4)], axis=0
    )
    late = (rows_in, last[:, rows_in])
    expand(factor, late, 2 * rows, 2 * rows)

    def write(k, f, total):
        cols = columns_of(f)
        result[:, cols] = (stream[:, cols] + 0.5 * total).astype(bf16)

    contract(2, hidden, down_full, 0, None, last_order(), write, near=lambda: expand(factor, late, 0, 2 * rows))
    assert not queue
    for stage in range(3):
        parts_sent(stage)
    for i, a in enumerate((0, 0, 2)):
        remote(
            last.at[slot(a)], last.at[slot(a)], block_send.at[i], block_recv.at[0], tp_peer
        ).wait_send()
    handed_over()
    for finish in sending.values():
        finish()
    for copy in started:
        copy.wait_send()


def fused(
    n_rep,
    n_fs,
    n_tp,
    tokens_in,
    norm_gains,
    gate_w,
    gate_scale,
    up_w,
    up_scale,
    down_w,
    down_scale,
    query_w,
    query_scale,
    key_w,
    key_scale,
    value_w,
    value_scale,
    out_w,
    out_scale,
    head_gain,
    decay_rate,
):
    f32, bf16 = jnp.float32, jnp.bfloat16
    n = n_fs
    rows, features = tokens_in.shape
    width, units = gate_w.shape[0], gate_w.shape[1] // 2
    heads = decay_rate.shape[0] // 2
    kinds = heads + 6
    span_of = n - 2
    any_space = pl.BlockSpec(memory_space=pl.ANY)
    vmem = pl.BlockSpec(memory_space=pltpu.VMEM)
    smem = pl.BlockSpec(memory_space=pltpu.SMEM)
    dma = pltpu.SemaphoreType.DMA

    return pl.pallas_call(
        functools.partial(layer_kernel, n),
        out_shape=pltpu.VMEM((rows, features), bf16),
        in_specs=[any_space] * 17 + [smem],
        out_specs=vmem,
        scratch_shapes=[
            pltpu.VMEM(norm_gains.shape, f32),
        ]
        + [
            pltpu.VMEM((1, x.shape[0]), f32)
            for x in (
                gate_scale,
                up_scale,
                down_scale,
                query_scale,
                key_scale,
                value_scale,
                out_scale,
                head_gain,
            )
        ]
        + [
            pltpu.VMEM((rows, features), bf16),
            pltpu.VMEM((2, width, units), f32),
            pltpu.VMEM((2, width, units), f32),
            pltpu.VMEM((2, units, width), f32),
            pltpu.VMEM((2, width, heads * DK), f32),
            pltpu.VMEM((2, width, heads * DK), f32),
            pltpu.VMEM((2, width, heads * DV), f32),
            pltpu.VMEM((2, heads * DV, width), f32),
            pltpu.VMEM((width, units), bf16),
            pltpu.VMEM((width, units), bf16),
            pltpu.VMEM((units, width), bf16),
            pltpu.VMEM((heads, width, 2 * DK + DV), bf16),
            pltpu.VMEM((heads * DV, width), bf16),
            pltpu.VMEM((16, width), f32),
            pltpu.VMEM((features, units), bf16),
            pltpu.VMEM((features, units), bf16),
            pltpu.VMEM((n, units, width), bf16),
            pltpu.VMEM((heads, features, 2 * DK + DV), bf16),
            pltpu.VMEM((n, heads * DV, width), bf16),
            pltpu.VMEM((n, 16, width), f32),
            pltpu.VMEM((3, 4 * rows, features), bf16),
            pltpu.VMEM((4, 8, rows), f32),
            pltpu.VMEM((rows, features), f32),
            pltpu.VMEM((rows, 128), f32),
            pltpu.VMEM((2, 4 * rows, units), f32),
            pltpu.VMEM((4 * rows, 2 * DK + DV), f32),
            pltpu.VMEM((4 * rows, units), bf16),
            pltpu.VMEM((4 * rows, heads * DV), bf16),
            pltpu.VMEM((n, rows, width), f32),
            pltpu.VMEM((n, rows, width), f32),
            pltpu.VMEM((3, n, 2, rows, width), bf16),
            pltpu.VMEM((3, n, 2, rows, width), bf16),
            pltpu.VMEM((3, n, rows, width), bf16),
            pltpu.VMEM((3, n, rows, width), bf16),
            dma((24,)),
            dma((kinds + 3,)),
            dma((kinds + 3,)),
            dma((6 * span_of,)),
            dma((kinds * span_of,)),
            dma((kinds,)),
            dma((kinds * span_of,)),
            dma((6,)),
            dma((3 * n,)),
            dma((6,)),
            dma((6,)),
            dma((6,)),
            dma((3 * n + 3,)),
        ],
        compiler_params=pltpu.CompilerParams(
            collective_id=0, has_side_effects=True, vmem_limit_bytes=VMEM_LIMIT
        ),
        name="layer",
    )(
        tokens_in,
        norm_gains,
        gate_w,
        gate_scale,
        up_w,
        up_scale,
        down_w,
        down_scale,
        query_w,
        query_scale,
        key_w,
        key_scale,
        value_w,
        value_scale,
        out_w,
        out_scale,
        head_gain,
        decay_rate,
    )


def solution(mesh):
    sizes = [mesh.shape[axis] for axis in ("rep", "fs", "tp")]
    placed = (
        P(("rep", "fs", "tp"), None),
        P(),
        P("fs", "tp"),
        P("tp"),
        P("fs", "tp"),
        P("tp"),
        P("tp", "fs"),
        P("fs"),
        P("fs", "tp"),
        P("tp"),
        P("fs", "tp"),
        P("tp"),
        P("fs", "tp"),
        P("tp"),
        P("tp", "fs"),
        P("fs"),
        P(),
        P("tp"),
    )
    return jax.shard_map(
        lambda *args: (fused if fits(*sizes, *args) else on_device)(*sizes, *args),
        mesh=mesh,
        in_specs=placed,
        out_specs=P(("rep", "fs", "tp"), None),
        check_vma=False,
    )
```

```python
import functools
import math

import jax
import jax.numpy as jnp
from jax import lax
from jax.experimental import pallas as pl
from jax.experimental.pallas import tpu as pltpu
from jax.sharding import PartitionSpec as P

DK = 256
DV = 256
BLOCK = 64

EPSILON = 1e-05


def rms_scale(stream, gain):
    return stream * lax.rsqrt(jnp.mean(stream * stream, axis=-1, keepdims=True) + EPSILON) * gain


def snake(n):
    return [i for i in range(0, n, 2)] + [i for i in range(n - 1, 0, -1) if i % 2 == 1]


def snake_place(index, n):
    return jnp.where(index % 2 == 0, index // 2, n - 1 - index // 2)


def snake_index(place, n):
    half = (n + 1) // 2
    return jnp.where(place < half, 2 * place, 2 * (n - 1 - place) + 1)


def shift(x, axis, n, by):
    return lax.ppermute(x, axis, [(i, (i + by) % n) for i in range(n)])


def ring_gather(shards, n, forward_steps):
    order = snake(n)
    ahead = [(order[i], order[(i + 1) % n]) for i in range(n)]
    behind = [(b, a) for a, b in ahead]
    found = []
    for x, steps in zip(shards, forward_steps):
        forward, back = [x], [x]
        found.append((forward, back))
    for step in range(n):
        for (forward, back), steps in zip(found, forward_steps):
            if step < steps:
                forward.append(lax.ppermute(forward[-1], "fs", ahead))
            if step < n - 1 - steps:
                back.append(lax.ppermute(back[-1], "fs", behind))
    return [forward + back[:0:-1] for forward, back in found]


def chained(shards, before, hops):
    if not before:
        return shards
    last = []
    n = len(before[0])
    for pieces in before:
        last.extend([pieces[hops], pieces[n - hops]])
    return lax.optimization_barrier((tuple(shards), tuple(last)))[0]


def with_scale(weight, scale):
    high = lax.reduce_precision(scale, 8, 7)
    middle = lax.reduce_precision(scale - high, 8, 7)
    rows = jnp.stack([high, middle, scale - high - middle]).astype(jnp.bfloat16)
    return jnp.concatenate([weight, jnp.pad(rows, ((0, 13), (0, 0)))], axis=0)


def without_scale(pieces):
    size = pieces[0].shape[0] - 16
    weight = jnp.concatenate([p[:size] for p in pieces], axis=1)
    rows = jnp.concatenate([p[size:] for p in pieces], axis=1)[:3].astype(jnp.float32)
    return weight, rows[0] + rows[1] + rows[2]


def retain(query, key_rows, value, decay, head_gain):
    seq_len = query.shape[0]
    row = lax.broadcasted_iota(jnp.int32, (seq_len, seq_len), 0)
    col = lax.broadcasted_iota(jnp.int32, (seq_len, seq_len), 1)
    distance = jnp.abs(row - col).astype(jnp.float32)
    weight = jnp.where(col // BLOCK <= row // BLOCK, jnp.exp(-decay * distance), 0.0)
    scores = lax.dot_general(
        query, key_rows, (((1,), (1,)), ((), ())), preferred_element_type=jnp.float32
    )
    scores = (scores * weight).astype(jnp.bfloat16)
    retained = jnp.dot(scores, value, preferred_element_type=jnp.float32)
    centred = retained - jnp.mean(retained, axis=-1, keepdims=True)
    normed = (
        centred
        * lax.rsqrt(jnp.mean(centred * centred, axis=-1, keepdims=True) + EPSILON)
        * head_gain
    )
    return normed.astype(jnp.bfloat16)


def on_device(
    n_rep,
    n_fs,
    n_tp,
    tokens_in,
    norm_gains,
    gate_w,
    gate_scale,
    up_w,
    up_scale,
    down_w,
    down_scale,
    query_w,
    query_scale,
    key_w,
    key_scale,
    value_w,
    value_scale,
    out_w,
    out_scale,
    head_gain,
    decay_rate,
):
    rows = tokens_in.shape[0]
    width = gate_w.shape[0]
    heads = decay_rate.shape[0]
    units = gate_w.shape[1]
    share = n_rep if heads % n_rep == 0 and units % (n_rep * 128) == 0 else 1
    heads //= share
    units //= share
    rep = lax.axis_index("rep") if share > 1 else 0
    tp = lax.axis_index("tp")
    place = snake_place(lax.axis_index("fs"), n_fs)

    def part(x, axis):
        size = x.shape[axis] // share
        return lax.dynamic_slice_in_dim(x, rep * size, size, axis)

    gate_b, up_b, query_b, key_b, value_b = (
        part(w, 1).astype(jnp.bfloat16) for w in (gate_w, up_w, query_w, key_w, value_w)
    )
    down_b, out_b = (part(w, 0).astype(jnp.bfloat16) for w in (down_w, out_w))

    few, many = (n_fs - 1) // 2, n_fs // 2
    first_pieces = ring_gather([gate_b, up_b], n_fs, [many, few])
    half = down_b.shape[0] // 2
    second_pieces = ring_gather(
        chained([with_scale(down_b[:half], down_scale), down_b[half:]], first_pieces, max(1, n_fs // 4)),
        n_fs,
        [many, few],
    )
    third_pieces = ring_gather(chained([query_b, key_b], second_pieces, few), n_fs, [many, few])
    value_pieces, out_pieces = ring_gather(
        chained([value_b, with_scale(out_b, out_scale)], third_pieces, few), n_fs, [many, few]
    )

    gate_full, up_full = (jnp.concatenate(p, axis=0) for p in first_pieces)
    down_top, down_cols = without_scale(second_pieces[0])
    down_rest = jnp.concatenate(second_pieces[1], axis=1)
    down_full = lax.optimization_barrier(jnp.concatenate([down_top, down_rest], axis=0))
    query_full, key_full = (jnp.concatenate(p, axis=0) for p in third_pieces)
    value_full = jnp.concatenate(value_pieces, axis=0)
    out_full, out_cols = without_scale(out_pieces)

    def to_ring(x):
        blocks = [
            lax.dynamic_slice_in_dim(
                x, snake_index((place - k) % n_fs, n_fs) * width, width, axis=1
            )
            for k in range(n_fs)
        ]
        return jnp.concatenate(blocks, axis=1)

    def from_ring(x):
        blocks = [
            lax.dynamic_slice_in_dim(x, (place - snake(n_fs).index(o)) % n_fs * width, width, axis=1)
            for o in range(n_fs)
        ]
        return jnp.concatenate(blocks, axis=1)

    def over_tp(x, ordered):
        found = [x] + [shift(x, "tp", n_tp, k) for k in range(1, n_tp)]
        if not ordered:
            return jnp.concatenate(found, axis=0)
        twice = jnp.concatenate(found[::-1] * 2, axis=0)
        return lax.dynamic_slice_in_dim(twice, (n_tp - 1 - tp) * rows, n_tp * rows, axis=0)

    def gather_rows(normed, ordered=False):
        found = [normed] + [shift(normed, "rep", n_rep, k) for k in range(1, share)]
        return [over_tp(x, ordered) for x in found]

    def return_rows(parts, ordered=False):
        total = None
        for k in range(share - 1, -1, -1):

            def block(j):
                at = (tp - j) % n_tp * rows if ordered else j * rows
                return lax.dynamic_slice_in_dim(parts[k], at, rows, axis=0)

            mine = block(0)
            for j in range(1, n_tp):
                other = shift(block(j).astype(jnp.bfloat16), "tp", n_tp, n_tp - j)
                mine = mine + other.astype(jnp.float32)
            if k > 0:
                mine = shift(mine.astype(jnp.bfloat16), "rep", n_rep, n_rep - k).astype(jnp.float32)
            total = mine if total is None else total + mine
        return total

    def dot(a, b):
        return jnp.dot(a, b, preferred_element_type=jnp.float32)

    gate_col, up_col = part(gate_scale, 0), part(up_scale, 0)

    def feed_forward(stream, gain):
        parts = []
        for gathered in gather_rows(rms_scale(stream, gain).astype(jnp.bfloat16)):
            gate_value = dot(gathered, gate_full) * gate_col
            up_value = dot(gathered, up_full) * up_col
            hidden = (jax.nn.silu(gate_value) * up_value).astype(jnp.bfloat16)
            hidden = lax.optimization_barrier(hidden)
            parts.append(dot(hidden, down_full) * down_cols)
        return return_rows(parts)

    query_col, key_col, value_col = (part(s, 0) for s in (query_scale, key_scale, value_scale))
    decay = part(decay_rate, 0)
    gains = to_ring(norm_gains)

    stream = to_ring(tokens_in).astype(jnp.float32)
    stream = stream + 0.5 * feed_forward(stream, gains[0])
    parts = []
    for gathered in gather_rows(
        rms_scale(stream, gains[1]).astype(jnp.bfloat16), ordered=True
    ):
        query = (dot(gathered, query_full) * query_col).astype(jnp.bfloat16)
        key_rows = (dot(gathered, key_full) * key_col / math.sqrt(DK)).astype(jnp.bfloat16)
        value = (dot(gathered, value_full) * value_col).astype(jnp.bfloat16)
        mixed = [
            retain(
                query[:, h * DK : (h + 1) * DK],
                key_rows[:, h * DK : (h + 1) * DK],
                value[:, h * DV : (h + 1) * DV],
                decay[h],
                head_gain,
            )
            for h in range(heads)
        ]
        parts.append(dot(jnp.concatenate(mixed, axis=1), out_full) * out_cols)
    stream = stream + return_rows(parts, ordered=True)
    stream = stream + 0.5 * feed_forward(stream, gains[2])
    return from_ring(stream.astype(jnp.bfloat16))


MESH = pl.DeviceIdType.MESH
VMEM_LIMIT = 62 * 1024 * 1024


def fits(n_rep, n_fs, n_tp, tokens_in, norm_gains, gate_w, *rest):
    rows, features = tokens_in.shape
    width, units = gate_w.shape
    heads = rest[-1].shape[0]
    return (
        n_rep == 2
        and n_tp == 2
        and n_fs >= 6
        and n_fs % 2 == 0
        and n_fs <= 16
        and rows % 128 == 0
        and width % 256 == 0
        and features == n_fs * width
        and units % 512 == 0
        and heads % 2 == 0
    )


def layer_kernel(
    n,
    tokens_in,
    norm_gains_in,
    gate_w,
    gate_scale_in,
    up_w,
    up_scale_in,
    down_w,
    down_scale_in,
    query_w,
    query_scale_in,
    key_w,
    key_scale_in,
    value_w,
    value_scale_in,
    out_w,
    out_scale_in,
    head_gain_in,
    decay_rate,
    result,
    norm_gains,
    gate_scale,
    up_scale,
    down_scale,
    query_scale,
    key_scale,
    value_scale,
    out_scale,
    head_gain,
    staged_in,
    staged_gate,
    staged_up,
    staged_down,
    staged_query,
    staged_key,
    staged_value,
    staged_out,
    gate_away,
    up_away,
    down_away,
    head_away,
    out_away,
    cols_away,
    gate_full,
    up_full,
    down_full,
    head_full,
    out_full,
    cols_full,
    gathered,
    factors,
    stream,
    squares,
    summed,
    projected,
    hidden,
    mixed,
    own_part,
    far_part,
    tp_out,
    tp_in,
    rep_out,
    rep_in,
    local_sem,
    side_send,
    side_recv,
    line_send,
    line_recv,
    twin_send,
    twin_recv,
    part_send,
    part_recv,
    row_send,
    row_recv,
    block_send,
    block_recv,
):
    f32, bf16 = jnp.float32, jnp.bfloat16
    rows, features = tokens_in.shape
    width = gate_w.shape[0]
    units = hidden.shape[1]
    heads = head_full.shape[0]
    tile = 256

    twin, fs, tp = (lax.axis_index(axis) for axis in ("rep", "fs", "tp"))
    line = n // 2
    side, spot = lax.rem(fs, 2), lax.div(fs, 2)
    above, below = {"fs": fs + 2}, {"fs": fs - 2}
    side_peer, twin_peer, tp_peer = {"fs": fs + 1 - 2 * side}, {"rep": 1 - twin}, {"tp": 1 - tp}
    has_above, has_below = spot + 1 < line, spot > 0

    barrier = pltpu.get_barrier_semaphore()

    def greet(peer):
        pl.semaphore_signal(barrier, inc=1, device_id=peer, device_id_type=MESH)

    def meet():
        for peer in (side_peer, twin_peer, tp_peer):
            greet(peer)
        pl.when(has_above)(lambda: greet(above))
        pl.when(has_below)(lambda: greet(below))

    def columns_of(f):
        return pl.ds(pl.multiple_of(f * width, width), width)

    def halves(size):
        return [pl.ds(pl.multiple_of(i * size, 128), size) for i in (side, 1 - side)]

    local, copies_of = [], {}

    def fetch(name, src, dst):
        copy = pltpu.make_async_copy(src, dst, local_sem.at[len(local)])
        copy.start()
        copies_of.setdefault(name, []).append(copy)
        local.append(copy)

    def fetched(name):
        for copy in copies_of[name]:
            copy.wait()

    gate_halves = halves(units)
    fetch(("gate", 0), gate_w.at[:, gate_halves[0]], staged_gate.at[0])
    meet()
    fetch(("gate", 1), gate_w.at[:, gate_halves[1]], staged_gate.at[1])
    for i, cols in enumerate(halves(units)):
        fetch(("up", i), up_w.at[:, cols], staged_up.at[i])
    fetch("rows", tokens_in, staged_in)
    for src, dst in (
        (gate_scale_in, gate_scale),
        (up_scale_in, up_scale),
        (down_scale_in, down_scale),
        (query_scale_in, query_scale),
        (key_scale_in, key_scale),
        (value_scale_in, value_scale),
        (out_scale_in, out_scale),
        (head_gain_in, head_gain),
    ):
        fetch("small", src, dst.at[0])
    fetch("small", norm_gains_in, norm_gains)
    for i, cols in enumerate(halves(units)):
        fetch("down", down_w.at[cols, :], staged_down.at[i])
    for i, cols in enumerate(halves(heads * DK)):
        fetch("heads", query_w.at[:, cols], staged_query.at[i])
        fetch("heads", key_w.at[:, cols], staged_key.at[i])
    for i, cols in enumerate(halves(heads * DV)):
        fetch("heads", value_w.at[:, cols], staged_value.at[i])
        fetch("out", out_w.at[cols, :], staged_out.at[i])

    started = []
    half_units, half_width, half_out = units // 2, width // 2, heads * DV // 2

    def rows_of(f):
        return pl.ds(pl.multiple_of(f * width, width), width)

    def cut(ref, s, size):
        return ref.at[pl.ds(pl.multiple_of(s * size, size), size), :]

    def half_rows(f, i):
        return pl.ds(pl.multiple_of(f * width + i * half_width, half_width), half_width)

    kinds, head_kinds = [], []
    for i in range(2):
        kinds.append(
            (
                lambda f, i=i: gate_full.at[half_rows(f, i), :],
                gate_away.at[pl.ds(i * half_width, half_width), :],
                half_width // 2,
            )
        )
    kinds.append((lambda f: up_full.at[rows_of(f), :], up_away, half_width))
    kinds.append((lambda f: down_full.at[f], down_away, half_units))
    up_kind, down_kind = 2, 3
    for h in range(heads):
        head_kinds.append([len(kinds)])
        kinds.append(
            (lambda f, h=h: head_full.at[h, rows_of(f), :], head_away.at[h], half_width)
        )
    out_kind = len(kinds)
    kinds.append((lambda f: out_full.at[f], out_away, half_out))
    scales = len(kinds)
    kinds.append((lambda f: cols_full.at[f], cols_away, 8))
    rounds = [[0, 1, up_kind], [down_kind, scales], *head_kinds, [out_kind]]
    bank_of, last_bank = {}, 0
    for members in rounds:
        for kind in members:
            bank_of[kind] = last_bank
            last_bank = (last_bank + 1) % 3

    def piece(kind, f, s):
        if kind == scales:
            return kinds[kind][0](f).at[pl.ds(pl.multiple_of(s * 8, 8), 1), :]
        return cut(kinds[kind][0](f), s, kinds[kind][2])

    def remote(src, dst, send_sem, recv_sem, peer):
        return pltpu.make_async_remote_copy(
            src_ref=src,
            dst_ref=dst,
            send_sem=send_sem,
            recv_sem=recv_sem,
            device_id=peer,
            device_id_type=MESH,
        )

    def across(o):
        return spot * 2 + side + o * (1 - 2 * side)

    def side_slot(kind, i):
        return kind * 2 + i if kind <= up_kind else kind + 3

    def side_copy(kind, i, f):
        slot_of = side_slot(kind, i)
        sems = side_send.at[slot_of], side_recv.at[slot_of]
        if kind <= up_kind:
            s = twin if i == 0 else 1 - twin
            return remote(
                cut(kinds[kind][1], s, kinds[kind][2]), piece(kind, f, s), *sems, side_peer
            )
        return remote(kinds[kind][1], kinds[kind][0](f), *sems, side_peer)

    def side_start(kind, i=0):
        copy = side_copy(kind, i, fs)
        copy.start()
        started.append(copy)

    side_done = set()

    def side_need(kind, i):
        i = i if kind <= up_kind else 0
        if (kind, i) not in side_done:
            side_done.add((kind, i))
            side_copy(kind, i, across(1)).wait_recv()

    span_of = 2 * (line - 1)
    sending = {}

    def push(kind, group, index, f, where, recv, peer):
        bank = bank_of[kind]
        slot_of = (bank * 2 + group) * span_of + index
        copy = remote(piece(kind, f, twin), piece(kind, f, twin), line_send.at[slot_of], recv, peer)
        if slot_of in sending:
            sending.pop(slot_of)()
        guard = functools.partial(pl.when, where) if where is not None else None

        def begin():
            copy.start()

        def finish():
            copy.wait_send()

        if guard is None:
            begin()
            sending[slot_of] = finish
        else:
            guard()(begin)
            sending[slot_of] = lambda: guard()(finish)

    def line_slot(kind, away, o):
        return line_recv.at[kind * span_of + (away % line - 1) * 2 + o]

    def twin_slot(kind, away, o):
        return twin_recv.at[kind * span_of + (away - 1) * 2 + o]

    def send_own(kind, o):
        if o == 1:
            side_need(kind, 0)
        f = across(o)
        push(kind, 0, o, f, has_above, line_slot(kind, -1, o), above)
        push(kind, 1, o, f, has_below, line_slot(kind, 1, o), below)

    def places(d, o):
        for group, away in ((1, d), (0, -d)):
            from_spot = spot + away
            exists = from_spot >= 0 if away < 0 else from_spot < line
            yield group, away, exists, from_spot * 2 + side + o * (1 - 2 * side)

    def take_in(kind, d, o):
        for group, away, exists, f in places(d, o):

            def receive(kind=kind, away=away, f=f):
                remote(
                    piece(kind, f, twin),
                    piece(kind, f, twin),
                    line_send.at[0],
                    line_slot(kind, away, o),
                    above,
                ).wait_recv()

            pl.when(exists)(receive)
            hand_over(kind, away, o, f, exists)

    def move_on(kind, d, o):
        if d > line - 2:
            return
        for group, away, exists, f in places(d, o):
            further = -d - 1 if away < 0 else d + 1
            push(
                kind,
                group,
                2 * d + o,
                f,
                jnp.logical_and(exists, has_above if away < 0 else has_below),
                line_slot(kind, further, o),
                above if away < 0 else below,
            )

    def pass_along(kind, d, o):
        take_in(kind, d, o)
        move_on(kind, d, o)

    def hand_over(kind, away, o, f, exists):
        copy = remote(
            piece(kind, f, twin),
            piece(kind, f, twin),
            twin_send.at[kind],
            twin_slot(kind, away % line, o),
            twin_peer,
        )
        pl.when(exists)(lambda: copy.start())

    def handed_over():
        shards = pl.ds(0, line - 1)
        sent = [gate_full.at[pl.ds(0, (line - 1) * half_width), :]] * 2
        sent += [up_full.at[pl.ds(0, (line - 1) * width), :], down_full.at[shards]]
        sent += [head_full.at[h, pl.ds(0, (line - 1) * width), :] for h in range(heads)]
        sent += [out_full.at[shards], cols_full.at[0, pl.ds(0, span_of), :]]
        for kind, ref in enumerate(sent):
            remote(ref, ref, twin_send.at[kind], twin_recv.at[0], twin_peer).wait_send()

    def pick(table):
        total = 0
        for v in range(line):
            total = total + (spot == v).astype(jnp.int32) * table[v]
        return total

    near = []
    for v in range(line):
        near.append(sorted((u for u in range(line) if u != v), key=lambda u: (abs(u - v), -u)))
    sources = [across(0), across(1)]
    twin_index = [None, None]
    for r in range(line - 1):
        at = pick([near[v][r] for v in range(line)])
        away = pick([(near[v][r] - v) % line for v in range(line)])
        for o in range(2):
            sources.append(at * 2 + side + o * (1 - 2 * side))
            twin_index.append((away - 1) * 2 + o)

    def need_piece(kind, k):
        if k == 1:
            side_need(kind, 0)
            side_need(kind, 1)
        if k > 1:
            remote(
                piece(kind, sources[k], 1 - twin),
                piece(kind, sources[k], 1 - twin),
                line_send.at[0],
                twin_recv.at[kind * span_of + twin_index[k]],
                twin_peer,
            ).wait_recv()

    spots = [spot] + [lax.div(sources[2 * r], 2) for r in range(1, line)]
    queue = []
    later = []
    for members in rounds:
        for o in range(2):
            queue.append([functools.partial(send_own, m, o) for m in members])
        queue.extend(later)
        later = []
        for d in range(1, line):
            for o in range(2):
                unit = [functools.partial(pass_along, m, d, o) for m in members]
                (queue if d < line - 1 else later).append(unit)
    queue.extend(later)
    middle = 2 * (line - 2)

    def pump(count):
        for _ in range(count):
            for action in queue.pop(0):
                action()

    def send(src, dst, send_sem, recv_sem, peer):
        copy = remote(src, dst, send_sem, recv_sem, peer)
        copy.start()
        started.append(copy)
        return copy

    own_rows = rows_of(fs)
    fetched(("gate", 0))
    gate_full[own_rows, :] = staged_gate[0].astype(bf16)
    neighbours = has_above.astype(jnp.int32) + has_below.astype(jnp.int32)
    pl.semaphore_wait(barrier, 3 + neighbours)
    first, second, _ = (queue.pop(0) for _ in range(3))
    first[0]()
    first[1]()
    fetched(("gate", 1))
    gate_away[...] = staged_gate[1].astype(bf16)
    side_start(0)
    side_start(1)
    fetched(("up", 0))
    up_full[own_rows, :] = staged_up[0].astype(bf16)
    first[2]()
    fetched(("up", 1))
    up_away[...] = staged_up[1].astype(bf16)
    side_start(up_kind)
    fetched("rows")
    fetched("small")

    def norm_rows(source, which, target):
        gain = norm_gains[which : which + 1, :]

        def step(i, carry):
            block = pl.ds(pl.multiple_of(i * 16, 16), 16)
            x = source[block, :].astype(f32)
            mean = jnp.mean(x * x, axis=-1, keepdims=True)
            target[block, :] = (x * lax.rsqrt(mean + EPSILON) * gain).astype(bf16)
            return carry

        lax.fori_loop(0, rows // 16, step, 0)

    def slot(j, cols=slice(None)):
        return (pl.ds(j * rows, rows), cols)

    def share_rows(stage):
        part = gathered.at[stage]
        base = 3 * stage
        send(part.at[slot(0)], part.at[slot(1)], row_send.at[base], row_recv.at[base], tp_peer)
        send(
            part.at[slot(0)],
            part.at[slot(2)],
            row_send.at[base + 1],
            row_recv.at[base + 1],
            side_peer,
        )

    def wait_rows(stage, i, j):
        part = gathered.at[stage]
        pltpu.make_async_remote_copy(
            src_ref=part.at[slot(0)],
            dst_ref=part.at[slot(j)],
            send_sem=row_send.at[3 * stage + i],
            recv_sem=row_recv.at[3 * stage + i],
            device_id=tp_peer,
            device_id_type=MESH,
        ).wait_recv()

    def relay_rows(stage):
        wait_rows(stage, 1, 2)
        part = gathered.at[stage]
        send(
            part.at[slot(2)],
            part.at[slot(3)],
            row_send.at[3 * stage + 2],
            row_recv.at[3 * stage + 2],
            tp_peer,
        )

    norm_rows(staged_in, 0, gathered.at[0])
    stream[...] = staged_in[...].astype(f32)
    fetched("down")
    down_full[fs] = staged_down[0].astype(bf16)
    down_away[...] = staged_down[1].astype(bf16)
    cols_full[fs, 0:1, :] = down_scale[...]
    cols_full[fs, 8:9, :] = out_scale[...]
    cols_away[0:1, :] = down_scale[...]
    cols_away[8:9, :] = out_scale[...]
    side_start(0, 1)
    side_start(1, 1)
    side_start(up_kind, 1)
    side_start(down_kind)
    side_start(scales)
    take_in(0, 1, 0)
    take_in(1, 1, 0)
    second[0]()
    second[1]()
    take_in(up_kind, 1, 0)
    second[2]()
    move_on(0, 1, 0)
    move_on(1, 1, 0)
    move_on(up_kind, 1, 0)
    share_rows(0)
    fetched("heads")
    for h in range(heads):
        keys, vals = slice(h * DK, (h + 1) * DK), slice(h * DV, (h + 1) * DV)
        for i in range(2):
            made = jnp.concatenate(
                [staged_query[i, :, keys], staged_key[i, :, keys], staged_value[i, :, vals]], axis=1
            ).astype(bf16)
            if i == 0:
                head_full[h, own_rows, :] = made
            else:
                head_away[h] = made
        for kind in head_kinds[h]:
            side_start(kind)
    fetched("out")
    out_full[fs] = staged_out[0].astype(bf16)
    out_away[...] = staged_out[1].astype(bf16)
    side_start(out_kind)

    pump(middle + 2)
    relay_rows(0)
    pump(middle + 1)
    wait_rows(0, 0, 1)
    wait_rows(0, 2, 3)

    def dot(a, b):
        return jnp.dot(a, b, preferred_element_type=f32)

    def expand(factor, part, first=0, count=4 * rows):
        for c in range(units // tile):
            cols = slice(c * tile, (c + 1) * tile)
            span = pl.ds(pl.multiple_of(side * units + c * tile, 128), tile)
            rows_in, lhs = part
            block = slice(first, first + count)
            gate = dot(lhs[block], gate_full[rows_in, cols])
            up = dot(lhs[block], up_full[rows_in, cols])
            if factor is not None:
                gate = (gate + summed[0, block, cols]) * factor[block]
                up = (up + summed[1, block, cols]) * factor[block]
            gate, up = gate * gate_scale[:, span], up * up_scale[:, span]
            hidden[block, cols] = (gate / (1.0 + jnp.exp(-gate)) * up).astype(bf16)

    def part_copy(stage, k, way, landing):
        store_out, store_in = (rep_out, rep_in) if way == 2 else (tp_out, tp_in)
        return remote(
            store_out.at[stage, k] if way == 2 else store_out.at[stage, k, way],
            store_in.at[stage, landing] if way == 2 else store_in.at[stage, landing, way],
            part_send.at[stage * 2 + way // 2],
            part_recv.at[landing * 3 + way],
            side_peer if way == 2 else tp_peer,
        )

    def part_start(stage, k, way):
        part_copy(stage, k, way, k ^ 1 if way == 2 else k).start()

    def part_wait(stage, k, way):
        part_copy(stage, k, way, k).wait_recv()

    def parts_sent(stage):
        for over_side, (src, dst) in enumerate(((tp_out, tp_in), (rep_out, rep_in))):
            remote(
                src.at[stage],
                dst.at[stage],
                part_send.at[stage * 2 + over_side],
                part_recv.at[0],
                side_peer,
            ).wait_send()

    def contract(stage, lhs, weight, row, fresh, order, finish, relay=None, extra=None, near=None):
        def ready(k):
            if fresh is not None:
                need_piece(fresh, k)
                if fresh == down_kind:
                    need_piece(scales, k)

        def product(k, block):
            f = sources[k]
            return dot(lhs[block, :], weight[f]) * cols_full[f, 8 * row : 8 * row + 1, :]

        def keep(k, way, part):
            (far_part if way else own_part)[k] = part[:rows]
            tp_out[stage, k, way] = part[rows:].astype(bf16)
            part_start(stage, k, way)

        def multiply(k):
            ready(k)
            part = product(k, slice(None))
            keep(k, 1, part[2 * rows :])
            keep(k, 0, part[: 2 * rows])

        def multiply_far(k):
            ready(k)
            keep(k, 1, product(k, slice(2 * rows, 4 * rows)))

        def multiply_near(k):
            keep(k, 0, product(k, slice(0, 2 * rows)))

        def pass_on(k):
            part_wait(stage, k, 1)
            rep_out[stage, k] = (far_part[k] + tp_in[stage, k, 1].astype(f32)).astype(bf16)
            part_start(stage, k, 2)

        def collect(k):
            part_wait(stage, k, 0)
            part_wait(stage, k, 2)
            total = own_part[k] + tp_in[stage, k, 0].astype(f32) + rep_in[stage, k].astype(f32)
            finish(k, sources[k], total)

        actions = {"m": multiply, "p": pass_on, "c": collect, "r": relay, "u": pump, "x": extra}
        actions.update({"f": multiply_far, "n": multiply_near, "near": lambda _: near()})
        for action, k in order:
            actions[action](k)

    def last_order():
        order = []
        for k in range(n):
            order.append(("f", k))
            if k > 0:
                order.append(("p", k - 1))
        order += [("p", n - 1), ("near", 0)]
        return order + [("n", k) for k in range(n)] + [("c", k) for k in range(n)]

    def first_order():
        order = [("m", 0), ("m", 1), ("p", 0), ("p", 1), ("u", 4)]
        for k in range(2, n):
            if k == 2 * (line - 1):
                order.append(("u", 2))
            order.append(("m", k))
            if k > 2:
                order.append(("p", k - 1))
        order.append(("p", n - 1))
        order += [("c", k) for k in range(n)]
        order.insert(-2, ("u", 1))
        return order

    def tail_order():
        order, waiting, relayed = [], [], []

        def advance(r):
            ks = (2 * r, 2 * r + 1)
            order.extend([("m", k) for k in ks] + [("p", k) for k in ks])
            waiting.append(ks)

        def take():
            if waiting:
                ks = waiting.pop(0)
                order.extend(("c", k) for k in ks)
                relayed.append(ks)

        order.extend([("f", 0), ("f", 1), ("p", 0), ("p", 1), ("u", 2)])
        order.extend([("f", 2), ("near", 0), ("n", 0), ("n", 1), ("n", 2)])
        order.extend([("p", 2), ("f", 3), ("n", 3), ("p", 3), ("c", 0), ("c", 1)])
        waiting.append((2, 3))
        relayed.append((0, 1))
        for r in range(3, line):
            order.append(("u", 2))
            advance(r - 1)
            take()
        advance(line - 1)
        for ks in relayed[:1]:
            order.extend(("r", k) for k in relayed.pop(0))
        while waiting:
            take()
            order.extend(("r", k) for k in relayed.pop(0))
        order.extend(("r", k) for ks in relayed for k in ks)
        for r in range(line - 2):
            order.insert(order.index(("r", 2 * r + 3)) + 1, ("x", r))
        return order

    def need_all(kind):
        for k in range(1, n):
            need_piece(kind, k)

    need_all(0)
    need_all(1)
    need_all(up_kind)
    expand(None, (slice(None), gathered[0]))

    def add_half(k, f, total):
        cols = columns_of(f)
        stream[:, cols] = stream[:, cols] + 0.5 * total

    contract(0, hidden, down_full, 0, down_kind, first_order(), add_half)

    norm_rows(stream, 1, gathered.at[1])
    share_rows(1)
    pump(middle + 1)
    relay_rows(1)
    pump(2)

    seq_len = 2 * rows
    row = lax.rem(
        lax.broadcasted_iota(jnp.int32, (seq_len, seq_len), 0) + tp * rows, seq_len
    )
    col = lax.rem(
        lax.broadcasted_iota(jnp.int32, (seq_len, seq_len), 1) + tp * rows, seq_len
    )

    def retain(h, parts=(0, 1), again=False):
        start, stop = parts[0] * seq_len, (parts[-1] + 1) * seq_len
        places = [
            (query_scale, 0, DK, 1.0),
            (key_scale, DK, DK, 1.0 / math.sqrt(DK)),
            (value_scale, 2 * DK, DV, 1.0),
        ]
        for r in range(line - 1 if again else 0, line):
            for k in (2 * r, 2 * r + 1):
                for kind in head_kinds[h] if not again else []:
                    need_piece(kind, k)
            rows_in = pl.ds(pl.multiple_of(spots[r] * 2 * width, 2 * width), 2 * width)
            block = slice(start, stop) if r == line - 1 else slice(0, 2 * seq_len)
            lhs, made = gathered[1, block, rows_in], []
            for scale, first, size, factor in places:
                cols = slice(first, first + size)
                product = dot(lhs, head_full[h, rows_in, cols])
                if r > 0:
                    product = product + projected[block, cols]
                if r < line - 1:
                    projected[block, cols] = product
                else:
                    span = pl.ds(pl.multiple_of((side * heads + h) * size, 128), size)
                    made.append((product * (scale[:, span] * factor)).astype(bf16))
        query, keys, values = made
        decay = decay_rate[side * heads + h]
        distance = jnp.abs(row - col).astype(f32)
        weight = jnp.where(
            lax.div(col, BLOCK) <= lax.div(row, BLOCK), jnp.exp(-decay * distance), 0.0
        )
        for s in parts:
            span = slice(s * seq_len - start, (s + 1) * seq_len - start)
            scores = lax.dot_general(
                query[span], keys[span], (((1,), (1,)), ((), ())), preferred_element_type=f32
            )
            scores = (scores * weight).astype(bf16)
            retained = dot(scores, values[span])
            centred = retained - jnp.mean(retained, axis=-1, keepdims=True)
            spread = jnp.mean(centred * centred, axis=-1, keepdims=True)
            mixed[s * seq_len : (s + 1) * seq_len, h * DV : (h + 1) * DV] = (
                centred * lax.rsqrt(spread + EPSILON) * head_gain[...]
            ).astype(bf16)

    for h in range(heads):
        if h == 0:
            wait_rows(1, 0, 1)
            wait_rows(1, 2, 3)
        if h < heads - 1:
            retain(h)
            pump(1)
        else:
            retain(h, (1,))
        if h < heads - 1:
            pump(middle - 3 + 6)

    last = gathered.at[2]

    def block_copy(k, i, start):
        cols = columns_of(sources[k])
        a, b, peer = ((0, 1, tp_peer), (0, 2, side_peer), (2, 3, tp_peer))[i]
        return pltpu.make_async_remote_copy(
            src_ref=last.at[slot(a, cols)],
            dst_ref=last.at[slot(b, cols)],
            send_sem=block_send.at[i],
            recv_sem=block_recv.at[n + (k ^ 1 if start else k) if i == 1 else i * line // 2 + k // 2],
            device_id=peer,
            device_id_type=MESH,
        )

    def factor_copy(i):
        a, b, peer = ((0, 1, tp_peer), (0, 2, side_peer), (2, 3, tp_peer))[i]
        return pltpu.make_async_remote_copy(
            src_ref=factors.at[a],
            dst_ref=factors.at[b],
            send_sem=block_send.at[3 + i],
            recv_sem=block_recv.at[2 * n + i],
            device_id=peer,
            device_id_type=MESH,
        )

    squares[...] = jnp.zeros_like(squares)

    def add_mix(k, f, total):
        cols = columns_of(f)
        second = stream[:, cols] + total
        stream[:, cols] = second
        last[slot(0, cols)] = (second * norm_gains[2:3, cols]).astype(bf16)
        square = second * second
        added = squares[...]
        for i in range(width // 128):
            added = added + square[:, i * 128 : (i + 1) * 128]
        squares[...] = added
        for i in (0, 1):
            block_copy(k, i, True).start()
        if k == n - 1:
            mean = jnp.sum(added, axis=-1, keepdims=True) / features
            wide = jnp.broadcast_to(lax.rsqrt(mean + EPSILON), (rows, rows))
            factors[0] = wide.T[:8, :]
            for i in (0, 1):
                copy = factor_copy(i)
                copy.start()
                started.append(copy)

    def relay_block(k):
        block_copy(k, 1, False).wait_recv()
        block_copy(k, 2, True).start()
        if k == n - 1:
            factor_copy(1).wait_recv()
            copy = factor_copy(2)
            copy.start()
            started.append(copy)


    def arrived_block(r):
        both = pl.ds(pl.multiple_of(spots[r] * 2 * width, 2 * width), 2 * width)
        for i, j in ((0, 1), (2, 3)):
            block = last.at[slot(j, both)]
            recv_sem = block_recv.at[i * line // 2 + r]
            remote(block, block, block_send.at[0], recv_sem, tp_peer).wait_recv()
        return both

    def take_sum(r):
        rows_in = arrived_block(r)
        lhs = last[:, rows_in]
        for c in range(units // tile):
            cols = slice(c * tile, (c + 1) * tile)
            for i, weight in enumerate((gate_full, up_full)):
                part = dot(lhs, weight[rows_in, cols])
                summed[i, :, cols] = part if r == 0 else summed[i, :, cols] + part

    contract(1, mixed, out_full, 1, out_kind, tail_order(), add_mix, relay_block, take_sum, lambda: retain(heads - 1, (0,), True))
    take_sum(line - 2)
    rows_in = arrived_block(line - 1)
    factor_copy(0).wait_recv()
    factor_copy(2).wait_recv()
    factor = jnp.concatenate(
        [jnp.broadcast_to(factors[j, 0:1, :], (rows, rows)).T[:, 0:1] for j in range(4)], axis=0
    )
    late = (rows_in, last[:, rows_in])
    expand(factor, late, 2 * rows, 2 * rows)

    def write(k, f, total):
        cols = columns_of(f)
        result[:, cols] = (stream[:, cols] + 0.5 * total).astype(bf16)

    contract(2, hidden, down_full, 0, None, last_order(), write, near=lambda: expand(factor, late, 0, 2 * rows))
    assert not queue
    for stage in range(3):
        parts_sent(stage)
    for i, a in enumerate((0, 0, 2)):
        remote(
            last.at[slot(a)], last.at[slot(a)], block_send.at[i], block_recv.at[0], tp_peer
        ).wait_send()
    handed_over()
    for finish in sending.values():
        finish()
    for copy in started:
        copy.wait_send()


def fused(
    n_rep,
    n_fs,
    n_tp,
    tokens_in,
    norm_gains,
    gate_w,
    gate_scale,
    up_w,
    up_scale,
    down_w,
    down_scale,
    query_w,
    query_scale,
    key_w,
    key_scale,
    value_w,
    value_scale,
    out_w,
    out_scale,
    head_gain,
    decay_rate,
):
    f32, bf16 = jnp.float32, jnp.bfloat16
    n = n_fs
    rows, features = tokens_in.shape
    width, units = gate_w.shape[0], gate_w.shape[1] // 2
    heads = decay_rate.shape[0] // 2
    kinds = heads + 6
    span_of = n - 2
    any_space = pl.BlockSpec(memory_space=pl.ANY)
    vmem = pl.BlockSpec(memory_space=pltpu.VMEM)
    smem = pl.BlockSpec(memory_space=pltpu.SMEM)
    dma = pltpu.SemaphoreType.DMA

    return pl.pallas_call(
        functools.partial(layer_kernel, n),
        out_shape=pltpu.VMEM((rows, features), bf16),
        in_specs=[any_space] * 17 + [smem],
        out_specs=vmem,
        scratch_shapes=[
            pltpu.VMEM(norm_gains.shape, f32),
        ]
        + [
            pltpu.VMEM((1, x.shape[0]), f32)
            for x in (
                gate_scale,
                up_scale,
                down_scale,
                query_scale,
                key_scale,
                value_scale,
                out_scale,
                head_gain,
            )
        ]
        + [
            pltpu.VMEM((rows, features), bf16),
            pltpu.VMEM((2, width, units), f32),
            pltpu.VMEM((2, width, units), f32),
            pltpu.VMEM((2, units, width), f32),
            pltpu.VMEM((2, width, heads * DK), f32),
            pltpu.VMEM((2, width, heads * DK), f32),
            pltpu.VMEM((2, width, heads * DV), f32),
            pltpu.VMEM((2, heads * DV, width), f32),
            pltpu.VMEM((width, units), bf16),
            pltpu.VMEM((width, units), bf16),
            pltpu.VMEM((units, width), bf16),
            pltpu.VMEM((heads, width, 2 * DK + DV), bf16),
            pltpu.VMEM((heads * DV, width), bf16),
            pltpu.VMEM((16, width), f32),
            pltpu.VMEM((features, units), bf16),
            pltpu.VMEM((features, units), bf16),
            pltpu.VMEM((n, units, width), bf16),
            pltpu.VMEM((heads, features, 2 * DK + DV), bf16),
            pltpu.VMEM((n, heads * DV, width), bf16),
            pltpu.VMEM((n, 16, width), f32),
            pltpu.VMEM((3, 4 * rows, features), bf16),
            pltpu.VMEM((4, 8, rows), f32),
            pltpu.VMEM((rows, features), f32),
            pltpu.VMEM((rows, 128), f32),
            pltpu.VMEM((2, 4 * rows, units), f32),
            pltpu.VMEM((4 * rows, 2 * DK + DV), f32),
            pltpu.VMEM((4 * rows, units), bf16),
            pltpu.VMEM((4 * rows, heads * DV), bf16),
            pltpu.VMEM((n, rows, width), f32),
            pltpu.VMEM((n, rows, width), f32),
            pltpu.VMEM((3, n, 2, rows, width), bf16),
            pltpu.VMEM((3, n, 2, rows, width), bf16),
            pltpu.VMEM((3, n, rows, width), bf16),
            pltpu.VMEM((3, n, rows, width), bf16),
            dma((24,)),
            dma((kinds + 3,)),
            dma((kinds + 3,)),
            dma((6 * span_of,)),
            dma((kinds * span_of,)),
            dma((kinds,)),
            dma((kinds * span_of,)),
            dma((6,)),
            dma((3 * n,)),
            dma((6,)),
            dma((6,)),
            dma((6,)),
            dma((2 * n + 3,)),
        ],
        compiler_params=pltpu.CompilerParams(
            collective_id=0, has_side_effects=True, vmem_limit_bytes=VMEM_LIMIT
        ),
        name="layer",
    )(
        tokens_in,
        norm_gains,
        gate_w,
        gate_scale,
        up_w,
        up_scale,
        down_w,
        down_scale,
        query_w,
        query_scale,
        key_w,
        key_scale,
        value_w,
        value_scale,
        out_w,
        out_scale,
        head_gain,
        decay_rate,
    )


def solution(mesh):
    sizes = [mesh.shape[axis] for axis in ("rep", "fs", "tp")]
    placed = (
        P(("rep", "fs", "tp"), None),
        P(),
        P("fs", "tp"),
        P("tp"),
        P("fs", "tp"),
        P("tp"),
        P("tp", "fs"),
        P("fs"),
        P("fs", "tp"),
        P("tp"),
        P("fs", "tp"),
        P("tp"),
        P("fs", "tp"),
        P("tp"),
        P("tp", "fs"),
        P("fs"),
        P(),
        P("tp"),
    )
    return jax.shard_map(
        lambda *args: (fused if fits(*sizes, *args) else on_device)(*sizes, *args),
        mesh=mesh,
        in_specs=placed,
        out_specs=P(("rep", "fs", "tp"), None),
        check_vma=False,
    )
```
